128 devices in a mesh: sp: 16 (over z, y), tp: 8 (over x, core).
Axes of the slice: x: 4, y: 4, z: 4, core: 2. Of those that a mesh axis runs over, the one named last changes fastest.
Arguments:
- tokens: bfloat16 [12288, 2048], P(('sp', 'tp')), may hold values from -6 to 6
- norm_gain: float32 [2048], replicated, may hold values from 0.1 to 1.9
- w_query: bfloat16 [2048, 1024], P('sp', 'tp'), may hold values from -0.125 to 0.125
- w_forget: bfloat16 [2048, 1024], P('sp', 'tp'), may hold values from -0.125 to 0.125
- w_input: bfloat16 [2048, 1024], P('sp', 'tp'), may hold values from -0.125 to 0.125
- w_outgate: bfloat16 [2048, 1024], P('sp', 'tp'), may hold values from -0.125 to 0.125
- w_conv_value: bfloat16 [2048, 1024], P('sp', 'tp'), may hold values from -0.125 to 0.125
- w_conv_gate: bfloat16 [2048, 1024], P('sp', 'tp'), may hold values from -0.125 to 0.125
- w_gate_rec: bfloat16 [2048, 2048], P('sp', 'tp'), may hold values from -0.125 to 0.125
- w_gate_conv: bfloat16 [2048, 2048], P('sp', 'tp'), may hold values from -0.125 to 0.125
- lower_bound: float32 [1024], P('tp'), may hold values from 0.92 to 0.9999593, as said below
- decay_shift: float32 [12288, 1024], P('sp', 'tp'), may hold values from -0.7 to 0, as said below
- state_init: float32 [8, 128, 128], P('tp'), may hold values from -0.125 to 0.125
- head_gain: float32 [1024], P('tp'), may hold values from 0.1 to 1.9
- conv_kernel: float32 [31, 1024], P(None, 'tp'), may hold values from -7.5 to 7.5
- channel_gain: float32 [1024], P('tp'), may hold values from 0.1 to 1.9
- channel_bias: float32 [1024], P('tp'), may hold values from -3 to 3
- w_out_rec: bfloat16 [1024, 2048], P('tp', 'sp'), may hold values from -0.1875 to 0.1875
- w_out_conv: bfloat16 [1024, 2048], P('tp', 'sp'), may hold values from -0.1875 to 0.1875
Outputs:
- mixed_out: bfloat16 [12288, 2048], P('sp', 'tp')
The draws below stay inside these ranges and needn't reach their ends.
Inputs may be any that keep to these rules, and one draw needn't show every extreme that they name: `lower_bound`: every entry is below one. `decay_shift`: no entry is positive.
All inputs are finite; a program needn't handle non-finite values.
Results may differ from the reference program's by a relative error of at most 0.017.
Values may be sent and summed in bfloat16 or wider, within the bound.
A program may use at most 64 MiB of HBM per device.

```python
import math
import jax
import jax.numpy as jnp
from jax import lax

D = 2048
HEADS = 8
HEAD = 128
CONV = 1024
KW = 31
BLOCK = 64
T_DEV = 768
HD = 1024
TOKENS = 12288


def draw_lower_bound(key, part):
    base_key = jax.random.fold_in(key, 11)
    head_key, slow_key, quick_seed = jax.random.split(base_key, 3)
    share = 0.5
    slow_heads = jax.random.uniform(head_key, (HEADS,), jnp.float32) < share
    slow_rate = jnp.exp(jax.random.uniform(slow_key, (HEADS, HEAD), jnp.float32, math.log(0.5), math.log(1.5))) / TOKENS
    fast_rate = jnp.exp(jax.random.uniform(quick_seed, (HEADS, HEAD), jnp.float32, math.log(0.03), math.log(0.08)))
    rate = jnp.where(slow_heads[:, None], slow_rate, fast_rate)
    return (1.0 - rate).reshape(HEADS * HEAD).astype(jnp.float32)


def draw_decay_shift(key, part):
    base_key = jax.random.fold_in(key, 23)
    block_key, position_key, depth_key = jax.random.split(base_key, 3)
    block_rate = jnp.exp(jax.random.uniform(block_key, (TOKENS // T_DEV,), jnp.float32, math.log(0.2), math.log(1.6)))
    starting_index = -jnp.repeat(block_rate, T_DEV) / TOKENS
    spots = jax.random.randint(position_key, (HEADS, 2), 0, TOKENS)
    places = jnp.arange(TOKENS, dtype=jnp.int32)
    dropped_sequence_items = jnp.any(places[:, None, None] == spots[None, :, :], axis=-1)
    memory_dimension = jax.random.uniform(depth_key, (TOKENS, HEADS, HEAD), jnp.float32, 0.22, 0.69)
    segment_span = jnp.where(dropped_sequence_items[:, :, None], -memory_dimension, 0.0)
    overall_aggregate = starting_index[:, None, None] + segment_span
    return overall_aggregate.reshape(TOKENS, HEADS * HEAD).astype(jnp.float32)


def draw_conv_kernel(key, part):
    base_key = jax.random.fold_in(key, 37)
    value_key = jax.random.fold_in(base_key, 0)
    rising = jnp.exp(math.log(6.0) * jnp.arange(CONV, dtype=jnp.float32) / CONV)
    entries = jnp.clip(jax.random.normal(value_key, (KW, CONV), jnp.float32), -4.0, 4.0)
    return (entries * rising / math.sqrt(KW)).astype(jnp.float32)


def block_levels(stream_key, dims, cuts, low, high):
    factor_of = 1.0
    for axis_at, parts in cuts:
        heights = jax.random.uniform(jax.random.fold_in(jax.random.fold_in(stream_key, 6), axis_at), (parts,), jnp.float32, low / len(cuts), high / len(cuts))
        factor_of = factor_of * jnp.repeat(jnp.exp(heights), dims[axis_at] // parts).reshape((-1,) + (1,) * (len(dims) - 1 - axis_at))
    return factor_of


def centred(key, dims, deviation, most, pieces=(), kind=jnp.bfloat16):
    values = deviation * jax.random.normal(key, dims, jnp.float32)
    if pieces:
        values = values * block_levels(key, dims, pieces, -0.22, 0.18)
    return jnp.clip(values, -most, most).astype(kind)


def setup_inputs(seed: int = 0) -> dict:
    key_of = jax.random.split(jax.random.key(seed), 20)
    tokens = centred(key_of[0], (TOKENS, D), 1.0, 6.0, ((0, 128),))
    norm_gain = jnp.clip(1.0 + 0.18 * jax.random.normal(key_of[1], (D,), jnp.float32), 0.1, 1.9)
    w_query = centred(key_of[2], (D, HD), D ** -0.5, 0.125, ((0, 16), (1, 8)))
    w_forget = centred(key_of[3], (D, HD), D ** -0.5, 0.125, ((0, 16), (1, 8)))
    w_input = centred(key_of[4], (D, HD), D ** -0.5, 0.125, ((0, 16), (1, 8)))
    w_outgate = centred(key_of[5], (D, HD), D ** -0.5, 0.125, ((0, 16), (1, 8)))
    w_conv_value = centred(key_of[6], (D, CONV), D ** -0.5, 0.125, ((0, 16), (1, 8)))
    w_conv_gate = centred(key_of[7], (D, CONV), D ** -0.5, 0.125, ((0, 16), (1, 8)))
    w_gate_rec = centred(key_of[8], (D, D), D ** -0.5, 0.125, ((0, 16), (1, 8)))
    w_gate_conv = centred(key_of[9], (D, D), D ** -0.5, 0.125, ((0, 16), (1, 8)))
    lower_bound = draw_lower_bound(jax.random.fold_in(key_of[19], 71), 0)
    decay_shift = draw_decay_shift(jax.random.fold_in(key_of[19], 71), 0)
    state_init = centred(key_of[12], (HEADS, HEAD, HEAD), (TOKENS ** -0.5), 0.125, ((0, 8),), jnp.float32)
    head_gain = jnp.clip(1.0 + 0.18 * jax.random.normal(key_of[13], (HD,), jnp.float32), 0.1, 1.9)
    conv_kernel = draw_conv_kernel(jax.random.fold_in(key_of[19], 71), 0)
    channel_gain = jnp.clip(1.0 + 0.18 * jax.random.normal(key_of[15], (CONV,), jnp.float32), 0.1, 1.9)
    channel_bias = centred(key_of[16], (CONV,), 0.5, 3.0, ((0, 8),), jnp.float32)
    w_out_rec = centred(key_of[17], (HD, D), HD ** -0.5, 0.1875, ((0, 8), (1, 16)))
    w_out_conv = centred(key_of[18], (CONV, D), CONV ** -0.5, 0.1875, ((0, 8), (1, 16)))
    return dict(tokens=tokens, norm_gain=norm_gain, w_query=w_query, w_forget=w_forget, w_input=w_input, w_outgate=w_outgate, w_conv_value=w_conv_value, w_conv_gate=w_conv_gate, w_gate_rec=w_gate_rec, w_gate_conv=w_gate_conv, lower_bound=lower_bound, decay_shift=decay_shift, state_init=state_init, head_gain=head_gain, conv_kernel=conv_kernel, channel_gain=channel_gain, channel_bias=channel_bias, w_out_rec=w_out_rec, w_out_conv=w_out_conv)


EPSILON = 1e-06
highest_precision = lax.Precision.HIGHEST

def normalize_rows(values, gain_vector):
    widened = values.astype(jnp.float32)
    scale = lax.rsqrt(lax.optimization_barrier(jnp.mean(widened * widened, axis=-1, keepdims=True)) + EPSILON)
    return (widened * scale * gain_vector).astype(jnp.bfloat16)

def block_step(state, inputs):
    query, input_gate, values, log_decay = inputs
    length = query.shape[1]
    causal_masked = (jnp.arange(length)[:, None] >= jnp.arange(length)[None, :])[None, :, :, None]
    cumulative = jnp.cumsum(log_decay, axis=1)
    spread = cumulative[:, :, None, :] - cumulative[:, None, :, :]
    weight = jnp.where(causal_masked, jnp.exp(jnp.where(causal_masked, spread, 0.0)), 0.0)
    scores = jnp.einsum('htd,hsd,htsd->hts', query, input_gate, weight, precision=highest_precision)
    output = jnp.einsum('hts,hsv->htv', scores, values, precision=highest_precision)
    output = output + jnp.einsum('htd,hdv->htv', query * jnp.exp(cumulative), state, precision=highest_precision)
    final = cumulative[:, -1:, :]
    carried = jnp.exp(final[:, 0, :])[:, :, None] * state
    carried = carried + jnp.einsum('hsd,hsv->hdv', input_gate * jnp.exp(final - cumulative), values, precision=highest_precision)
    return (carried, output)

def reference(tokens, norm_gain, w_query, w_forget, w_input, w_outgate, w_conv_value, w_conv_gate, w_gate_rec, w_gate_conv, lower_bound, decay_shift, state_init, head_gain, conv_kernel, channel_gain, channel_bias, w_out_rec, w_out_conv):
    normed = normalize_rows(tokens, norm_gain)

    def project(weight):
        return jnp.dot(normed, weight, preferred_element_type=jnp.float32).astype(jnp.bfloat16)
    query_raw = project(w_query)
    forget_raw = project(w_forget)
    input_raw = project(w_input)
    outgate_raw = project(w_outgate)
    value_raw = project(w_conv_value)
    gate_raw = project(w_conv_gate)
    gate_rec_raw = project(w_gate_rec)
    gate_conv_raw = project(w_gate_conv)
    query = jax.nn.silu(query_raw.astype(jnp.float32))
    input_gate = (1.0 - lower_bound) * jax.nn.sigmoid(-forget_raw.astype(jnp.float32))
    log_decay = jnp.log1p(-input_gate) + decay_shift
    values = input_raw.astype(jnp.float32)
    block_count = TOKENS // BLOCK

    def to_blocks(array):
        return array.reshape(block_count, BLOCK, HEADS, HEAD).transpose(0, 2, 1, 3)
    unused_state, blocks_out = lax.scan(block_step, state_init, (to_blocks(query), to_blocks(input_gate), to_blocks(values), to_blocks(log_decay)))
    head_out = blocks_out.transpose(0, 2, 1, 3).reshape(TOKENS, HEADS, HEAD)
    head_out = head_out * lax.rsqrt(lax.optimization_barrier(jnp.mean(head_out * head_out, axis=-1, keepdims=True)) + EPSILON)
    head_out = head_out * head_gain.reshape(HEADS, HEAD)
    mixed_rec = (head_out.reshape(TOKENS, HEADS * HEAD) * jax.nn.silu(outgate_raw.astype(jnp.float32))).astype(jnp.bfloat16)
    gated = (value_raw.astype(jnp.float32) * jax.nn.sigmoid(gate_raw.astype(jnp.float32))).astype(jnp.bfloat16)
    extended = jnp.concatenate([jnp.zeros((KW - 1, CONV), jnp.bfloat16), gated], axis=0).astype(jnp.float32)
    conv_out = jnp.zeros((TOKENS, CONV), jnp.float32)
    for tap_index in range(KW):
        conv_out = conv_out + conv_kernel[tap_index] * extended[tap_index:tap_index + TOKENS]
    scale = lax.rsqrt(lax.optimization_barrier(jnp.mean(conv_out * conv_out, axis=1, keepdims=True)) + EPSILON)
    mixed_conv = jax.nn.silu(conv_out * scale * channel_gain + channel_bias).astype(jnp.bfloat16)
    y_rec = jnp.dot(mixed_rec, w_out_rec, preferred_element_type=jnp.float32).astype(jnp.bfloat16)
    y_conv = jnp.dot(mixed_conv, w_out_conv, preferred_element_type=jnp.float32).astype(jnp.bfloat16)
    merged = jax.nn.sigmoid(gate_rec_raw.astype(jnp.float32)) * y_rec.astype(jnp.float32)
    merged = merged + jax.nn.sigmoid(gate_conv_raw.astype(jnp.float32)) * y_conv.astype(jnp.float32)
    return merged.astype(jnp.bfloat16)
```

```python
import functools

import jax
import jax.numpy as jnp
from jax import lax
from jax.experimental import pallas as pl
from jax.experimental.pallas import tpu as pltpu
from jax.sharding import PartitionSpec as P

MESH = pl.DeviceIdType.MESH
F32 = jnp.float32
BF16 = jnp.bfloat16
HEAD = 128
CONV = 1024
KW = 31
EPS = 1e-06
L = 64
T = 768
NC = T // L
TD = 96
RT = 256
HALO = 32


class Wires:
    def __init__(self, send_sem, recv_sem):
        self.send_sem, self.recv_sem = send_sem, recv_sem
        self.count = 0
        self.sent = []

    def new(self):
        self.count += 1
        return self.count - 1

    def make(self, k, src, dst, dev):
        return pltpu.make_async_remote_copy(
            src_ref=src,
            dst_ref=dst,
            send_sem=self.send_sem.at[k],
            recv_sem=self.recv_sem.at[k],
            device_id=dev,
            device_id_type=MESH,
        )

    def start(self, k, src, dst, dev):
        copy = self.make(k, src, dst, dev)
        copy.start()
        self.sent.append(copy)

    def arrive(self, k, dst, dev):
        self.make(k, dst, dst, dev).wait_recv()


class Ring:
    def __init__(self, wires, pos, plus, minus, part, mate=None):
        self.w, self.pos, self.plus, self.minus = wires, pos, plus, minus
        self.part, self.mate = part, mate
        self.k = {n: wires.new() for n in ("L0", "L1", "R0", "R1", "F0", "F1")}
        names = ("O0", "O1", "L0", "L1", "R0", "R1", "F0", "F1")
        if mate is not None:
            self.m = {n: wires.new() for n in names}
        self.at = {
            "O": pos,
            "L": lax.rem(pos + 3, 4),
            "R": lax.rem(pos + 1, 4),
            "F": lax.rem(pos + 2, 4),
        }

    def ref(self, name):
        return self.part(self.at[name[0]], int(name[1]))

    def to_mate(self, *names):
        if self.mate is not None:
            for n in names:
                self.w.start(self.m[n], self.ref(n), self.ref(n), self.mate[0])

    def start(self):
        for n, h, dev in (
            ("L0", 0, self.plus),
            ("R1", 1, self.minus),
            ("L1", 1, self.plus),
            ("R0", 0, self.minus),
        ):
            mine = self.part(self.pos, h)
            self.w.start(self.k[n], mine, mine, dev)
        self.to_mate("O0", "O1")

    def take(self, name):
        self.w.arrive(self.k[name], self.ref(name), self.minus if name[0] == "L" else self.plus)

    def relay(self):
        self.take("L0")
        self.w.start(self.k["F0"], self.ref("L0"), self.ref("L0"), self.plus)
        self.take("R1")
        self.w.start(self.k["F1"], self.ref("R1"), self.ref("R1"), self.minus)
        self.to_mate("L0", "R1")

    def near(self):
        self.take("L1")
        self.take("R0")
        self.to_mate("L1", "R0")

    def far(self):
        self.w.arrive(self.k["F0"], self.ref("F0"), self.minus)
        self.w.arrive(self.k["F1"], self.ref("F1"), self.plus)
        self.to_mate("F0", "F1")

    def from_mate(self):
        for n in ("O0", "O1", "L0", "R1", "L1", "R0", "F0", "F1"):
            other = self.mate[1](self.at[n[0]], int(n[1]))
            self.w.arrive(self.m[n], other, self.mate[0])


def dot(a, b):
    return jnp.dot(a, b, preferred_element_type=F32)


def dot_last(a, b):
    return lax.dot_general(a, b, (((1,), (1,)), ((), ())), preferred_element_type=F32)


def dot_first(a, b):
    return lax.dot_general(a, b, (((0,), (0,)), ((), ())), preferred_element_type=F32)


def rounded(v):
    return v.astype(BF16).astype(F32)


def two(v):
    high = v.astype(BF16)
    return high, (v - high.astype(F32)).astype(BF16)


def kernel(
    tokens, gain, w_f, w_i, w_q, w_o, w_v, w_g, w_gr, w_gc, lb, shift, sinit, hgain, ck, cgain, cbias, w_or, w_oc,
    out,
    tok, gainv, xs, wb, stage, lbv, shv, siv, hgv, ckv, cgv, cbv,
    kgb, cb, vb, qb, ogb, ext, hsend, hrecv, sgr, sgc, mc, mcn, mr, head, qd, stb, rbuf, sty, stz, outv,
    load_sem, send_sem, recv_sem,
):
    s, t = lax.axis_index("sp"), lax.axis_index("tp")
    z, y, x, c = s // 4, lax.rem(s, 4), t // 2, lax.rem(t, 2)
    w = Wires(send_sem, recv_sem)

    def at(zz, yy):
        return (lax.rem(zz + 4, 4) * 4 + lax.rem(yy + 4, 4), t)

    def across(xx):
        return (s, lax.rem(xx + 4, 4) * 2 + c)

    mate = (s, 1 - c + 2 * x)
    swap = (2 * t + lax.rem(s, 2), s // 2)
    home = s // 2 == t
    following, preceding = (lax.rem(s + 1, 16), t), (lax.rem(s + 15, 16), t)

    loads = []

    def load(src, dst):
        copy = pltpu.make_async_copy(src, dst, load_sem.at[len(loads)])
        copy.start()
        loads.append(copy)
        return copy

    first = [load(tokens, tok), load(gain, gainv)]
    own = [
        load(src, wb.at[b, z, y])
        for b, src in enumerate(
            (
                w_f, w_i, w_q, w_o, w_v, w_g,
                w_gr.at[:, pl.ds(0, 128)], w_gr.at[:, pl.ds(128, 128)],
                w_gc.at[:, pl.ds(0, 128)], w_gc.at[:, pl.ds(128, 128)],
            )
        )
    ]
    staged = [load(w_or, stage.at[0]), load(w_oc, stage.at[1])]
    rest = [
        load(a, b)
        for a, b in (
            (shift, shv), (lb, lbv), (sinit.at[0], siv), (hgain, hgv), (ck, ckv), (cgain, cgv), (cbias, cbv),
        )
    ]

    barrier = pltpu.get_barrier_semaphore()
    partners = [at(z, y + 1), at(z, y - 1), at(z, y + 2), at(z + 1, y), at(z - 1, y), at(z + 2, y)]
    partners += [across(x + 1), across(x - 1), mate, following, preceding]
    for dev in partners:
        pl.semaphore_signal(barrier, inc=1, device_id=dev, device_id_type=MESH)

    @pl.when(jnp.logical_not(home))
    def _():
        pl.semaphore_signal(barrier, inc=1, device_id=swap, device_id_type=MESH)

    for copy in first:
        copy.wait()
    base = pl.multiple_of(t * TD, 16)

    def normalize(r, _):
        wide = tok[pl.ds(pl.multiple_of(r * 16, 16), 16), :].astype(F32)
        scale = lax.rsqrt(jnp.mean(wide * wide, axis=-1, keepdims=True) + EPS)
        xs[pl.ds(pl.multiple_of(base + r * 16, 16), 16), :] = (wide * scale * gainv[...]).astype(BF16)
        return 0

    lax.fori_loop(0, TD // 16, normalize, 0)
    for copy in own + staged:
        copy.wait()
    pl.semaphore_wait(barrier, len(partners) + jnp.where(home, 0, 1))

    def row_part(core):
        return lambda xx, h: xs.at[pl.ds(pl.multiple_of((xx * 2 + core) * TD + h * (TD // 2), 16), TD // 2), :]

    def half_of(buf, core):
        return lambda xx, h: buf.at[xx * 2 + core, pl.ds(384 * h, 384 if h == 0 else buf.shape[1] - 384)]

    def tp_ring(part_of):
        return Ring(w, x, across(x + 1), across(x - 1), part_of(c), (mate, part_of(1 - c)))

    token_ring = tp_ring(row_part)
    conv_ring = tp_ring(lambda core: half_of(mc, core))
    rec_ring = tp_ring(lambda core: half_of(mr, core))

    def along_y(part):
        return Ring(w, y, at(z, y + 1), at(z, y - 1), part)

    def along_z(part):
        return Ring(w, z, at(z + 1, y), at(z - 1, y), part)

    p1, p2 = [], []
    for b in range(12):
        if b % 2 == 0:
            p1.append(along_y(lambda p, h, b=b: wb.at[b, z, p, pl.ds(64 * h, 64)]))
            p2.append(along_z(lambda p, h, b=b: wb.at[b, p, pl.ds(2 * h, 2)]))
        else:
            p1.append(along_z(lambda p, h, b=b: wb.at[b, p, y, pl.ds(64 * h, 64)]))
            p2.append(along_y(lambda p, h, b=b: wb.at[b, pl.ds(2 * h, 2), p]))

    def each(rings, group, *steps):
        for step in steps:
            for b in (2 * group, 2 * group + 1):
                getattr(rings[b], step)()

    token_ring.start()
    each(p1, 0, "start")
    each(p1, 1, "start")
    swap_k = [w.new(), w.new()]

    @pl.when(jnp.logical_not(home))
    def _():
        for i in range(2):
            w.make(swap_k[i], stage.at[i], wb.at[10 + i, swap[0] // 4, lax.rem(swap[0], 4)], swap).start()

    @pl.when(home)
    def _():
        for i in range(2):
            pltpu.make_async_copy(stage.at[i], wb.at[10 + i, z, y], recv_sem.at[swap_k[i]]).start()

    each(p1, 0, "relay")
    each(p1, 1, "relay")
    each(p1, 2, "start")
    each(p1, 0, "near", "far")
    each(p2, 0, "start")
    each(p1, 2, "relay")
    each(p1, 3, "start")
    each(p1, 4, "start")
    each(p1, 1, "near", "far")
    token_ring.relay()
    each(p1, 3, "relay")
    each(p1, 4, "relay")
    each(p1, 2, "near", "far")
    each(p2, 0, "relay")
    each(p2, 1, "start")

    @pl.when(jnp.logical_not(home))
    def _():
        for i in range(2):
            w.make(swap_k[i], stage.at[i], wb.at[10 + i, z, y], swap).wait()

    @pl.when(home)
    def _():
        for i in range(2):
            pltpu.make_async_copy(stage.at[i], wb.at[10 + i, z, y], recv_sem.at[swap_k[i]]).wait()

    each(p1, 5, "start")
    token_ring.near()
    each(p1, 3, "near", "far")
    each(p1, 4, "near", "far")
    each(p1, 5, "relay")
    for copy in rest:
        copy.wait()
    each(p2, 0, "near", "far")
    each(p2, 1, "relay")
    each(p2, 2, "start")
    token_ring.far()
    token_ring.from_mate()
    each(p1, 5, "near", "far")

    def whole(b):
        return wb[b].reshape(2048, 128)

    def project(group, finish):
        weight = jnp.concatenate([whole(2 * group), whole(2 * group + 1)], axis=1)

        def tile(r, _):
            rows = pl.ds(pl.multiple_of(r * RT, RT), RT)
            finish(r, rows, dot(xs[rows, :], weight))
            return 0

        lax.fori_loop(0, T // RT, tile, 0)

    def finish_fi(r, rows, v):
        gate = (1.0 - lbv[...]) * jax.nn.sigmoid(-rounded(v[:, :128]))
        kgb[rows, :] = gate
        cb[rows, :] = jnp.log1p(-gate) + shv[rows, :]
        vb[rows, :] = v[:, 128:].astype(BF16)

    project(0, finish_fi)

    at_or_after = lax.broadcasted_iota(jnp.int32, (L, L), 0) >= lax.broadcasted_iota(jnp.int32, (L, L), 1)
    ones_below = jnp.where(at_or_after, 1.0, 0.0).astype(F32)
    state = jnp.zeros((HEAD, HEAD), F32)
    before = jnp.zeros((1, HEAD), F32)
    for i in range(NC):
        rows = pl.ds(i * L, L)
        total = jnp.dot(ones_below, cb[rows, :], precision=lax.Precision.HIGHEST, preferred_element_type=F32)
        cb[rows, :] = total
        last = total[L - 1 : L, :]
        ending = (kgb[rows, :] * jnp.exp(last - total)).astype(BF16)
        stb[i] = state.astype(BF16)
        rbuf[pl.ds(i, 1), :] = before
        state = jnp.exp(last) * state + dot_first(vb[rows, :], ending)
        before = before + last
    decay = jnp.exp(before)
    sty[y, pl.ds(0, HEAD), :] = state.astype(BF16)
    extra = jnp.concatenate([a.astype(F32) for a in two(decay)] + [jnp.zeros((14, HEAD), F32)], axis=0)
    sty[y, pl.ds(HEAD, 16), :] = extra.astype(BF16)
    y_k = [w.new() for _ in range(3)]
    z_k = [w.new() for _ in range(3)]
    for i in range(3):
        w.start(y_k[i], sty.at[y], sty.at[y], at(z, y + 1 + i))

    each(p2, 1, "near", "far")
    each(p2, 2, "relay")
    each(p2, 3, "start")

    def finish_qo(r, rows, v):
        raw = rounded(v[:, :128])
        qb[rows, :] = raw * jax.nn.sigmoid(raw)
        raw = rounded(v[:, 128:])
        ogb[rows, :] = raw * jax.nn.sigmoid(raw)

    project(1, finish_qo)

    def block_of(buf, i):
        both = buf[i, pl.ds(HEAD, 16), :].astype(F32)
        return both[0:1, :] + both[1:2, :], buf[i, pl.ds(0, HEAD), :].astype(F32)

    for i in range(3):
        w.arrive(y_k[i], sty.at[lax.rem(y + 3 - i, 4)], at(z, y + 1 + i))
    row_decay, row_state = jnp.ones((1, HEAD), F32), jnp.zeros((HEAD, HEAD), F32)
    my_decay, my_state = row_decay, row_state
    for i in range(4):
        d, v = block_of(sty, i)
        row_decay, row_state = row_decay * d, d * row_state + v
        if i < 3:
            take = i < y
            my_decay = jnp.where(take, row_decay, my_decay)
            my_state = jnp.where(take, row_state, my_state)
    stz[z, pl.ds(0, HEAD), :] = row_state.astype(BF16)
    extra = jnp.concatenate([a.astype(F32) for a in two(row_decay)] + [jnp.zeros((14, HEAD), F32)], axis=0)
    stz[z, pl.ds(HEAD, 16), :] = extra.astype(BF16)
    for i in range(3):
        w.start(z_k[i], stz.at[z], stz.at[z], at(z + 1 + i, y))

    for i in range(NC):
        rows = pl.ds(i * L, L)
        total, q = cb[rows, :], qb[rows, :]
        middle = 0.5 * total[L - 1 : L, :]
        left = (q * jnp.exp(total - middle)).astype(BF16)
        right = (kgb[rows, :] * jnp.exp(middle - total)).astype(BF16)
        scores = jnp.where(at_or_after, dot_last(left, right), 0.0).astype(BF16)
        o = dot(scores, vb[rows, :])
        o = o + dot_last((q * jnp.exp(total)).astype(BF16), stb[i])
        head[rows, :] = o
        qd[rows, :] = (q * jnp.exp(total + rbuf[pl.ds(i, 1), :])).astype(BF16)

    each(p2, 2, "near", "far")
    each(p2, 3, "relay")
    each(p2, 4, "start")

    def finish_vg(r, rows, v):
        gated = (rounded(v[:, :128]) * jax.nn.sigmoid(rounded(v[:, 128:]))).astype(BF16)
        ext[pl.ds(pl.multiple_of(r * RT + HALO, 8), RT), :] = gated.astype(F32)

    project(2, finish_vg)
    hsend[...] = ext[pl.ds(T, HALO), :].astype(BF16)
    h_k = w.new()
    w.start(h_k, hsend, hrecv, following)

    for i in range(3):
        w.arrive(z_k[i], stz.at[lax.rem(z + 3 - i, 4)], at(z + 1 + i, y))
    entering = siv[...].T
    for i in range(3):
        d, v = block_of(stz, i)
        entering = jnp.where(i < z, d * entering + v, entering)
    entering = (my_decay * entering + my_state).astype(BF16)

    def finish_head(r, _):
        rows = pl.ds(pl.multiple_of(r * RT, RT), RT)
        h = head[rows, :] + dot_last(qd[rows, :], entering)
        h = h * lax.rsqrt(jnp.mean(h * h, axis=-1, keepdims=True) + EPS) * hgv[...]
        mr[t, rows, :] = (h * ogb[rows, :]).astype(BF16)
        return 0

    lax.fori_loop(0, T // RT, finish_head, 0)
    rec_ring.start()
    each(p2, 3, "near", "far")
    each(p2, 4, "relay")
    each(p2, 5, "start")

    w.arrive(h_k, hrecv, preceding)
    ext[pl.ds(0, HALO), :] = jnp.where(s > 0, hrecv[...].astype(F32), 0.0)
    for i in range(T // 128):
        acc = jnp.zeros((128, HEAD), F32)
        for j in range(KW):
            acc = acc + ckv[pl.ds(j, 1), :] * ext[pl.ds(i * 128 + HALO - KW + 1 + j, 128), :]
        mc[t, pl.ds(i * 128, 128), :] = acc.astype(BF16)
    extra = [a.astype(F32) for v in (cgv[...], cbv[...]) for a in two(v)]
    mc[t, pl.ds(T, 16), :] = jnp.concatenate(extra + [jnp.zeros((12, HEAD), F32)], axis=0).astype(BF16)
    rec_ring.relay()
    conv_ring.start()

    def finish_gate(buf):
        def finish(r, rows, v):
            buf[rows, :] = jax.nn.sigmoid(rounded(v))

        return finish

    project(3, finish_gate(sgr))
    rec_ring.near()
    each(p2, 4, "near", "far")
    each(p2, 5, "relay")
    project(4, finish_gate(sgc))
    rec_ring.far()
    conv_ring.relay()
    each(p2, 5, "near", "far")
    rec_ring.from_mate()
    conv_ring.near()
    conv_ring.far()
    conv_ring.from_mate()

    gains, biases = [], []
    for k in range(8):
        four = mc[k, pl.ds(T, 16), :].astype(F32)
        gains.append(four[0:1, :] + four[1:2, :])
        biases.append(four[2:3, :] + four[3:4, :])

    def normalize_conv(r, _):
        rows = pl.ds(pl.multiple_of(r * 32, 32), 32)
        blocks = [mc[k, rows, :].astype(F32) for k in range(8)]
        squares = sum(v * v for v in blocks)
        scale = lax.rsqrt(jnp.sum(squares, axis=-1, keepdims=True) / CONV + EPS)
        for k in range(8):
            v = blocks[k] * scale * gains[k] + biases[k]
            mcn[rows, pl.ds(k * 128, 128)] = (v * jax.nn.sigmoid(v)).astype(BF16)
        return 0

    lax.fori_loop(0, T // 32, normalize_conv, 0)

    def out_weight(b):
        sides = [
            jnp.concatenate([wb[b, k // 2, (k % 2) * 2 + j] for k in range(8)], axis=0) for j in range(2)
        ]
        return jnp.concatenate(sides, axis=1)

    w_rec, w_conv = out_weight(10), out_weight(11)

    def last_tile(r, _):
        rows = pl.ds(pl.multiple_of(r * RT, RT), RT)
        mixed = jnp.concatenate([mr[k, rows, :] for k in range(8)], axis=1)
        merged = sgr[rows, :] * rounded(dot(mixed, w_rec))
        merged = merged + sgc[rows, :] * rounded(dot(mcn[rows, :], w_conv))
        outv[rows, :] = merged.astype(BF16)
        return 0

    lax.fori_loop(0, T // RT, last_tile, 0)
    done = pltpu.make_async_copy(outv, out, load_sem.at[0])
    done.start()
    for copy in w.sent:
        copy.wait_send()
    done.wait()


def local(
    tokens, norm_gain, w_query, w_forget, w_input, w_outgate, w_conv_value, w_conv_gate, w_gate_rec, w_gate_conv,
    lower_bound, decay_shift, state_init, head_gain, conv_kernel, channel_gain, channel_bias, w_out_rec, w_out_conv,
):
    line = lambda v: v.reshape(1, -1)
    args = (
        tokens, line(norm_gain), w_forget, w_input, w_query, w_outgate, w_conv_value, w_conv_gate, w_gate_rec,
        w_gate_conv, line(lower_bound), decay_shift, state_init, line(head_gain), conv_kernel, line(channel_gain),
        line(channel_bias), w_out_rec, w_out_conv,
    )
    v = pltpu.VMEM
    scratch = [
        v((TD, 2048), BF16), v((1, 2048), F32), v((T, 2048), BF16), v((12, 4, 4, 128, 128), BF16),
        v((2, 128, 128), BF16), v((1, 128), F32), v((T, 128), F32), v((128, 128), F32), v((1, 128), F32),
        v((KW, 128), F32), v((1, 128), F32), v((1, 128), F32),
        v((T, 128), F32), v((T, 128), F32), v((T, 128), BF16), v((T, 128), F32), v((T, 128), F32),
        v((T + HALO, 128), F32), v((HALO, 128), BF16), v((HALO, 128), BF16), v((T, 256), F32), v((T, 256), F32),
        v((8, T + 16, 128), BF16), v((T, CONV), BF16), v((8, T, 128), BF16), v((T, 128), F32), v((T, 128), BF16),
        v((NC, 128, 128), BF16), v((16, 128), F32), v((4, 144, 128), BF16), v((4, 144, 128), BF16), v((T, 256), BF16),
        pltpu.SemaphoreType.DMA((24,)), pltpu.SemaphoreType.DMA((200,)), pltpu.SemaphoreType.DMA((200,)),
    ]
    return pl.pallas_call(
        kernel,
        out_shape=jax.ShapeDtypeStruct((T, 256), BF16),
        in_specs=[pl.BlockSpec(memory_space=pl.ANY)] * len(args),
        out_specs=pl.BlockSpec(memory_space=pl.ANY),
        scratch_shapes=scratch,
        compiler_params=pltpu.CompilerParams(
            collective_id=0, has_side_effects=True, vmem_limit_bytes=56 * 1024 * 1024
        ),
    )(*args)


def solution(mesh):
    both = P("sp", "tp")
    in_specs = (
        P(("sp", "tp"), None), P(), both, both, both, both, both, both, both, both, P("tp"), both,
        P("tp", None, None), P("tp"), P(None, "tp"), P("tp"), P("tp"), P("tp", "sp"), P("tp", "sp"),
    )
    return jax.shard_map(local, mesh=mesh, in_specs=in_specs, out_specs=both, check_vma=False)
```

```python
import functools

import jax
import jax.numpy as jnp
from jax import lax
from jax.experimental import pallas as pl
from jax.experimental.pallas import tpu as pltpu
from jax.sharding import PartitionSpec as P

MESH = pl.DeviceIdType.MESH
F32 = jnp.float32
BF16 = jnp.bfloat16
HEAD = 128
CONV = 1024
KW = 31
EPS = 1e-06
L = 64
T = 768
NC = T // L
TD = 96
RT = 256
HALO = 32


class Wires:
    def __init__(self, send_sem, recv_sem):
        self.send_sem, self.recv_sem = send_sem, recv_sem
        self.count = 0
        self.sent = []

    def new(self):
        self.count += 1
        return self.count - 1

    def make(self, k, src, dst, dev):
        return pltpu.make_async_remote_copy(
            src_ref=src,
            dst_ref=dst,
            send_sem=self.send_sem.at[k],
            recv_sem=self.recv_sem.at[k],
            device_id=dev,
            device_id_type=MESH,
        )

    def start(self, k, src, dst, dev):
        copy = self.make(k, src, dst, dev)
        copy.start()
        self.sent.append(copy)

    def arrive(self, k, dst, dev):
        self.make(k, dst, dst, dev).wait_recv()


class Ring:
    def __init__(self, wires, pos, plus, minus, part, mate=None):
        self.w, self.pos, self.plus, self.minus = wires, pos, plus, minus
        self.part, self.mate = part, mate
        self.k = {n: wires.new() for n in ("L0", "L1", "R0", "R1", "F0", "F1")}
        names = ("O0", "O1", "L0", "L1", "R0", "R1", "F0", "F1")
        if mate is not None:
            self.m = {n: wires.new() for n in names}
        self.at = {
            "O": pos,
            "L": lax.rem(pos + 3, 4),
            "R": lax.rem(pos + 1, 4),
            "F": lax.rem(pos + 2, 4),
        }

    def ref(self, name):
        return self.part(self.at[name[0]], int(name[1]))

    def to_mate(self, *names):
        if self.mate is not None:
            for n in names:
                self.w.start(self.m[n], self.ref(n), self.ref(n), self.mate[0])

    def start(self):
        for n, h, dev in (
            ("L0", 0, self.plus),
            ("R1", 1, self.minus),
            ("L1", 1, self.plus),
            ("R0", 0, self.minus),
        ):
            mine = self.part(self.pos, h)
            self.w.start(self.k[n], mine, mine, dev)
        self.to_mate("O0", "O1")

    def take(self, name):
        self.w.arrive(self.k[name], self.ref(name), self.minus if name[0] == "L" else self.plus)

    def relay(self):
        self.take("L0")
        self.w.start(self.k["F0"], self.ref("L0"), self.ref("L0"), self.plus)
        self.take("R1")
        self.w.start(self.k["F1"], self.ref("R1"), self.ref("R1"), self.minus)
        self.to_mate("L0", "R1")

    def near(self):
        self.take("L1")
        self.take("R0")
        self.to_mate("L1", "R0")

    def far(self):
        self.w.arrive(self.k["F0"], self.ref("F0"), self.minus)
        self.w.arrive(self.k["F1"], self.ref("F1"), self.plus)
        self.to_mate("F0", "F1")

    def from_mate(self):
        for n in ("O0", "O1", "L0", "R1", "L1", "R0", "F0", "F1"):
            other = self.mate[1](self.at[n[0]], int(n[1]))
            self.w.arrive(self.m[n], other, self.mate[0])


def dot(a, b):
    return jnp.dot(a, b, preferred_element_type=F32)


def dot_last(a, b):
    return lax.dot_general(a, b, (((1,), (1,)), ((), ())), preferred_element_type=F32)


def dot_first(a, b):
    return lax.dot_general(a, b, (((0,), (0,)), ((), ())), preferred_element_type=F32)


def rounded(v):
    return v.astype(BF16).astype(F32)


def two(v):
    high = v.astype(BF16)
    return high, (v - high.astype(F32)).astype(BF16)


def kernel(
    tokens, gain, w_f, w_i, w_q, w_o, w_v, w_g, w_gr, w_gc, lb, shift, sinit, hgain, ck, cgain, cbias, w_or, w_oc,
    out,
    tok, gainv, xs, wb, stage, lbv, shv, siv, hgv, ckv, cgv, cbv,
    kgb, cb, vb, qb, ogb, ext, hsend, hrecv, sgr, sgc, mc, mcn, mr, head, qd, stb, rbuf, sty, stz, kv,
    load_sem, send_sem, recv_sem,
):
    s, t = lax.axis_index("sp"), lax.axis_index("tp")
    z, y, x, c = s // 4, lax.rem(s, 4), t // 2, lax.rem(t, 2)
    w = Wires(send_sem, recv_sem)

    def at(zz, yy):
        return (lax.rem(zz + 4, 4) * 4 + lax.rem(yy + 4, 4), t)

    def across(xx):
        return (s, lax.rem(xx + 4, 4) * 2 + c)

    mate = (s, 1 - c + 2 * x)
    swap = (2 * t + lax.rem(s, 2), s // 2)
    home = s // 2 == t
    following, preceding = (lax.rem(s + 1, 16), t), (lax.rem(s + 15, 16), t)

    loads = []

    def load(src, dst):
        copy = pltpu.make_async_copy(src, dst, load_sem.at[len(loads)])
        copy.start()
        loads.append(copy)
        return copy

    first = [load(tokens, tok), load(gain, gainv)]
    own = [
        load(src, wb.at[b, z, y])
        for b, src in enumerate(
            (
                w_f, w_i, w_v, w_g, w_q, w_o,
                w_gr.at[:, pl.ds(0, 128)], w_gr.at[:, pl.ds(128, 128)],
                w_gc.at[:, pl.ds(0, 128)], w_gc.at[:, pl.ds(128, 128)],
            )
        )
    ]
    staged = [load(w_or, stage.at[0]), load(w_oc, stage.at[1])]
    rest = [
        load(a, b)
        for a, b in (
            (shift, shv), (lb, lbv), (sinit.at[0], siv), (hgain, hgv), (ck, ckv), (cgain, cgv), (cbias, cbv),
        )
    ]

    barrier = pltpu.get_barrier_semaphore()
    partners = [at(z, y + 1), at(z, y - 1), at(z, y + 2), at(z + 1, y), at(z - 1, y), at(z + 2, y)]
    partners += [across(x + 1), across(x - 1), mate, following, preceding]
    for dev in partners:
        pl.semaphore_signal(barrier, inc=1, device_id=dev, device_id_type=MESH)

    @pl.when(jnp.logical_not(home))
    def _():
        pl.semaphore_signal(barrier, inc=1, device_id=swap, device_id_type=MESH)

    for copy in first:
        copy.wait()
    base = pl.multiple_of(t * TD, 16)

    def normalize(r, _):
        wide = tok[pl.ds(pl.multiple_of(r * 16, 16), 16), :].astype(F32)
        scale = lax.rsqrt(jnp.mean(wide * wide, axis=-1, keepdims=True) + EPS)
        xs[pl.ds(pl.multiple_of(base + r * 16, 16), 16), :] = (wide * scale * gainv[...]).astype(BF16)
        return 0

    lax.fori_loop(0, TD // 16, normalize, 0)
    for copy in own + staged:
        copy.wait()
    pl.semaphore_wait(barrier, len(partners) + jnp.where(home, 0, 1))

    def row_part(core):
        return lambda xx, h: xs.at[pl.ds(pl.multiple_of((xx * 2 + core) * TD + h * (TD // 2), 16), TD // 2), :]

    def half_of(buf, core):
        return lambda xx, h: buf.at[xx * 2 + core, pl.ds(384 * h, 384 if h == 0 else buf.shape[1] - 384)]

    def tp_ring(part_of):
        return Ring(w, x, across(x + 1), across(x - 1), part_of(c), (mate, part_of(1 - c)))

    token_ring = tp_ring(row_part)
    conv_ring = tp_ring(lambda core: half_of(mc, core))
    rec_ring = tp_ring(lambda core: half_of(mr, core))

    def along_y(part):
        return Ring(w, y, at(z, y + 1), at(z, y - 1), part)

    def along_z(part):
        return Ring(w, z, at(z + 1, y), at(z - 1, y), part)

    p1, p2 = [], []
    for b in range(12):
        if b % 2 == 0:
            p1.append(along_y(lambda p, h, b=b: wb.at[b, z, p, pl.ds(64 * h, 64)]))
            p2.append(along_z(lambda p, h, b=b: wb.at[b, p, pl.ds(2 * h, 2)]))
        else:
            p1.append(along_z(lambda p, h, b=b: wb.at[b, p, y, pl.ds(64 * h, 64)]))
            p2.append(along_y(lambda p, h, b=b: wb.at[b, pl.ds(2 * h, 2), p]))

    def each(rings, group, *steps):
        for step in steps:
            for b in (2 * group, 2 * group + 1):
                getattr(rings[b], step)()

    token_ring.start()
    each(p1, 0, "start")
    each(p1, 1, "start")
    swap_k = [w.new(), w.new()]

    @pl.when(jnp.logical_not(home))
    def _():
        for i in range(2):
            w.make(swap_k[i], stage.at[i], wb.at[10 + i, swap[0] // 4, lax.rem(swap[0], 4)], swap).start()

    @pl.when(home)
    def _():
        for i in range(2):
            pltpu.make_async_copy(stage.at[i], wb.at[10 + i, z, y], recv_sem.at[swap_k[i]]).start()

    def swapped():
        @pl.when(jnp.logical_not(home))
        def _():
            for i in range(2):
                w.make(swap_k[i], stage.at[i], wb.at[10 + i, z, y], swap).wait()

        @pl.when(home)
        def _():
            for i in range(2):
                pltpu.make_async_copy(stage.at[i], wb.at[10 + i, z, y], recv_sem.at[swap_k[i]]).wait()

    def whole(b):
        return wb[b].reshape(2048, 128)

    def project(group, finish):
        weight = jnp.concatenate([whole(2 * group), whole(2 * group + 1)], axis=1)

        def tile(r, _):
            rows = pl.ds(pl.multiple_of(r * RT, RT), RT)
            finish(r, rows, dot(xs[rows, :], weight))
            return 0

        lax.fori_loop(0, T // RT, tile, 0)

    def finish_fi(r, rows, v):
        gate = (1.0 - lbv[...]) * jax.nn.sigmoid(-rounded(v[:, :128]))
        kgb[rows, :] = gate
        cb[rows, :] = jnp.log1p(-gate) + shv[rows, :]
        vb[rows, :] = v[:, 128:].astype(BF16)

    def finish_vg(r, rows, v):
        gated = (rounded(v[:, :128]) * jax.nn.sigmoid(rounded(v[:, 128:]))).astype(BF16)
        ext[pl.ds(pl.multiple_of(r * RT + HALO, 8), RT), :] = gated.astype(F32)

    def finish_qo(r, rows, v):
        raw = rounded(v[:, :128])
        qb[rows, :] = raw * jax.nn.sigmoid(raw)
        raw = rounded(v[:, 128:])
        ogb[rows, :] = raw * jax.nn.sigmoid(raw)

    def finish_gate(buf):
        def finish(r, rows, v):
            buf[rows, :] = jax.nn.sigmoid(rounded(v))

        return finish

    at_or_after = lax.broadcasted_iota(jnp.int32, (L, L), 0) >= lax.broadcasted_iota(jnp.int32, (L, L), 1)
    ones_below = jnp.where(at_or_after, 1.0, 0.0).astype(BF16)

    def pack_block(buf, i, decay, state):
        buf[i, pl.ds(0, HEAD), :] = state.astype(BF16)
        extra = jnp.concatenate([a.astype(F32) for a in two(decay)] + [jnp.zeros((14, HEAD), F32)], axis=0)
        buf[i, pl.ds(HEAD, 16), :] = extra.astype(BF16)

    def block_of(buf, i):
        both = buf[i, pl.ds(HEAD, 16), :].astype(F32)
        return both[0:1, :] + both[1:2, :], buf[i, pl.ds(0, HEAD), :].astype(F32)

    def local_states():
        for i in range(NC):
            rows = pl.ds(i * L, L)
            sides = dot(ones_below, jnp.concatenate(two(cb[rows, :]), axis=1))
            total = sides[:, :128] + sides[:, 128:]
            cb[rows, :] = total
            ending = (kgb[rows, :] * jnp.exp(total[L - 1 : L, :] - total)).astype(BF16)
            kv[i] = dot_first(vb[rows, :], ending)
        state = jnp.zeros((HEAD, HEAD), F32)
        before = jnp.zeros((1, HEAD), F32)
        for i in range(NC):
            last = cb[pl.ds(i * L + L - 1, 1), :]
            stb[i] = state.astype(BF16)
            rbuf[pl.ds(i, 1), :] = before
            state = jnp.exp(last) * state + kv[i]
            before = before + last
        pack_block(sty, y, jnp.exp(before), state)

    def local_outputs():
        for i in range(NC):
            rows = pl.ds(i * L, L)
            total, q = cb[rows, :], qb[rows, :]
            middle = 0.5 * total[L - 1 : L, :]
            left = (q * jnp.exp(total - middle)).astype(BF16)
            right = (kgb[rows, :] * jnp.exp(middle - total)).astype(BF16)
            scores = jnp.where(at_or_after, dot_last(left, right), 0.0).astype(BF16)
            o = dot(scores, vb[rows, :])
            o = o + dot_last((q * jnp.exp(total)).astype(BF16), stb[i])
            head[rows, :] = o
            qd[rows, :] = (q * jnp.exp(total + rbuf[pl.ds(i, 1), :])).astype(BF16)

    def convolve():
        ext[pl.ds(0, HALO), :] = jnp.where(s > 0, hrecv[...].astype(F32), 0.0)
        for i in range(T // 128):
            acc = jnp.zeros((128, HEAD), F32)
            for j in range(KW):
                acc = acc + ckv[pl.ds(j, 1), :] * ext[pl.ds(i * 128 + HALO - KW + 1 + j, 128), :]
            mc[t, pl.ds(i * 128, 128), :] = acc.astype(BF16)
        extra = [a.astype(F32) for v in (cgv[...], cbv[...]) for a in two(v)]
        mc[t, pl.ds(T, 16), :] = jnp.concatenate(extra + [jnp.zeros((12, HEAD), F32)], axis=0).astype(BF16)

    def out_weight(b):
        sides = [
            jnp.concatenate([wb[b, k // 2, (k % 2) * 2 + j] for k in range(8)], axis=0) for j in range(2)
        ]
        return jnp.concatenate(sides, axis=1)

    each(p1, 0, "relay")
    each(p1, 1, "relay")
    each(p1, 2, "start")
    each(p1, 0, "near", "far")
    each(p2, 0, "start")
    each(p1, 2, "relay")
    each(p1, 1, "near", "far")
    each(p2, 1, "start")
    token_ring.relay()
    each(p1, 3, "start")
    each(p2, 0, "relay")
    each(p1, 2, "near", "far")
    token_ring.near()
    each(p2, 1, "relay")
    each(p2, 2, "start")
    each(p1, 3, "relay")
    each(p1, 4, "start")
    for copy in rest:
        copy.wait()
    each(p2, 0, "near", "far")
    token_ring.far()
    token_ring.from_mate()
    project(0, finish_fi)
    local_states()
    y_k = [w.new() for _ in range(3)]
    z_k = [w.new() for _ in range(3)]
    for i in range(3):
        w.start(y_k[i], sty.at[y], sty.at[y], at(z, y + 1 + i))

    each(p1, 3, "near", "far")
    each(p2, 1, "near", "far")
    each(p2, 2, "relay")
    each(p2, 3, "start")
    each(p1, 4, "relay")
    project(1, finish_vg)
    hsend[...] = ext[pl.ds(T, HALO), :].astype(BF16)
    h_k = w.new()
    w.start(h_k, hsend, hrecv, following)
    each(p1, 4, "near", "far")
    swapped()
    each(p1, 5, "start")

    for i in range(3):
        w.arrive(y_k[i], sty.at[lax.rem(y + 3 - i, 4)], at(z, y + 1 + i))
    row_decay, row_state = jnp.ones((1, HEAD), F32), jnp.zeros((HEAD, HEAD), F32)
    my_decay, my_state = row_decay, row_state
    for i in range(4):
        d, v = block_of(sty, i)
        row_decay, row_state = row_decay * d, d * row_state + v
        if i < 3:
            take = i < y
            my_decay = jnp.where(take, row_decay, my_decay)
            my_state = jnp.where(take, row_state, my_state)
    pack_block(stz, z, row_decay, row_state)
    for i in range(3):
        w.start(z_k[i], stz.at[z], stz.at[z], at(z + 1 + i, y))

    w.arrive(h_k, hrecv, preceding)
    convolve()
    conv_ring.start()
    each(p2, 2, "near", "far")
    each(p2, 3, "relay")
    each(p2, 4, "start")
    each(p1, 5, "relay")
    project(2, finish_qo)
    local_outputs()
    each(p1, 5, "near", "far")

    for i in range(3):
        w.arrive(z_k[i], stz.at[lax.rem(z + 3 - i, 4)], at(z + 1 + i, y))
    entering = siv[...].T
    for i in range(3):
        d, v = block_of(stz, i)
        entering = jnp.where(i < z, d * entering + v, entering)
    entering = (my_decay * entering + my_state).astype(BF16)

    def finish_head(r, _):
        rows = pl.ds(pl.multiple_of(r * RT, RT), RT)
        h = head[rows, :] + dot_last(qd[rows, :], entering)
        h = h * lax.rsqrt(jnp.mean(h * h, axis=-1, keepdims=True) + EPS) * hgv[...]
        mr[t, rows, :] = (h * ogb[rows, :]).astype(BF16)
        return 0

    lax.fori_loop(0, T // RT, finish_head, 0)
    conv_ring.relay()
    rec_ring.start()
    each(p2, 3, "near", "far")
    each(p2, 4, "relay")
    each(p2, 5, "start")
    project(3, finish_gate(sgr))
    conv_ring.near()
    each(p2, 4, "near", "far")
    each(p2, 5, "relay")
    rec_ring.relay()
    project(4, finish_gate(sgc))
    conv_ring.far()
    conv_ring.from_mate()
    rec_ring.near()

    gains, biases = [], []
    for k in range(8):
        four = mc[k, pl.ds(T, 16), :].astype(F32)
        gains.append(0.5 * (four[0:1, :] + four[1:2, :]))
        biases.append(0.5 * (four[2:3, :] + four[3:4, :]))

    def normalize_conv(r, _):
        rows = pl.ds(pl.multiple_of(r * 32, 32), 32)
        blocks = [mc[k, rows, :].astype(F32) for k in range(8)]
        squares = sum(v * v for v in blocks)
        scale = lax.rsqrt(jnp.sum(squares, axis=-1, keepdims=True) * (1.0 / CONV) + EPS)
        for k in range(8):
            half = blocks[k] * scale * gains[k] + biases[k]
            mcn[rows, pl.ds(k * 128, 128)] = (half + half * jnp.tanh(half)).astype(BF16)
        return 0

    lax.fori_loop(0, T // 32, normalize_conv, 0)
    each(p2, 5, "near", "far")
    w_rec, w_conv = out_weight(10), out_weight(11)

    def conv_tile(r, _):
        rows = pl.ds(pl.multiple_of(r * RT, RT), RT)
        sgc[rows, :] = sgc[rows, :] * rounded(dot(mcn[rows, :], w_conv))
        return 0

    lax.fori_loop(0, T // RT, conv_tile, 0)
    rec_ring.far()
    rec_ring.from_mate()

    def last_tile(r, _):
        rows = pl.ds(pl.multiple_of(r * RT, RT), RT)
        mixed = jnp.concatenate([mr[k, rows, :] for k in range(8)], axis=1)
        out[rows, :] = (sgr[rows, :] * rounded(dot(mixed, w_rec)) + sgc[rows, :]).astype(BF16)
        return 0

    lax.fori_loop(0, T // RT, last_tile, 0)
    for copy in w.sent:
        copy.wait_send()


def local(
    tokens, norm_gain, w_query, w_forget, w_input, w_outgate, w_conv_value, w_conv_gate, w_gate_rec, w_gate_conv,
    lower_bound, decay_shift, state_init, head_gain, conv_kernel, channel_gain, channel_bias, w_out_rec, w_out_conv,
):
    line = lambda v: v.reshape(1, -1)
    args = (
        tokens, line(norm_gain), w_forget, w_input, w_query, w_outgate, w_conv_value, w_conv_gate, w_gate_rec,
        w_gate_conv, line(lower_bound), decay_shift, state_init, line(head_gain), conv_kernel, line(channel_gain),
        line(channel_bias), w_out_rec, w_out_conv,
    )
    v = pltpu.VMEM
    scratch = [
        v((TD, 2048), BF16), v((1, 2048), F32), v((T, 2048), BF16), v((12, 4, 4, 128, 128), BF16),
        v((2, 128, 128), BF16), v((1, 128), F32), v((T, 128), F32), v((128, 128), F32), v((1, 128), F32),
        v((KW, 128), F32), v((1, 128), F32), v((1, 128), F32),
        v((T, 128), F32), v((T, 128), F32), v((T, 128), BF16), v((T, 128), F32), v((T, 128), F32),
        v((T + HALO, 128), F32), v((HALO, 128), BF16), v((HALO, 128), BF16), v((T, 256), F32), v((T, 256), F32),
        v((8, T + 16, 128), BF16), v((T, CONV), BF16), v((8, T, 128), BF16), v((T, 128), F32), v((T, 128), BF16),
        v((NC, 128, 128), BF16), v((16, 128), F32), v((4, 144, 128), BF16), v((4, 144, 128), BF16), v((NC, 128, 128), F32),
        pltpu.SemaphoreType.DMA((24,)), pltpu.SemaphoreType.DMA((200,)), pltpu.SemaphoreType.DMA((200,)),
    ]
    return pl.pallas_call(
        kernel,
        out_shape=jax.ShapeDtypeStruct((T, 256), BF16),
        in_specs=[pl.BlockSpec(memory_space=pl.ANY)] * len(args),
        out_specs=pl.BlockSpec(memory_space=pltpu.VMEM),
        scratch_shapes=scratch,
        compiler_params=pltpu.CompilerParams(
            collective_id=0, has_side_effects=True, vmem_limit_bytes=56 * 1024 * 1024
        ),
    )(*args)


def solution(mesh):
    both = P("sp", "tp")
    in_specs = (
        P(("sp", "tp"), None), P(), both, both, both, both, both, both, both, both, P("tp"), both,
        P("tp", None, None), P("tp"), P(None, "tp"), P("tp"), P("tp"), P("tp", "sp"), P("tp", "sp"),
    )
    return jax.shard_map(local, mesh=mesh, in_specs=in_specs, out_specs=both, check_vma=False)
```

```python
import functools

import jax
import jax.numpy as jnp
from jax import lax
from jax.experimental import pallas as pl
from jax.experimental.pallas import tpu as pltpu
from jax.sharding import PartitionSpec as P

MESH = pl.DeviceIdType.MESH
F32 = jnp.float32
BF16 = jnp.bfloat16
HEAD = 128
CONV = 1024
KW = 31
EPS = 1e-06
L = 64
T = 768
NC = T // L
TD = 96
RT = 256
XT = 192
PT = 384
HALO = 32


class Wires:
    def __init__(self, send_sem, recv_sem):
        self.send_sem, self.recv_sem = send_sem, recv_sem
        self.count = 0
        self.sent = []

    def new(self):
        self.count += 1
        return self.count - 1

    def make(self, k, src, dst, dev):
        return pltpu.make_async_remote_copy(
            src_ref=src,
            dst_ref=dst,
            send_sem=self.send_sem.at[k],
            recv_sem=self.recv_sem.at[k],
            device_id=dev,
            device_id_type=MESH,
        )

    def start(self, k, src, dst, dev):
        copy = self.make(k, src, dst, dev)
        copy.start()
        self.sent.append(copy)

    def arrive(self, k, dst, dev):
        self.make(k, dst, dst, dev).wait_recv()


class Ring:
    def __init__(self, wires, pos, plus, minus, part, mate=None):
        self.w, self.pos, self.plus, self.minus = wires, pos, plus, minus
        self.part, self.mate = part, mate
        self.k = {n: wires.new() for n in ("L0", "L1", "R0", "R1", "F0", "F1")}
        names = ("O0", "O1", "L0", "L1", "R0", "R1", "F0", "F1")
        if mate is not None:
            self.m = {n: wires.new() for n in names}
        self.at = {
            "O": pos,
            "L": lax.rem(pos + 3, 4),
            "R": lax.rem(pos + 1, 4),
            "F": lax.rem(pos + 2, 4),
        }

    def ref(self, name):
        return self.part(self.at[name[0]], int(name[1]))

    def to_mate(self, *names):
        if self.mate is not None:
            for n in names:
                self.w.start(self.m[n], self.ref(n), self.ref(n), self.mate[0])

    def start(self):
        for n, h, dev in (
            ("L0", 0, self.plus),
            ("R1", 1, self.minus),
            ("L1", 1, self.plus),
            ("R0", 0, self.minus),
        ):
            mine = self.part(self.pos, h)
            self.w.start(self.k[n], mine, mine, dev)
        self.to_mate("O0", "O1")

    def take(self, name):
        self.w.arrive(self.k[name], self.ref(name), self.minus if name[0] == "L" else self.plus)

    def relay(self):
        self.take("L0")
        self.w.start(self.k["F0"], self.ref("L0"), self.ref("L0"), self.plus)
        self.take("R1")
        self.w.start(self.k["F1"], self.ref("R1"), self.ref("R1"), self.minus)
        self.to_mate("L0", "R1")

    def near(self):
        self.take("L1")
        self.take("R0")
        self.to_mate("L1", "R0")

    def far(self):
        self.w.arrive(self.k["F0"], self.ref("F0"), self.minus)
        self.w.arrive(self.k["F1"], self.ref("F1"), self.plus)
        self.to_mate("F0", "F1")

    def mate_near(self):
        self.from_mate("O0", "O1", "L0", "R1", "L1", "R0")

    def mate_far(self):
        self.from_mate("F0", "F1")

    def from_mate(self, *names):
        for n in names:
            other = self.mate[1](self.at[n[0]], int(n[1]))
            self.w.arrive(self.m[n], other, self.mate[0])


def dot(a, b):
    return jnp.dot(a, b, preferred_element_type=F32)


def dot_last(a, b):
    return lax.dot_general(a, b, (((1,), (1,)), ((), ())), preferred_element_type=F32)


def dot_first(a, b):
    return lax.dot_general(a, b, (((0,), (0,)), ((), ())), preferred_element_type=F32)


def rounded(v):
    return v.astype(BF16).astype(F32)


def two(v):
    high = v.astype(BF16)
    return high, (v - high.astype(F32)).astype(BF16)


def kernel(
    tokens, gain, w_f, w_i, w_q, w_o, w_v, w_g, w_gr, w_gc, lb, shift, sinit, hgain, ck, cgain, cbias, w_or, w_oc,
    out,
    tok, gainv, xs, wb, stage, lbv, shv, siv, hgv, ckv, cgv, cbv,
    kgb, cb, vb, qb, ogb, ext, hsend, hrecv, sgr, sgc, mc, mcn, mr, head, qd, stb, rbuf, sty, stz, kv, scales,
    load_sem, send_sem, recv_sem,
):
    s, t = lax.axis_index("sp"), lax.axis_index("tp")
    z, y, x, c = s // 4, lax.rem(s, 4), t // 2, lax.rem(t, 2)
    w = Wires(send_sem, recv_sem)

    def at(zz, yy):
        return (lax.rem(zz + 4, 4) * 4 + lax.rem(yy + 4, 4), t)

    def across(xx):
        return (s, lax.rem(xx + 4, 4) * 2 + c)

    mate = (s, 1 - c + 2 * x)
    swap = (2 * t + lax.rem(s, 2), s // 2)
    home = s // 2 == t
    following, preceding = (lax.rem(s + 1, 16), t), (lax.rem(s + 15, 16), t)

    loads = []

    def load(src, dst):
        copy = pltpu.make_async_copy(src, dst, load_sem.at[len(loads)])
        copy.start()
        loads.append(copy)
        return copy

    first = [load(tokens, tok), load(gain, gainv)]
    own = [
        load(src, wb.at[b, z, y])
        for b, src in enumerate(
            (
                w_v, w_g, w_f, w_i, w_q, w_o,
                w_gr.at[:, pl.ds(0, 128)], w_gr.at[:, pl.ds(128, 128)],
                w_gc.at[:, pl.ds(0, 128)], w_gc.at[:, pl.ds(128, 128)],
            )
        )
    ]
    staged = [load(w_or, stage.at[0]), load(w_oc, stage.at[1])]
    rest = [
        load(a, b)
        for a, b in (
            (shift, shv), (lb, lbv), (sinit.at[0], siv), (hgain, hgv), (ck, ckv), (cgain, cgv), (cbias, cbv),
        )
    ]

    barrier = pltpu.get_barrier_semaphore()
    partners = [at(z, y + 1), at(z, y - 1), at(z, y + 2), at(z + 1, y), at(z - 1, y), at(z + 2, y)]
    partners += [across(x + 1), across(x - 1), mate, following, preceding]
    for dev in partners:
        pl.semaphore_signal(barrier, inc=1, device_id=dev, device_id_type=MESH)

    @pl.when(jnp.logical_not(home))
    def _():
        pl.semaphore_signal(barrier, inc=1, device_id=swap, device_id_type=MESH)

    for copy in first:
        copy.wait()
    base = pl.multiple_of(t * TD, 16)

    def normalize(r, _):
        wide = tok[pl.ds(pl.multiple_of(r * 16, 16), 16), :].astype(F32)
        scale = lax.rsqrt(jnp.mean(wide * wide, axis=-1, keepdims=True) + EPS)
        xs[pl.ds(pl.multiple_of(base + r * 16, 16), 16), :] = (wide * scale * gainv[...]).astype(BF16)
        return 0

    lax.fori_loop(0, TD // 16, normalize, 0)
    for copy in own + staged:
        copy.wait()
    pl.semaphore_wait(barrier, len(partners) + jnp.where(home, 0, 1))

    def row_part(core):
        return lambda xx, h: xs.at[pl.ds(pl.multiple_of((xx * 2 + core) * TD + h * (TD // 2), 16), TD // 2), :]

    def half_of(buf, core):
        return lambda xx, h: buf.at[xx * 2 + core, pl.ds(384 * h, 384 if h == 0 else buf.shape[1] - 384)]

    def tp_ring(part_of):
        return Ring(w, x, across(x + 1), across(x - 1), part_of(c), (mate, part_of(1 - c)))

    token_ring = tp_ring(row_part)
    conv_ring = tp_ring(lambda core: half_of(mc, core))
    rec_ring = tp_ring(lambda core: half_of(mr, core))

    def along_y(part):
        return Ring(w, y, at(z, y + 1), at(z, y - 1), part)

    def along_z(part):
        return Ring(w, z, at(z + 1, y), at(z - 1, y), part)

    p1, p2 = [], []
    for b in range(12):
        if b % 2 == 0:
            p1.append(along_y(lambda p, h, b=b: wb.at[b, z, p, pl.ds(64 * h, 64)]))
            p2.append(along_z(lambda p, h, b=b: wb.at[b, p, pl.ds(2 * h, 2)]))
        else:
            p1.append(along_z(lambda p, h, b=b: wb.at[b, p, y, pl.ds(64 * h, 64)]))
            p2.append(along_y(lambda p, h, b=b: wb.at[b, pl.ds(2 * h, 2), p]))

    def each(rings, group, *steps):
        for step in steps:
            for b in (2 * group, 2 * group + 1):
                getattr(rings[b], step)()

    each(p1, 0, "start")
    each(p1, 1, "start")
    token_ring.start()
    swap_k = [w.new(), w.new()]

    @pl.when(jnp.logical_not(home))
    def _():
        for i in range(2):
            w.make(swap_k[i], stage.at[i], wb.at[10 + i, swap[0] // 4, lax.rem(swap[0], 4)], swap).start()

    @pl.when(home)
    def _():
        for i in range(2):
            pltpu.make_async_copy(stage.at[i], wb.at[10 + i, z, y], recv_sem.at[swap_k[i]]).start()

    def swapped():
        @pl.when(jnp.logical_not(home))
        def _():
            for i in range(2):
                w.make(swap_k[i], stage.at[i], wb.at[10 + i, z, y], swap).wait()

        @pl.when(home)
        def _():
            for i in range(2):
                pltpu.make_async_copy(stage.at[i], wb.at[10 + i, z, y], recv_sem.at[swap_k[i]]).wait()

    def whole(b):
        return wb[b].reshape(2048, 128)

    def project(group, finish, size, starts):
        weight = jnp.concatenate([whole(2 * group), whole(2 * group + 1)], axis=1)

        def tile(r, _):
            start = pl.multiple_of(starts(r), 32)
            rows = pl.ds(start, size)
            finish(start, rows, dot(xs[rows, :], weight))
            return 0

        return lambda low, high: lax.fori_loop(low, high, tile, 0)

    def project_all(group, finish):
        project(group, finish, PT, lambda r: r * PT)(0, T // PT)

    def by_ring(r):
        return lax.rem(x + jnp.where(r == 1, 3, jnp.where(r == 2, 1, jnp.where(r == 3, 2, 0))), 4) * XT

    def finish_fi(start, rows, v):
        gate = (1.0 - lbv[...]) * jax.nn.sigmoid(-rounded(v[:, :128]))
        kgb[rows, :] = gate
        cb[rows, :] = jnp.log1p(-gate) + shv[rows, :]
        vb[rows, :] = v[:, 128:].astype(BF16)

    def finish_vg(start, rows, v):
        gated = (rounded(v[:, :128]) * jax.nn.sigmoid(rounded(v[:, 128:]))).astype(BF16)
        ext[pl.ds(pl.multiple_of(start + HALO, 8), XT), :] = gated.astype(F32)

    def finish_qo(start, rows, v):
        raw = rounded(v[:, :128])
        qb[rows, :] = raw * jax.nn.sigmoid(raw)
        raw = rounded(v[:, 128:])
        ogb[rows, :] = raw * jax.nn.sigmoid(raw)

    def finish_gate(buf):
        def finish(start, rows, v):
            buf[rows, :] = jax.nn.sigmoid(rounded(v))

        return finish

    at_or_after = lax.broadcasted_iota(jnp.int32, (L, L), 0) >= lax.broadcasted_iota(jnp.int32, (L, L), 1)
    ones_below = jnp.where(at_or_after, 1.0, 0.0).astype(BF16)

    def pack_block(buf, i, decay, state):
        buf[i, pl.ds(0, HEAD), :] = state.astype(BF16)
        extra = jnp.concatenate([a.astype(F32) for a in two(decay)] + [jnp.zeros((14, HEAD), F32)], axis=0)
        buf[i, pl.ds(HEAD, 16), :] = extra.astype(BF16)

    def block_of(buf, i):
        both = buf[i, pl.ds(HEAD, 16), :].astype(F32)
        return both[0:1, :] + both[1:2, :], buf[i, pl.ds(0, HEAD), :].astype(F32)

    def local_states():
        for i in range(NC):
            rows = pl.ds(i * L, L)
            sides = dot(ones_below, jnp.concatenate(two(cb[rows, :]), axis=1))
            total = sides[:, :128] + sides[:, 128:]
            cb[rows, :] = total
            ending = (kgb[rows, :] * jnp.exp(total[L - 1 : L, :] - total)).astype(BF16)
            kv[i] = dot_first(vb[rows, :], ending)
        state = jnp.zeros((HEAD, HEAD), F32)
        before = jnp.zeros((1, HEAD), F32)
        for i in range(NC):
            last = cb[pl.ds(i * L + L - 1, 1), :]
            stb[i] = state.astype(BF16)
            rbuf[pl.ds(i, 1), :] = before
            state = jnp.exp(last) * state + kv[i]
            before = before + last
        pack_block(sty, y, jnp.exp(before), state)

    def local_outputs():
        for i in range(NC):
            rows = pl.ds(i * L, L)
            total, q = cb[rows, :], qb[rows, :]
            middle = 0.5 * total[L - 1 : L, :]
            left = (q * jnp.exp(total - middle)).astype(BF16)
            right = (kgb[rows, :] * jnp.exp(middle - total)).astype(BF16)
            scores = jnp.where(at_or_after, dot_last(left, right), 0.0).astype(BF16)
            o = dot(scores, vb[rows, :])
            o = o + dot_last((q * jnp.exp(total)).astype(BF16), stb[i])
            head[rows, :] = o
            qd[rows, :] = (q * jnp.exp(total + rbuf[pl.ds(i, 1), :])).astype(BF16)

    def convolve():
        ext[pl.ds(0, HALO), :] = jnp.where(s > 0, hrecv[...].astype(F32), 0.0)
        for i in range(T // 128):
            acc = jnp.zeros((128, HEAD), F32)
            for j in range(KW):
                acc = acc + ckv[pl.ds(j, 1), :] * ext[pl.ds(i * 128 + HALO - KW + 1 + j, 128), :]
            mc[t, pl.ds(i * 128, 128), :] = acc.astype(BF16)
        extra = [a.astype(F32) for v in (cgv[...], cbv[...]) for a in two(v)]
        mc[t, pl.ds(T, 16), :] = jnp.concatenate(extra + [jnp.zeros((12, HEAD), F32)], axis=0).astype(BF16)

    def out_weight(b):
        sides = [
            jnp.concatenate([wb[b, k // 2, (k % 2) * 2 + j] for k in range(8)], axis=0) for j in range(2)
        ]
        return jnp.concatenate(sides, axis=1)

    each(p1, 0, "relay")
    each(p1, 1, "relay")
    each(p1, 2, "start")
    each(p1, 0, "near", "far")
    each(p2, 0, "start")
    each(p1, 1, "near", "far")
    each(p2, 1, "start")
    each(p1, 2, "relay")
    token_ring.relay()
    each(p2, 0, "relay")
    each(p1, 2, "near", "far")
    token_ring.near()
    each(p2, 1, "relay")
    each(p2, 2, "start")
    for copy in rest:
        copy.wait()
    each(p2, 0, "near", "far")
    token_ring.mate_near()
    project_vg = project(0, finish_vg, XT, by_ring)
    project_vg(0, 3)
    each(p1, 3, "start")
    token_ring.far()
    each(p2, 2, "relay")
    each(p1, 4, "start")
    token_ring.mate_far()
    project_vg(3, 4)
    hsend[...] = ext[pl.ds(T, HALO), :].astype(BF16)
    h_k = w.new()
    w.start(h_k, hsend, hrecv, following)
    each(p2, 1, "near", "far")
    project_all(1, finish_fi)
    local_states()
    y_k = [w.new() for _ in range(3)]
    z_k = [w.new() for _ in range(3)]
    for i in range(3):
        w.start(y_k[i], sty.at[y], sty.at[y], at(z, y + 1 + i))

    each(p1, 3, "relay")
    each(p1, 4, "relay")
    w.arrive(h_k, hrecv, preceding)
    convolve()
    conv_ring.start()
    each(p1, 3, "near", "far")
    each(p2, 3, "start")
    each(p2, 2, "near", "far")
    project_all(2, finish_qo)

    for i in range(3):
        w.arrive(y_k[i], sty.at[lax.rem(y + 3 - i, 4)], at(z, y + 1 + i))
    row_decay, row_state = jnp.ones((1, HEAD), F32), jnp.zeros((HEAD, HEAD), F32)
    my_decay, my_state = row_decay, row_state
    for i in range(4):
        d, v = block_of(sty, i)
        row_decay, row_state = row_decay * d, d * row_state + v
        if i < 3:
            take = i < y
            my_decay = jnp.where(take, row_decay, my_decay)
            my_state = jnp.where(take, row_state, my_state)
    pack_block(stz, z, row_decay, row_state)
    for i in range(3):
        w.start(z_k[i], stz.at[z], stz.at[z], at(z + 1 + i, y))

    each(p1, 4, "near", "far")
    local_outputs()
    each(p2, 3, "relay")
    each(p2, 4, "start")
    swapped()
    each(p1, 5, "start")
    conv_ring.relay()

    for i in range(3):
        w.arrive(z_k[i], stz.at[lax.rem(z + 3 - i, 4)], at(z + 1 + i, y))
    entering = siv[...].T
    for i in range(3):
        d, v = block_of(stz, i)
        entering = jnp.where(i < z, d * entering + v, entering)
    entering = (my_decay * entering + my_state).astype(BF16)

    def finish_head(r, _):
        rows = pl.ds(pl.multiple_of(r * RT, RT), RT)
        h = head[rows, :] + dot_last(qd[rows, :], entering)
        h = h * lax.rsqrt(jnp.mean(h * h, axis=-1, keepdims=True) + EPS) * hgv[...]
        mr[t, rows, :] = (h * ogb[rows, :]).astype(BF16)
        return 0

    lax.fori_loop(0, T // RT, finish_head, 0)
    rec_ring.start()
    each(p1, 5, "relay")
    each(p2, 4, "relay")
    conv_ring.near()
    each(p2, 3, "near", "far")
    project_all(3, finish_gate(sgr))
    each(p1, 5, "near", "far")
    each(p2, 5, "start")
    conv_ring.far()
    rec_ring.relay()
    conv_ring.mate_near()
    conv_ring.mate_far()

    gains, biases = [], []
    for k in range(8):
        four = mc[k, pl.ds(T, 16), :].astype(F32)
        gains.append(0.5 * (four[0:1, :] + four[1:2, :]))
        biases.append(0.5 * (four[2:3, :] + four[3:4, :]))

    def conv_scale(r, _):
        rows = pl.ds(pl.multiple_of(r * 64, 64), 64)
        squares = sum(v * v for v in (mc[k, rows, :].astype(F32) for k in range(8)))
        scale = lax.rsqrt(jnp.sum(squares, axis=-1, keepdims=True) * (1.0 / CONV) + EPS)
        scales[rows, :] = jnp.broadcast_to(scale, (64, 128))
        return 0

    def normalize_conv(r, _):
        rows = pl.ds(pl.multiple_of(r * 64, 64), 64)
        scale = scales[rows, :]
        for k in range(8):
            half = mc[k, rows, :].astype(F32) * scale * gains[k] + biases[k]
            mcn[rows, pl.ds(k * 128, 128)] = (half + half * jnp.tanh(half)).astype(BF16)
        return 0

    lax.fori_loop(0, T // 64, conv_scale, 0, unroll=4)
    lax.fori_loop(0, T // 64, normalize_conv, 0, unroll=2)
    each(p2, 5, "relay")
    rec_ring.near()
    each(p2, 4, "near", "far")
    project_all(4, finish_gate(sgc))
    each(p2, 5, "near", "far")
    w_rec, w_conv = out_weight(10), out_weight(11)

    def conv_tile(r, _):
        rows = pl.ds(pl.multiple_of(r * RT, RT), RT)
        sgc[rows, :] = sgc[rows, :] * rounded(dot(mcn[rows, :], w_conv))
        return 0

    lax.fori_loop(0, T // RT, conv_tile, 0)
    rec_ring.far()
    rec_ring.mate_near()
    rec_ring.mate_far()

    def last_tile(r, _):
        rows = pl.ds(pl.multiple_of(r * RT, RT), RT)
        mixed = jnp.concatenate([mr[k, rows, :] for k in range(8)], axis=1)
        out[rows, :] = (sgr[rows, :] * rounded(dot(mixed, w_rec)) + sgc[rows, :]).astype(BF16)
        return 0

    lax.fori_loop(0, T // RT, last_tile, 0)
    for copy in w.sent:
        copy.wait_send()


def local(
    tokens, norm_gain, w_query, w_forget, w_input, w_outgate, w_conv_value, w_conv_gate, w_gate_rec, w_gate_conv,
    lower_bound, decay_shift, state_init, head_gain, conv_kernel, channel_gain, channel_bias, w_out_rec, w_out_conv,
):
    line = lambda v: v.reshape(1, -1)
    args = (
        tokens, line(norm_gain), w_forget, w_input, w_query, w_outgate, w_conv_value, w_conv_gate, w_gate_rec,
        w_gate_conv, line(lower_bound), decay_shift, state_init, line(head_gain), conv_kernel, line(channel_gain),
        line(channel_bias), w_out_rec, w_out_conv,
    )
    v = pltpu.VMEM
    scratch = [
        v((TD, 2048), BF16), v((1, 2048), F32), v((T, 2048), BF16), v((12, 4, 4, 128, 128), BF16),
        v((2, 128, 128), BF16), v((1, 128), F32), v((T, 128), F32), v((128, 128), F32), v((1, 128), F32),
        v((KW, 128), F32), v((1, 128), F32), v((1, 128), F32),
        v((T, 128), F32), v((T, 128), F32), v((T, 128), BF16), v((T, 128), F32), v((T, 128), F32),
        v((T + HALO, 128), F32), v((HALO, 128), BF16), v((HALO, 128), BF16), v((T, 256), F32), v((T, 256), F32),
        v((8, T + 16, 128), BF16), v((T, CONV), BF16), v((8, T, 128), BF16), v((T, 128), F32), v((T, 128), BF16),
        v((NC, 128, 128), BF16), v((16, 128), F32), v((4, 144, 128), BF16), v((4, 144, 128), BF16), v((NC, 128, 128), F32), v((T, 128), F32),
        pltpu.SemaphoreType.DMA((24,)), pltpu.SemaphoreType.DMA((200,)), pltpu.SemaphoreType.DMA((200,)),
    ]
    return pl.pallas_call(
        kernel,
        out_shape=jax.ShapeDtypeStruct((T, 256), BF16),
        in_specs=[pl.BlockSpec(memory_space=pltpu.HBM)] * len(args),
        out_specs=pl.BlockSpec(memory_space=pltpu.VMEM),
        scratch_shapes=scratch,
        compiler_params=pltpu.CompilerParams(
            collective_id=0, has_side_effects=True, vmem_limit_bytes=56 * 1024 * 1024
        ),
    )(*args)


def solution(mesh):
    both = P("sp", "tp")
    in_specs = (
        P(("sp", "tp"), None), P(), both, both, both, both, both, both, both, both, P("tp"), both,
        P("tp", None, None), P("tp"), P(None, "tp"), P("tp"), P("tp"), P("tp", "sp"), P("tp", "sp"),
    )
    return jax.shard_map(local, mesh=mesh, in_specs=in_specs, out_specs=both, check_vma=False)
```

```python
import functools

import jax
import jax.numpy as jnp
from jax import lax
from jax.experimental import pallas as pl
from jax.experimental.pallas import tpu as pltpu
from jax.sharding import PartitionSpec as P

MESH = pl.DeviceIdType.MESH
F32 = jnp.float32
BF16 = jnp.bfloat16
HEAD = 128
CONV = 1024
KW = 31
EPS = 1e-06
L = 64
T = 768
NC = T // L
TD = 96
RT = 256
XT = 192
PT = 384
HALO = 32


class Wires:
    def __init__(self, send_sem, recv_sem):
        self.send_sem, self.recv_sem = send_sem, recv_sem
        self.count = 0

    def new(self):
        self.count += 1
        return self.count - 1

    def make(self, lane, k, src, dst, dev):
        return pltpu.make_async_remote_copy(
            src_ref=src,
            dst_ref=dst,
            send_sem=self.send_sem.at[lane],
            recv_sem=self.recv_sem.at[k],
            device_id=dev,
            device_id_type=MESH,
        )

    def start(self, lane, k, src, dst, dev):
        self.make(lane, k, src, dst, dev).start()

    def arrive(self, k, span, dev):
        self.make(0, k, span, span, dev).wait_recv()

    def left(self, lane, span, dev):
        self.make(lane, 0, span, span, dev).wait_send()


class Exchange:
    def __init__(self, wires, lane, rings, span, mate=None):
        self.w, self.lane, self.rings, self.span, self.mate = wires, lane, rings, span, mate
        self.k = {"relay": wires.new(), "near": wires.new()}
        self.k["far"] = self.k["near"] if mate is None else wires.new()
        if mate is not None:
            self.k["mate_near"], self.k["mate_far"] = wires.new(), wires.new()

    def go(self, sem, view, dev):
        self.w.start(self.lane, self.k[sem], view, view, dev)

    def to_mate(self, sem, *views):
        if self.mate is not None:
            for view in views:
                self.go(sem, view, self.mate)

    def await_blocks(self, sem, n):
        self.w.arrive(self.k[sem], self.span(n * len(self.rings)), self.rings[0][1])

    def first(self):
        for pos, plus, minus, part in self.rings:
            self.go("relay", part(pos, 0), plus)
            self.go("relay", part(pos, 1), minus)

    def second(self):
        for pos, plus, minus, part in self.rings:
            self.go("near", part(pos, 1), plus)
            self.go("near", part(pos, 0), minus)
            self.to_mate("mate_near", part(pos, 0), part(pos, 1))

    def start(self):
        self.first()
        self.second()

    def relay(self):
        self.await_blocks("relay", 1)
        for pos, plus, minus, part in self.rings:
            left, right = part(lax.rem(pos + 3, 4), 0), part(lax.rem(pos + 1, 4), 1)
            self.go("far", left, plus)
            self.go("far", right, minus)
            self.to_mate("mate_near", left, right)

    def near(self):
        self.await_blocks("near", 1)
        for pos, plus, minus, part in self.rings:
            self.to_mate("mate_near", part(lax.rem(pos + 3, 4), 1), part(lax.rem(pos + 1, 4), 0))

    def far(self):
        self.await_blocks("far", 1)
        for pos, plus, minus, part in self.rings:
            self.to_mate("mate_far", part(lax.rem(pos + 2, 4), 0), part(lax.rem(pos + 2, 4), 1))

    def rest(self):
        self.await_blocks("near", 2)

    def mate_near(self):
        self.w.arrive(self.k["mate_near"], self.span(3), self.mate)

    def mate_far(self):
        self.w.arrive(self.k["mate_far"], self.span(1), self.mate)


def dot(a, b):
    return jnp.dot(a, b, preferred_element_type=F32)


def dot_last(a, b):
    return lax.dot_general(a, b, (((1,), (1,)), ((), ())), preferred_element_type=F32)


def dot_first(a, b):
    return lax.dot_general(a, b, (((0,), (0,)), ((), ())), preferred_element_type=F32)


def rounded(v):
    return v.astype(BF16).astype(F32)


def two(v):
    high = v.astype(BF16)
    return high, (v - high.astype(F32)).astype(BF16)


def kernel(
    tokens, gain, w_f, w_i, w_q, w_o, w_v, w_g, w_gr, w_gc, lb, shift, sinit, hgain, ck, cgain, cbias, w_or, w_oc,
    out,
    tok, gainv, xs, wb, stage, lbv, shv, siv, hgv, ckv, cgv, cbv,
    kgb, cb, vb, qb, ogb, ext, hsend, hrecv, sgr, sgc, mc, mcn, mr, head, qd, stb, rbuf, sty, stz, kv, scales,
    load_sem, send_sem, recv_sem,
):
    s, t = lax.axis_index("sp"), lax.axis_index("tp")
    z, y, x, c = s // 4, lax.rem(s, 4), t // 2, lax.rem(t, 2)
    w = Wires(send_sem, recv_sem)

    def at(zz, yy):
        return (lax.rem(zz + 4, 4) * 4 + lax.rem(yy + 4, 4), t)

    def across(xx):
        return (s, lax.rem(xx + 4, 4) * 2 + c)

    mate = (s, 1 - c + 2 * x)
    swap = (2 * t + lax.rem(s, 2), s // 2)
    home = s // 2 == t
    following, preceding = (lax.rem(s + 1, 16), t), (lax.rem(s + 15, 16), t)

    def load(k, src, dst):
        copy = pltpu.make_async_copy(src, dst, load_sem.at[k])
        copy.start()
        return copy

    first = [load(0, tokens, tok), load(1, gain, gainv)]
    for b, src in enumerate(
        (
            w_v, w_g, w_f, w_i, w_q, w_o,
            w_gr.at[:, pl.ds(0, 128)], w_gr.at[:, pl.ds(128, 128)],
            w_gc.at[:, pl.ds(0, 128)], w_gc.at[:, pl.ds(128, 128)],
        )
    ):
        load(2, src, wb.at[b, z, y])
    load(2, w_or, stage.at[0])
    load(2, w_oc, stage.at[1])
    twelve = wb.at[0, pl.ds(0, 3)]
    own = pltpu.make_async_copy(twelve, twelve, load_sem.at[2])
    rest = [
        load(k + 3, a, b)
        for k, (a, b) in enumerate(
            (
                (shift, shv), (lb, lbv), (sinit.at[0], siv), (hgain, hgv), (ck, ckv), (cgain, cgv), (cbias, cbv),
            )
        )
    ]

    barrier = pltpu.get_barrier_semaphore()
    partners = [at(z, y + 1), at(z, y - 1), at(z, y + 2), at(z + 1, y), at(z - 1, y), at(z + 2, y)]
    partners += [across(x + 1), across(x - 1), mate, following, preceding]
    for dev in partners:
        pl.semaphore_signal(barrier, inc=1, device_id=dev, device_id_type=MESH)

    @pl.when(jnp.logical_not(home))
    def _():
        pl.semaphore_signal(barrier, inc=1, device_id=swap, device_id_type=MESH)

    for copy in first:
        copy.wait()
    base = pl.multiple_of(t * TD, 16)

    def normalize(r, _):
        wide = tok[pl.ds(pl.multiple_of(r * 16, 16), 16), :].astype(F32)
        scale = lax.rsqrt(jnp.mean(wide * wide, axis=-1, keepdims=True) + EPS)
        xs[pl.ds(pl.multiple_of(base + r * 16, 16), 16), :] = (wide * scale * gainv[...]).astype(BF16)
        return 0

    lax.fori_loop(0, TD // 16, normalize, 0)
    own.wait()
    pl.semaphore_wait(barrier, len(partners) + jnp.where(home, 0, 1))

    def row_part(core):
        return lambda xx, h: xs.at[pl.ds(pl.multiple_of((xx * 2 + core) * TD + h * (TD // 2), 16), TD // 2), :]

    def half_of(buf, core):
        return lambda xx, h: buf.at[xx * 2 + core, pl.ds(384 * h, 384 if h == 0 else buf.shape[1] - 384)]

    def tp_exchange(lane, part, span):
        return Exchange(w, lane, [(x, across(x + 1), across(x - 1), part)], span, mate)

    token_ring = tp_exchange(1, row_part(c), lambda n: xs.at[pl.ds(0, TD * n), :])
    conv_ring = tp_exchange(2, half_of(mc, c), lambda n: mc.at[pl.ds(0, n)])
    rec_ring = tp_exchange(3, half_of(mr, c), lambda n: mr.at[pl.ds(0, n)])

    def along_y(part):
        return (y, at(z, y + 1), at(z, y - 1), part)

    def along_z(part):
        return (z, at(z + 1, y), at(z - 1, y), part)

    p1, p2 = [], []
    for g in range(6):
        a, b = 2 * g, 2 * g + 1
        rings = [
            along_y(lambda p, h, b=a: wb.at[b, z, p, pl.ds(64 * h, 64)]),
            along_z(lambda p, h, b=b: wb.at[b, p, y, pl.ds(64 * h, 64)]),
        ]
        p1.append(Exchange(w, 0, rings, lambda n, b=a: wb.at[b, 0, pl.ds(0, n)]))
        rings = [
            along_z(lambda p, h, b=a: wb.at[b, p, pl.ds(2 * h, 2)]),
            along_y(lambda p, h, b=b: wb.at[b, pl.ds(2 * h, 2), p]),
        ]
        p2.append(Exchange(w, 8, rings, lambda n, b=a: wb.at[b, pl.ds(0, n)]))

    for g in range(5):
        p1[g].start()
    token_ring.start()
    swap_k = w.new()

    def place(i):
        return wb.at[10 + i, swap[0] // 4, lax.rem(swap[0], 4)]

    @pl.when(jnp.logical_not(home))
    def _():
        for i in range(2):
            w.start(4, swap_k, stage.at[i], place(i), swap)

    @pl.when(home)
    def _():
        for i in range(2):
            pltpu.make_async_copy(stage.at[i], wb.at[10 + i, z, y], recv_sem.at[swap_k]).start()

    def swapped():
        @pl.when(jnp.logical_not(home))
        def _():
            w.arrive(swap_k, stage, swap)
            w.left(4, stage, swap)

        @pl.when(home)
        def _():
            pltpu.make_async_copy(stage, stage, recv_sem.at[swap_k]).wait()

    def whole(b):
        return wb[b].reshape(2048, 128)

    def project(group, finish, size, starts):
        weight = jnp.concatenate([whole(2 * group), whole(2 * group + 1)], axis=1)

        def tile(r, _):
            start = pl.multiple_of(starts(r), 32)
            rows = pl.ds(start, size)
            finish(start, rows, dot(xs[rows, :], weight))
            return 0

        return lambda low, high: lax.fori_loop(low, high, tile, 0)

    def project_all(group, finish):
        project(group, finish, PT, lambda r: r * PT)(0, T // PT)

    def by_ring(r):
        return lax.rem(x + jnp.where(r == 1, 3, jnp.where(r == 2, 1, jnp.where(r == 3, 2, 0))), 4) * XT

    def finish_fi(start, rows, v):
        gate = (1.0 - lbv[...]) * jax.nn.sigmoid(-rounded(v[:, :128]))
        kgb[rows, :] = gate
        cb[rows, :] = jnp.log1p(-gate) + shv[rows, :]
        vb[rows, :] = v[:, 128:].astype(BF16)

    def finish_vg(start, rows, v):
        gated = (rounded(v[:, :128]) * jax.nn.sigmoid(rounded(v[:, 128:]))).astype(BF16)
        ext[pl.ds(pl.multiple_of(start + HALO, 8), XT), :] = gated.astype(F32)

    def finish_qo(start, rows, v):
        raw = rounded(v[:, :128])
        qb[rows, :] = raw * jax.nn.sigmoid(raw)
        raw = rounded(v[:, 128:])
        ogb[rows, :] = raw * jax.nn.sigmoid(raw)

    def finish_gate(buf):
        def finish(start, rows, v):
            buf[rows, :] = jax.nn.sigmoid(rounded(v))

        return finish

    at_or_after = lax.broadcasted_iota(jnp.int32, (L, L), 0) >= lax.broadcasted_iota(jnp.int32, (L, L), 1)
    ones_below = jnp.where(at_or_after, 1.0, 0.0).astype(BF16)

    def pack_block(buf, i, decay, state):
        buf[i, pl.ds(0, HEAD), :] = state.astype(BF16)
        extra = jnp.concatenate([a.astype(F32) for a in two(decay)] + [jnp.zeros((14, HEAD), F32)], axis=0)
        buf[i, pl.ds(HEAD, 16), :] = extra.astype(BF16)

    def block_of(buf, i):
        both = buf[i, pl.ds(HEAD, 16), :].astype(F32)
        return both[0:1, :] + both[1:2, :], buf[i, pl.ds(0, HEAD), :].astype(F32)

    def local_states():
        for i in range(NC):
            rows = pl.ds(i * L, L)
            sides = dot(ones_below, jnp.concatenate(two(cb[rows, :]), axis=1))
            total = sides[:, :128] + sides[:, 128:]
            cb[rows, :] = total
            ending = (kgb[rows, :] * jnp.exp(total[L - 1 : L, :] - total)).astype(BF16)
            kv[i] = dot_first(vb[rows, :], ending)
        state = jnp.zeros((HEAD, HEAD), F32)
        before = jnp.zeros((1, HEAD), F32)
        for i in range(NC):
            last = cb[pl.ds(i * L + L - 1, 1), :]
            stb[i] = state.astype(BF16)
            rbuf[pl.ds(i, 1), :] = before
            state = jnp.exp(last) * state + kv[i]
            before = before + last
        pack_block(sty, y, jnp.exp(before), state)

    def local_outputs():
        for i in range(NC):
            rows = pl.ds(i * L, L)
            total, q = cb[rows, :], qb[rows, :]
            middle = 0.5 * total[L - 1 : L, :]
            left = (q * jnp.exp(total - middle)).astype(BF16)
            right = (kgb[rows, :] * jnp.exp(middle - total)).astype(BF16)
            scores = jnp.where(at_or_after, dot_last(left, right), 0.0).astype(BF16)
            o = dot(scores, vb[rows, :])
            o = o + dot_last((q * jnp.exp(total)).astype(BF16), stb[i])
            head[rows, :] = o
            qd[rows, :] = (q * jnp.exp(total + rbuf[pl.ds(i, 1), :])).astype(BF16)

    def convolve():
        ext[pl.ds(0, HALO), :] = jnp.where(s > 0, hrecv[...].astype(F32), 0.0)
        for i in range(T // 128):
            acc = jnp.zeros((128, HEAD), F32)
            for j in range(KW):
                acc = acc + ckv[pl.ds(j, 1), :] * ext[pl.ds(i * 128 + HALO - KW + 1 + j, 128), :]
            mc[t, pl.ds(i * 128, 128), :] = acc.astype(BF16)
        extra = [a.astype(F32) for v in (cgv[...], cbv[...]) for a in two(v)]
        mc[t, pl.ds(T, 16), :] = jnp.concatenate(extra + [jnp.zeros((12, HEAD), F32)], axis=0).astype(BF16)

    def out_weight(b):
        sides = [
            jnp.concatenate([wb[b, k // 2, (k % 2) * 2 + j] for k in range(8)], axis=0) for j in range(2)
        ]
        return jnp.concatenate(sides, axis=1)

    p1[0].relay()
    p1[1].relay()
    p1[2].relay()
    p1[3].relay()
    p1[4].relay()
    p1[0].rest()
    p2[0].first()
    p2[0].second()
    p1[1].rest()
    p2[1].first()
    token_ring.relay()
    p1[2].rest()
    p1[3].rest()
    p1[4].rest()
    p2[0].relay()
    p2[1].second()
    token_ring.near()
    p2[1].relay()
    p2[2].first()
    for copy in rest:
        copy.wait()
    p2[0].rest()
    token_ring.mate_near()
    project_vg = project(0, finish_vg, XT, by_ring)
    project_vg(0, 3)
    p2[2].second()
    swapped()
    p1[5].start()
    token_ring.far()
    token_ring.mate_far()
    project_vg(3, 4)
    hsend[...] = ext[pl.ds(T, HALO), :].astype(BF16)
    h_k = w.new()
    w.start(5, h_k, hsend, hrecv, following)
    p2[2].relay()
    p2[3].first()
    p2[1].rest()
    project_all(1, finish_fi)
    p1[5].relay()
    local_states()
    y_k, z_k = w.new(), w.new()
    for i in range(3):
        w.start(6, y_k, sty.at[y], sty.at[y], at(z, y + 1 + i))

    p2[3].second()
    w.arrive(h_k, hrecv, preceding)
    convolve()
    conv_ring.start()
    p2[2].rest()
    project_all(2, finish_qo)
    p2[3].relay()
    p2[4].first()

    w.arrive(y_k, sty.at[pl.ds(0, 3)], at(z, y + 1))
    row_decay, row_state = jnp.ones((1, HEAD), F32), jnp.zeros((HEAD, HEAD), F32)
    my_decay, my_state = row_decay, row_state
    for i in range(4):
        d, v = block_of(sty, i)
        row_decay, row_state = row_decay * d, d * row_state + v
        if i < 3:
            take = i < y
            my_decay = jnp.where(take, row_decay, my_decay)
            my_state = jnp.where(take, row_state, my_state)
    pack_block(stz, z, row_decay, row_state)
    for i in range(3):
        w.start(7, z_k, stz.at[z], stz.at[z], at(z + 1 + i, y))

    p2[4].second()
    local_outputs()
    conv_ring.relay()
    p1[5].rest()
    p2[4].relay()
    p2[5].first()

    w.arrive(z_k, stz.at[pl.ds(0, 3)], at(z + 1, y))
    entering = siv[...].T
    for i in range(3):
        d, v = block_of(stz, i)
        entering = jnp.where(i < z, d * entering + v, entering)
    entering = (my_decay * entering + my_state).astype(BF16)

    def finish_head(r, _):
        rows = pl.ds(pl.multiple_of(r * RT, RT), RT)
        h = head[rows, :] + dot_last(qd[rows, :], entering)
        h = h * lax.rsqrt(jnp.mean(h * h, axis=-1, keepdims=True) + EPS) * hgv[...]
        mr[t, rows, :] = (h * ogb[rows, :]).astype(BF16)
        return 0

    lax.fori_loop(0, T // RT, finish_head, 0)
    rec_ring.start()
    p2[5].second()
    conv_ring.near()
    p2[3].rest()
    project_all(3, finish_gate(sgr))
    conv_ring.far()
    conv_ring.mate_near()
    p2[5].relay()
    rec_ring.relay()
    conv_ring.mate_far()

    gains, biases = [], []
    for k in range(8):
        four = mc[k, pl.ds(T, 16), :].astype(F32)
        gains.append(0.5 * (four[0:1, :] + four[1:2, :]))
        biases.append(0.5 * (four[2:3, :] + four[3:4, :]))

    def conv_scale(r, _):
        rows = pl.ds(pl.multiple_of(r * 64, 64), 64)
        squares = sum(v * v for v in (mc[k, rows, :].astype(F32) for k in range(8)))
        scale = lax.rsqrt(jnp.sum(squares, axis=-1, keepdims=True) * (1.0 / CONV) + EPS)
        scales[rows, :] = jnp.broadcast_to(scale, (64, 128))
        return 0

    def normalize_conv(r, _):
        rows = pl.ds(pl.multiple_of(r * 64, 64), 64)
        scale = scales[rows, :]
        for k in range(8):
            half = mc[k, rows, :].astype(F32) * scale * gains[k] + biases[k]
            mcn[rows, pl.ds(k * 128, 128)] = (half + half * jnp.tanh(half)).astype(BF16)
        return 0

    lax.fori_loop(0, T // 64, conv_scale, 0, unroll=4)
    lax.fori_loop(0, T // 64, normalize_conv, 0, unroll=2)
    rec_ring.near()
    p2[4].rest()
    project_all(4, finish_gate(sgc))
    p2[5].rest()
    w_rec, w_conv = out_weight(10), out_weight(11)

    def conv_tile(r, _):
        rows = pl.ds(pl.multiple_of(r * RT, RT), RT)
        sgc[rows, :] = sgc[rows, :] * rounded(dot(mcn[rows, :], w_conv))
        return 0

    lax.fori_loop(0, T // RT, conv_tile, 0)
    rec_ring.far()
    rec_ring.mate_near()
    rec_ring.mate_far()

    def last_tile(r, _):
        rows = pl.ds(pl.multiple_of(r * RT, RT), RT)
        mixed = jnp.concatenate([mr[k, rows, :] for k in range(8)], axis=1)
        out[rows, :] = (sgr[rows, :] * rounded(dot(mixed, w_rec)) + sgc[rows, :]).astype(BF16)
        return 0

    lax.fori_loop(0, T // RT, last_tile, 0)
    w.left(0, wb.at[pl.ds(0, 3), pl.ds(0, 3)], mate)
    w.left(8, wb.at[pl.ds(0, 9)], mate)
    w.left(1, xs.at[pl.ds(0, 7 * TD), :], mate)
    w.left(2, mc.at[pl.ds(0, 7)], mate)
    w.left(3, mr.at[pl.ds(0, 7)], mate)
    w.left(5, hsend, following)
    w.left(6, sty.at[pl.ds(0, 3)], mate)
    w.left(7, stz.at[pl.ds(0, 3)], mate)


def local(
    tokens, norm_gain, w_query, w_forget, w_input, w_outgate, w_conv_value, w_conv_gate, w_gate_rec, w_gate_conv,
    lower_bound, decay_shift, state_init, head_gain, conv_kernel, channel_gain, channel_bias, w_out_rec, w_out_conv,
):
    line = lambda v: v.reshape(1, -1)
    args = (
        tokens, line(norm_gain), w_forget, w_input, w_query, w_outgate, w_conv_value, w_conv_gate, w_gate_rec,
        w_gate_conv, line(lower_bound), decay_shift, state_init, line(head_gain), conv_kernel, line(channel_gain),
        line(channel_bias), w_out_rec, w_out_conv,
    )
    v = pltpu.VMEM
    scratch = [
        v((TD, 2048), BF16), v((1, 2048), F32), v((T, 2048), BF16), v((12, 4, 4, 128, 128), BF16),
        v((2, 128, 128), BF16), v((1, 128), F32), v((T, 128), F32), v((128, 128), F32), v((1, 128), F32),
        v((KW, 128), F32), v((1, 128), F32), v((1, 128), F32),
        v((T, 128), F32), v((T, 128), F32), v((T, 128), BF16), v((T, 128), F32), v((T, 128), F32),
        v((T + HALO, 128), F32), v((HALO, 128), BF16), v((HALO, 128), BF16), v((T, 256), F32), v((T, 256), F32),
        v((8, T + 16, 128), BF16), v((T, CONV), BF16), v((8, T, 128), BF16), v((T, 128), F32), v((T, 128), BF16),
        v((NC, 128, 128), BF16), v((16, 128), F32), v((4, 144, 128), BF16), v((4, 144, 128), BF16), v((NC, 128, 128), F32), v((T, 128), F32),
        pltpu.SemaphoreType.DMA((10,)), pltpu.SemaphoreType.DMA((9,)), pltpu.SemaphoreType.DMA((43,)),
    ]
    return pl.pallas_call(
        kernel,
        out_shape=jax.ShapeDtypeStruct((T, 256), BF16),
        in_specs=[pl.BlockSpec(memory_space=pltpu.HBM)] * len(args),
        out_specs=pl.BlockSpec(memory_space=pltpu.VMEM),
        scratch_shapes=scratch,
        compiler_params=pltpu.CompilerParams(
            collective_id=0, has_side_effects=True, vmem_limit_bytes=40 * 1024 * 1024
        ),
    )(*[pltpu.with_memory_space_constraint(a, pltpu.HBM) for a in args])


def solution(mesh):
    both = P("sp", "tp")
    in_specs = (
        P(("sp", "tp"), None), P(), both, both, both, both, both, both, both, both, P("tp"), both,
        P("tp", None, None), P("tp"), P(None, "tp"), P("tp"), P("tp"), P("tp", "sp"), P("tp", "sp"),
    )
    return jax.shard_map(local, mesh=mesh, in_specs=in_specs, out_specs=both, check_vma=False)
```

```python
import functools

import jax
import jax.numpy as jnp
from jax import lax
from jax.experimental import pallas as pl
from jax.experimental.pallas import tpu as pltpu
from jax.sharding import PartitionSpec as P

MESH = pl.DeviceIdType.MESH
F32 = jnp.float32
BF16 = jnp.bfloat16
HEAD = 128
CONV = 1024
KW = 31
EPS = 1e-06
L = 64
T = 768
NC = T // L
TD = 96
RT = 256
XT = 192
PT = 384
HALO = 32


class Wires:
    def __init__(self, send_sem, recv_sem):
        self.send_sem, self.recv_sem = send_sem, recv_sem
        self.count = 0

    def new(self):
        self.count += 1
        return self.count - 1

    def make(self, lane, k, src, dst, dev):
        return pltpu.make_async_remote_copy(
            src_ref=src,
            dst_ref=dst,
            send_sem=self.send_sem.at[lane],
            recv_sem=self.recv_sem.at[k],
            device_id=dev,
            device_id_type=MESH,
        )

    def start(self, lane, k, src, dst, dev):
        self.make(lane, k, src, dst, dev).start()

    def arrive(self, k, span, dev):
        self.make(0, k, span, span, dev).wait_recv()

    def left(self, lane, span, dev):
        self.make(lane, 0, span, span, dev).wait_send()


class Exchange:
    def __init__(self, wires, lane, rings, span, mate=None):
        self.w, self.lane, self.rings, self.span, self.mate = wires, lane, rings, span, mate
        self.k = {"relay": wires.new(), "near": wires.new()}
        self.k["far"] = self.k["near"] if mate is None else wires.new()
        if mate is not None:
            self.k["mate_near"], self.k["mate_far"] = wires.new(), wires.new()

    def go(self, sem, view, dev):
        self.w.start(self.lane, self.k[sem], view, view, dev)

    def to_mate(self, sem, *views):
        if self.mate is not None:
            for view in views:
                self.go(sem, view, self.mate)

    def await_blocks(self, sem, n):
        self.w.arrive(self.k[sem], self.span(n * len(self.rings)), self.rings[0][1])

    def first(self):
        for pos, plus, minus, part in self.rings:
            self.go("relay", part(pos, 0), plus)
            self.go("relay", part(pos, 1), minus)

    def second(self):
        for pos, plus, minus, part in self.rings:
            self.go("near", part(pos, 1), plus)
            self.go("near", part(pos, 0), minus)
            self.to_mate("mate_near", part(pos, 0), part(pos, 1))

    def start(self):
        self.first()
        self.second()

    def relay(self):
        self.await_blocks("relay", 1)
        for pos, plus, minus, part in self.rings:
            left, right = part(lax.rem(pos + 3, 4), 0), part(lax.rem(pos + 1, 4), 1)
            self.go("far", left, plus)
            self.go("far", right, minus)
            self.to_mate("mate_near", left, right)

    def near(self):
        self.await_blocks("near", 1)
        for pos, plus, minus, part in self.rings:
            self.to_mate("mate_near", part(lax.rem(pos + 3, 4), 1), part(lax.rem(pos + 1, 4), 0))

    def far(self):
        self.await_blocks("far", 1)
        for pos, plus, minus, part in self.rings:
            self.to_mate("mate_far", part(lax.rem(pos + 2, 4), 0), part(lax.rem(pos + 2, 4), 1))

    def rest(self):
        self.await_blocks("near", 2)

    def mate_near(self):
        self.w.arrive(self.k["mate_near"], self.span(3), self.mate)

    def mate_far(self):
        self.w.arrive(self.k["mate_far"], self.span(1), self.mate)


def dot(a, b):
    return jnp.dot(a, b, preferred_element_type=F32)


def dot_last(a, b):
    return lax.dot_general(a, b, (((1,), (1,)), ((), ())), preferred_element_type=F32)


def dot_first(a, b):
    return lax.dot_general(a, b, (((0,), (0,)), ((), ())), preferred_element_type=F32)


def rounded(v):
    return v.astype(BF16).astype(F32)


def two(v):
    high = v.astype(BF16)
    return high, (v - high.astype(F32)).astype(BF16)


def kernel(
    tokens, gain, w_f, w_i, w_q, w_o, w_v, w_g, w_gr, w_gc, lb, shift, sinit, hgain, ck, cgain, cbias, w_or, w_oc,
    out,
    tok, gainv, xs, wb, stage, lbv, shv, siv, hgv, ckv, cgv, cbv,
    kgb, cb, vb, qb, ogb, ext, hsend, hrecv, sgr, sgc, mc, mcn, mr, head, qd, stb, rbuf, sty, stz, kv, scales,
    load_sem, send_sem, recv_sem,
):
    s, t = lax.axis_index("sp"), lax.axis_index("tp")
    z, y, x, c = s // 4, lax.rem(s, 4), t // 2, lax.rem(t, 2)
    w = Wires(send_sem, recv_sem)

    def at(zz, yy):
        return (lax.rem(zz + 4, 4) * 4 + lax.rem(yy + 4, 4), t)

    def across(xx):
        return (s, lax.rem(xx + 4, 4) * 2 + c)

    mate = (s, 1 - c + 2 * x)
    swap = (2 * t + lax.rem(s, 2), s // 2)
    home = s // 2 == t
    following, preceding = (lax.rem(s + 1, 16), t), (lax.rem(s + 15, 16), t)

    def load(k, src, dst):
        copy = pltpu.make_async_copy(src, dst, load_sem.at[k])
        copy.start()
        return copy

    first = [load(0, tokens, tok), load(1, gain, gainv)]
    for b, src in enumerate(
        (
            w_v, w_g, w_f, w_i, w_q, w_o,
            w_gr.at[:, pl.ds(0, 128)], w_gr.at[:, pl.ds(128, 128)],
            w_gc.at[:, pl.ds(0, 128)], w_gc.at[:, pl.ds(128, 128)],
        )
    ):
        load(2, src, wb.at[b, z, y])
    load(2, w_or, stage.at[0])
    load(2, w_oc, stage.at[1])
    twelve = wb.at[0, pl.ds(0, 3)]
    own = pltpu.make_async_copy(twelve, twelve, load_sem.at[2])
    rest = [
        load(k + 3, a, b)
        for k, (a, b) in enumerate(
            (
                (shift, shv), (lb, lbv), (sinit.at[0], siv), (hgain, hgv), (ck, ckv), (cgain, cgv), (cbias, cbv),
            )
        )
    ]

    barrier = pltpu.get_barrier_semaphore()
    partners = [at(z, y + 1), at(z, y - 1), at(z, y + 2), at(z + 1, y), at(z - 1, y), at(z + 2, y)]
    partners += [across(x + 1), across(x - 1), mate, following, preceding]
    for dev in partners:
        pl.semaphore_signal(barrier, inc=1, device_id=dev, device_id_type=MESH)

    @pl.when(jnp.logical_not(home))
    def _():
        pl.semaphore_signal(barrier, inc=1, device_id=swap, device_id_type=MESH)

    def row_part(core):
        return lambda xx, h: xs.at[pl.ds(pl.multiple_of((xx * 2 + core) * TD + h * (TD // 2), 16), TD // 2), :]

    def half_of(buf, core):
        return lambda xx, h: buf.at[xx * 2 + core, pl.ds(384 * h, 384 if h == 0 else buf.shape[1] - 384)]

    def tp_exchange(lane, part, span):
        return Exchange(w, lane, [(x, across(x + 1), across(x - 1), part)], span, mate)

    token_ring = tp_exchange(1, row_part(c), lambda n: xs.at[pl.ds(0, TD * n), :])
    conv_ring = tp_exchange(2, half_of(mc, c), lambda n: mc.at[pl.ds(0, n)])
    rec_ring = tp_exchange(3, half_of(mr, c), lambda n: mr.at[pl.ds(0, n)])

    def along_y(part):
        return (y, at(z, y + 1), at(z, y - 1), part)

    def along_z(part):
        return (z, at(z + 1, y), at(z - 1, y), part)

    p1, p2 = [], []
    for g in range(6):
        a, b = 2 * g, 2 * g + 1
        rings = [
            along_y(lambda p, h, b=a: wb.at[b, z, p, pl.ds(64 * h, 64)]),
            along_z(lambda p, h, b=b: wb.at[b, p, y, pl.ds(64 * h, 64)]),
        ]
        p1.append(Exchange(w, 0, rings, lambda n, b=a: wb.at[b, 0, pl.ds(0, n)]))
        rings = [
            along_z(lambda p, h, b=a: wb.at[b, p, pl.ds(2 * h, 2)]),
            along_y(lambda p, h, b=b: wb.at[b, pl.ds(2 * h, 2), p]),
        ]
        p2.append(Exchange(w, 8, rings, lambda n, b=a: wb.at[b, pl.ds(0, n)]))

    stz[...] = jnp.zeros_like(stz)
    own.wait()
    pl.semaphore_wait(barrier, len(partners) + jnp.where(home, 0, 1))
    for g in range(3):
        p1[g].start()
    swap_k = w.new()

    def place(i):
        return wb.at[10 + i, swap[0] // 4, lax.rem(swap[0], 4)]

    @pl.when(jnp.logical_not(home))
    def _():
        for i in range(2):
            w.start(4, swap_k, stage.at[i], place(i), swap)

    @pl.when(home)
    def _():
        for i in range(2):
            pltpu.make_async_copy(stage.at[i], wb.at[10 + i, z, y], recv_sem.at[swap_k]).start()

    def swapped():
        @pl.when(jnp.logical_not(home))
        def _():
            w.arrive(swap_k, stage, swap)
            w.left(4, stage, swap)

        @pl.when(home)
        def _():
            pltpu.make_async_copy(stage, stage, recv_sem.at[swap_k]).wait()

    for copy in first:
        copy.wait()
    base = pl.multiple_of(t * TD, 16)

    def normalize(r, _):
        wide = tok[pl.ds(pl.multiple_of(r * 16, 16), 16), :].astype(F32)
        scale = lax.rsqrt(jnp.mean(wide * wide, axis=-1, keepdims=True) + EPS)
        xs[pl.ds(pl.multiple_of(base + r * 16, 16), 16), :] = (wide * scale * gainv[...]).astype(BF16)
        return 0

    lax.fori_loop(0, TD // 16, normalize, 0, unroll=TD // 16)
    token_ring.start()

    def whole(b):
        return wb[b].reshape(2048, 128)

    def project(group, finish, size, starts):
        weight = jnp.concatenate([whole(2 * group), whole(2 * group + 1)], axis=1)

        def tile(r, _):
            start = pl.multiple_of(starts(r), 32)
            rows = pl.ds(start, size)
            finish(start, rows, dot(xs[rows, :], weight))
            return 0

        return lambda low, high: lax.fori_loop(low, high, tile, 0)

    def project_all(group, finish):
        project(group, finish, PT, lambda r: r * PT)(0, T // PT)

    def by_ring(r):
        return lax.rem(x + jnp.where(r == 1, 3, jnp.where(r == 2, 1, jnp.where(r == 3, 2, 0))), 4) * XT

    def finish_fi(start, rows, v):
        gate = (1.0 - lbv[...]) * jax.nn.sigmoid(-rounded(v[:, :128]))
        kgb[rows, :] = gate
        cb[rows, :] = jnp.log1p(-gate) + shv[rows, :]
        vb[rows, :] = v[:, 128:].astype(BF16)

    def finish_vg(start, rows, v):
        gated = (rounded(v[:, :128]) * jax.nn.sigmoid(rounded(v[:, 128:]))).astype(BF16)
        ext[pl.ds(pl.multiple_of(start + HALO, 8), XT), :] = gated.astype(F32)

    def finish_qo(start, rows, v):
        raw = rounded(v[:, :128])
        qb[rows, :] = raw * jax.nn.sigmoid(raw)
        raw = rounded(v[:, 128:])
        ogb[rows, :] = raw * jax.nn.sigmoid(raw)

    def finish_gate(buf):
        def finish(start, rows, v):
            buf[rows, :] = jax.nn.sigmoid(rounded(v))

        return finish

    at_or_after = lax.broadcasted_iota(jnp.int32, (L, L), 0) >= lax.broadcasted_iota(jnp.int32, (L, L), 1)
    ones_below = jnp.where(at_or_after, 1.0, 0.0).astype(BF16)

    def pack_block(buf, i, decay, state):
        buf[i, pl.ds(0, HEAD), :] = state.astype(BF16)
        extra = jnp.concatenate([a.astype(F32) for a in two(decay)] + [jnp.zeros((14, HEAD), F32)], axis=0)
        buf[i, pl.ds(HEAD, 16), :] = extra.astype(BF16)

    def block_of(buf, i):
        both = buf[i, pl.ds(HEAD, 16), :].astype(F32)
        return both[0:1, :] + both[1:2, :], buf[i, pl.ds(0, HEAD), :].astype(F32)

    def local_states():
        for i in range(NC):
            rows = pl.ds(i * L, L)
            sides = dot(ones_below, jnp.concatenate(two(cb[rows, :]), axis=1))
            total = sides[:, :128] + sides[:, 128:]
            cb[rows, :] = total
            ending = (kgb[rows, :] * jnp.exp(total[L - 1 : L, :] - total)).astype(BF16)
            kv[i] = dot_first(vb[rows, :], ending)
        state = jnp.zeros((HEAD, HEAD), F32)
        before = jnp.zeros((1, HEAD), F32)
        for i in range(NC):
            last = cb[pl.ds(i * L + L - 1, 1), :]
            stb[i] = state.astype(BF16)
            rbuf[pl.ds(i, 1), :] = before
            state = jnp.exp(last) * state + kv[i]
            before = before + last
        pack_block(sty, y, jnp.exp(before), state)

    def local_outputs():
        for i in range(NC):
            rows = pl.ds(i * L, L)
            total, q = cb[rows, :], qb[rows, :]
            middle = 0.5 * total[L - 1 : L, :]
            left = (q * jnp.exp(total - middle)).astype(BF16)
            right = (kgb[rows, :] * jnp.exp(middle - total)).astype(BF16)
            scores = jnp.where(at_or_after, dot_last(left, right), 0.0).astype(BF16)
            o = dot(scores, vb[rows, :])
            o = o + dot_last((q * jnp.exp(total)).astype(BF16), stb[i])
            head[rows, :] = o
            qd[rows, :] = (q * jnp.exp(total + rbuf[pl.ds(i, 1), :])).astype(BF16)

    def convolve():
        ext[pl.ds(0, HALO), :] = jnp.where(s > 0, hrecv[...].astype(F32), 0.0)
        for i in range(T // 128):
            acc = jnp.zeros((128, HEAD), F32)
            for j in range(KW):
                acc = acc + ckv[pl.ds(j, 1), :] * ext[pl.ds(i * 128 + HALO - KW + 1 + j, 128), :]
            mc[t, pl.ds(i * 128, 128), :] = acc.astype(BF16)
        extra = [a.astype(F32) for v in (cgv[...], cbv[...]) for a in two(v)]
        mc[t, pl.ds(T, 16), :] = jnp.concatenate(extra + [jnp.zeros((12, HEAD), F32)], axis=0).astype(BF16)

    def out_weight(b):
        sides = [
            jnp.concatenate([wb[b, k // 2, (k % 2) * 2 + j] for k in range(8)], axis=0) for j in range(2)
        ]
        return jnp.concatenate(sides, axis=1)

    p1[0].relay()
    p1[1].relay()
    p1[3].start()
    p1[4].start()
    p1[2].relay()
    p1[0].rest()
    p2[0].start()
    p1[1].rest()
    p2[1].first()
    token_ring.relay()
    p2[0].relay()
    p2[1].second()
    token_ring.near()
    p1[2].rest()
    p2[1].relay()
    p2[2].first()
    p1[3].relay()
    p1[4].relay()
    swapped()
    p1[5].start()
    for copy in rest:
        copy.wait()
    token_ring.far()
    p2[0].rest()
    p2[2].second()
    token_ring.mate_near()
    project_vg = project(0, finish_vg, XT, by_ring)
    project_vg(0, 3)
    token_ring.mate_far()
    project_vg(3, 4)
    hsend[...] = ext[pl.ds(T, HALO), :].astype(BF16)
    h_k = w.new()
    w.start(5, h_k, hsend, hrecv, following)
    p2[1].rest()
    project_all(1, finish_fi)
    local_states()
    y_k, z_k = w.new(), w.new()
    for i in (2, 1, 3):
        w.start(6, y_k, sty.at[y], sty.at[y], at(z, y + i))

    p2[2].relay()
    p1[3].rest()
    p1[5].relay()
    p2[3].first()
    w.arrive(h_k, hrecv, preceding)
    convolve()
    conv_ring.start()
    w.arrive(y_k, sty.at[pl.ds(0, 3)], at(z, y + 1))
    row_decay, row_state = jnp.ones((1, HEAD), F32), jnp.zeros((HEAD, HEAD), F32)
    my_decay, my_state = row_decay, row_state
    for i in range(4):
        d, v = block_of(sty, i)
        row_decay, row_state = row_decay * d, d * row_state + v
        if i < 3:
            take = i < y
            my_decay = jnp.where(take, row_decay, my_decay)
            my_state = jnp.where(take, row_state, my_state)
    pack_block(stz, z, row_decay, row_state)
    for i in (2, 1, 3):

        @pl.when(z + i < 4)
        def _(i=i):
            w.start(7, z_k, stz.at[z], stz.at[z], at(z + i, y))


    p2[3].second()
    p1[4].rest()
    p2[4].first()
    p2[2].rest()
    project_all(2, finish_qo)
    conv_ring.relay()
    p2[3].relay()
    p2[4].second()
    p1[5].rest()
    p2[5].first()
    local_outputs()
    p2[5].second()
    for i in (1, 2, 3):

        @pl.when(z == i)
        def _(i=i):
            w.arrive(z_k, stz.at[pl.ds(0, i)], at(z + 1, y))

    entering = siv[...].T
    for i in range(3):
        d, v = block_of(stz, i)
        entering = jnp.where(i < z, d * entering + v, entering)
    entering = (my_decay * entering + my_state).astype(BF16)

    def finish_head(low, high):
        for r in range(low, high):
            rows = pl.ds(r * 128, 128)
            h = head[rows, :] + dot_last(qd[rows, :], entering)
            h = h * lax.rsqrt(jnp.mean(h * h, axis=-1, keepdims=True) + EPS) * hgv[...]
            mr[t, rows, :] = (h * ogb[rows, :]).astype(BF16)

    finish_head(0, T // 128)
    rec_ring.start()
    conv_ring.near()
    p2[4].relay()
    conv_ring.far()
    conv_ring.mate_near()
    p2[3].rest()
    project_all(3, finish_gate(sgr))
    rec_ring.relay()
    p2[5].relay()
    conv_ring.mate_far()

    gains, biases = [], []
    for k in range(8):
        four = mc[k, pl.ds(T, 16), :].astype(F32)
        gains.append(0.5 * (four[0:1, :] + four[1:2, :]))
        biases.append(0.5 * (four[2:3, :] + four[3:4, :]))

    def conv_scale(r, _):
        rows = pl.ds(pl.multiple_of(r * 64, 64), 64)
        squares = sum(v * v for v in (mc[k, rows, :].astype(F32) for k in range(8)))
        scale = lax.rsqrt(jnp.sum(squares, axis=-1, keepdims=True) * (1.0 / CONV) + EPS)
        scales[rows, :] = jnp.broadcast_to(scale, (64, 128))
        return 0

    def normalize_conv(r, _):
        rows = pl.ds(pl.multiple_of(r * 64, 64), 64)
        scale = scales[rows, :]
        for k in range(8):
            half = mc[k, rows, :].astype(F32) * scale * gains[k] + biases[k]
            mcn[rows, pl.ds(k * 128, 128)] = (half + half * jnp.tanh(half)).astype(BF16)
        return 0

    lax.fori_loop(0, T // 64, conv_scale, 0, unroll=4)
    lax.fori_loop(0, T // 64, normalize_conv, 0, unroll=2)
    rec_ring.near()
    p2[4].rest()
    project_all(4, finish_gate(sgc))
    p2[5].rest()
    w_rec, w_conv = out_weight(10), out_weight(11)

    def conv_tile(r, _):
        rows = pl.ds(pl.multiple_of(r * RT, RT), RT)
        sgc[rows, :] = sgc[rows, :] * rounded(dot(mcn[rows, :], w_conv))
        return 0

    lax.fori_loop(0, T // RT, conv_tile, 0)
    rec_ring.far()
    rec_ring.mate_near()
    rec_ring.mate_far()

    def last_tile(r, _):
        rows = pl.ds(pl.multiple_of(r * RT, RT), RT)
        mixed = jnp.concatenate([mr[k, rows, :] for k in range(8)], axis=1)
        out[rows, :] = (sgr[rows, :] * rounded(dot(mixed, w_rec)) + sgc[rows, :]).astype(BF16)
        return 0

    lax.fori_loop(0, T // RT, last_tile, 0)
    w.left(0, wb.at[pl.ds(0, 3), pl.ds(0, 3)], mate)
    w.left(8, wb.at[pl.ds(0, 9)], mate)
    w.left(1, xs.at[pl.ds(0, 7 * TD), :], mate)
    w.left(2, mc.at[pl.ds(0, 7)], mate)
    w.left(3, mr.at[pl.ds(0, 7)], mate)
    w.left(5, hsend, following)
    w.left(6, sty.at[pl.ds(0, 3)], mate)
    for i in (1, 2, 3):

        @pl.when(z == 3 - i)
        def _(i=i):
            w.left(7, stz.at[pl.ds(0, i)], mate)


def local(
    tokens, norm_gain, w_query, w_forget, w_input, w_outgate, w_conv_value, w_conv_gate, w_gate_rec, w_gate_conv,
    lower_bound, decay_shift, state_init, head_gain, conv_kernel, channel_gain, channel_bias, w_out_rec, w_out_conv,
):
    line = lambda v: v.reshape(1, -1)
    args = (
        tokens, line(norm_gain), w_forget, w_input, w_query, w_outgate, w_conv_value, w_conv_gate, w_gate_rec,
        w_gate_conv, line(lower_bound), decay_shift, state_init, line(head_gain), conv_kernel, line(channel_gain),
        line(channel_bias), w_out_rec, w_out_conv,
    )
    v = pltpu.VMEM
    scratch = [
        v((TD, 2048), BF16), v((1, 2048), F32), v((T, 2048), BF16), v((12, 4, 4, 128, 128), BF16),
        v((2, 128, 128), BF16), v((1, 128), F32), v((T, 128), F32), v((128, 128), F32), v((1, 128), F32),
        v((KW, 128), F32), v((1, 128), F32), v((1, 128), F32),
        v((T, 128), F32), v((T, 128), F32), v((T, 128), BF16), v((T, 128), F32), v((T, 128), F32),
        v((T + HALO, 128), F32), v((HALO, 128), BF16), v((HALO, 128), BF16), v((T, 256), F32), v((T, 256), F32),
        v((8, T + 16, 128), BF16), v((T, CONV), BF16), v((8, T, 128), BF16), v((T, 128), F32), v((T, 128), BF16),
        v((NC, 128, 128), BF16), v((16, 128), F32), v((4, 144, 128), BF16), v((4, 144, 128), BF16), v((NC, 128, 128), F32), v((T, 128), F32),
        pltpu.SemaphoreType.DMA((10,)), pltpu.SemaphoreType.DMA((9,)), pltpu.SemaphoreType.DMA((43,)),
    ]
    return pl.pallas_call(
        kernel,
        out_shape=jax.ShapeDtypeStruct((T, 256), BF16),
        in_specs=[pl.BlockSpec(memory_space=pltpu.HBM)] * len(args),
        out_specs=pl.BlockSpec(memory_space=pltpu.VMEM),
        scratch_shapes=scratch,
        compiler_params=pltpu.CompilerParams(
            collective_id=0, has_side_effects=True, vmem_limit_bytes=40 * 1024 * 1024
        ),
    )(*[pltpu.with_memory_space_constraint(a, pltpu.HBM) for a in args])


def solution(mesh):
    both = P("sp", "tp")
    in_specs = (
        P(("sp", "tp"), None), P(), both, both, both, both, both, both, both, both, P("tp"), both,
        P("tp", None, None), P("tp"), P(None, "tp"), P("tp"), P("tp"), P("tp", "sp"), P("tp", "sp"),
    )
    return jax.shard_map(local, mesh=mesh, in_specs=in_specs, out_specs=both, check_vma=False)
```

```python
import functools

import jax
import jax.numpy as jnp
from jax import lax
from jax.experimental import pallas as pl
from jax.experimental.pallas import tpu as pltpu
from jax.sharding import PartitionSpec as P

MESH = pl.DeviceIdType.MESH
F32 = jnp.float32
BF16 = jnp.bfloat16
HEAD = 128
CONV = 1024
KW = 31
EPS = 1e-06
L = 64
T = 768
NC = T // L
TD = 96
RT = 256
XT = 192
PT = 384
HALO = 32


class Wires:
    def __init__(self, send_sem, recv_sem):
        self.send_sem, self.recv_sem = send_sem, recv_sem
        self.count = 0

    def new(self):
        self.count += 1
        return self.count - 1

    def make(self, lane, k, src, dst, dev):
        return pltpu.make_async_remote_copy(
            src_ref=src,
            dst_ref=dst,
            send_sem=self.send_sem.at[lane],
            recv_sem=self.recv_sem.at[k],
            device_id=dev,
            device_id_type=MESH,
        )

    def start(self, lane, k, src, dst, dev):
        self.make(lane, k, src, dst, dev).start()

    def arrive(self, k, span, dev):
        self.make(0, k, span, span, dev).wait_recv()

    def left(self, lane, span, dev):
        self.make(lane, 0, span, span, dev).wait_send()


class Exchange:
    def __init__(self, wires, lane, rings, span):
        self.w, self.lane, self.rings, self.span = wires, lane, rings, span
        self.k = {"relay": wires.new(), "rest": wires.new()}

    def go(self, sem, view, dev):
        self.w.start(self.lane, self.k[sem], view, view, dev)

    def await_blocks(self, sem, n):
        self.w.arrive(self.k[sem], self.span(n * len(self.rings)), self.rings[0][1])

    def first(self):
        for pos, plus, minus, part in self.rings:
            self.go("relay", part(pos, 0), plus)
            self.go("relay", part(pos, 1), minus)

    def second(self):
        for pos, plus, minus, part in self.rings:
            self.go("rest", part(pos, 1), plus)
            self.go("rest", part(pos, 0), minus)

    def start(self):
        self.first()
        self.second()

    def relay(self):
        self.await_blocks("relay", 1)
        for pos, plus, minus, part in self.rings:
            self.go("rest", part(lax.rem(pos + 3, 4), 0), plus)
            self.go("rest", part(lax.rem(pos + 1, 4), 1), minus)

    def rest(self):
        self.await_blocks("rest", 2)


class ChipExchange:
    def __init__(self, wires, lane, pos, plus, minus, mate, sizes, view, span):
        self.w, self.lane, self.pos, self.plus, self.minus, self.mate = wires, lane, pos, plus, minus, mate
        self.sizes, self.view, self.span = sizes, view, span
        self.k = {n: wires.new() for n in ("relay0", "relay1", "near", "far0", "far1", "mate_near", "mate_far")}

    def piece(self, shift, half, i):
        row = sum(self.sizes[0]) * half + (self.sizes[half][0] if i else 0)
        return self.view(lax.rem(self.pos + shift, 4), row, self.sizes[half][i])

    def half(self, shift, half):
        return self.view(lax.rem(self.pos + shift, 4), sum(self.sizes[0]) * half, sum(self.sizes[half]))

    def go(self, sem, view, dev):
        self.w.start(self.lane, self.k[sem], view, view, dev)

    def take(self, sem, blocks, rows, dev):
        self.w.arrive(self.k[sem], self.span(blocks, rows), dev)

    def rows(self, i):
        return self.sizes[0][i] + self.sizes[1][i]

    def start(self):
        for i in range(2):
            self.go(f"relay{i}", self.piece(0, 0, i), self.plus)
            self.go(f"relay{i}", self.piece(0, 1, i), self.minus)
        self.go("near", self.half(0, 1), self.plus)
        self.go("near", self.half(0, 0), self.minus)
        for h in range(2):
            self.go("mate_near", self.half(0, h), self.mate)

    def relay(self, i):
        self.take(f"relay{i}", 0, self.rows(i), self.plus)
        left, right = self.piece(3, 0, i), self.piece(1, 1, i)
        self.go(f"far{i}", left, self.plus)
        self.go(f"far{i}", right, self.minus)
        self.go("mate_near", left, self.mate)
        self.go("mate_near", right, self.mate)

    def near(self):
        self.take("near", 1, 0, self.plus)
        self.go("mate_near", self.half(3, 1), self.mate)
        self.go("mate_near", self.half(1, 0), self.mate)

    def far(self, i):
        self.take(f"far{i}", 0, self.rows(i), self.plus)
        self.go("mate_far", self.piece(2, 0, i), self.mate)
        self.go("mate_far", self.piece(2, 1, i), self.mate)

    def mate_near(self):
        self.take("mate_near", 3, 0, self.mate)

    def mate_far(self):
        self.take("mate_far", 1, 0, self.mate)


def dot(a, b):
    return jnp.dot(a, b, preferred_element_type=F32)


def dot_last(a, b):
    return lax.dot_general(a, b, (((1,), (1,)), ((), ())), preferred_element_type=F32)


def dot_first(a, b):
    return lax.dot_general(a, b, (((0,), (0,)), ((), ())), preferred_element_type=F32)


def rounded(v):
    return v.astype(BF16).astype(F32)


def two(v):
    high = v.astype(BF16)
    return high, (v - high.astype(F32)).astype(BF16)


def kernel(
    tokens, gain, w_f, w_i, w_q, w_o, w_v, w_g, w_gr, w_gc, lb, shift, sinit, hgain, ck, cgain, cbias, w_or, w_oc,
    out,
    tok, gainv, xs, wb, stage, lbv, shv, siv, hgv, ckv, cgv, cbv,
    kgb, cb, vb, qb, ogb, ext, hsend, hrecv, sgr, sgc, mc, mcn, mr, head, qd, stb, rbuf, sty, stz, kv, scales,
    load_sem, send_sem, recv_sem,
):
    s, t = lax.axis_index("sp"), lax.axis_index("tp")
    z, y, x, c = s // 4, lax.rem(s, 4), t // 2, lax.rem(t, 2)
    w = Wires(send_sem, recv_sem)

    def at(zz, yy):
        return (lax.rem(zz + 4, 4) * 4 + lax.rem(yy + 4, 4), t)

    def across(xx):
        return (s, lax.rem(xx + 4, 4) * 2 + c)

    mate = (s, 1 - c + 2 * x)
    swap = (2 * t + lax.rem(s, 2), s // 2)
    home = s // 2 == t
    following, preceding = (lax.rem(s + 1, 16), t), (lax.rem(s + 15, 16), t)

    def load(k, src, dst):
        copy = pltpu.make_async_copy(src, dst, load_sem.at[k])
        copy.start()
        return copy

    first = [load(0, tokens, tok), load(1, gain, gainv)]
    for b, src in enumerate(
        (
            w_v, w_g, w_f, w_i, w_q, w_o,
            w_gr.at[:, pl.ds(0, 128)], w_gr.at[:, pl.ds(128, 128)],
            w_gc.at[:, pl.ds(0, 128)], w_gc.at[:, pl.ds(128, 128)],
        )
    ):
        load(2, src, wb.at[b, z, y])
    load(2, w_or, stage.at[0])
    load(2, w_oc, stage.at[1])
    twelve = wb.at[0, pl.ds(0, 3)]
    own = pltpu.make_async_copy(twelve, twelve, load_sem.at[2])
    rest = [
        load(k + 3, a, b)
        for k, (a, b) in enumerate(
            (
                (shift, shv), (lb, lbv), (sinit.at[0], siv), (hgain, hgv), (ck, ckv), (cgain, cgv), (cbias, cbv),
            )
        )
    ]

    barrier = pltpu.get_barrier_semaphore()
    partners = [at(z, y + 1), at(z, y - 1), at(z, y + 2), at(z + 1, y), at(z - 1, y), at(z + 2, y)]
    partners += [across(x + 1), across(x - 1), mate, following, preceding]
    for dev in partners:
        pl.semaphore_signal(barrier, inc=1, device_id=dev, device_id_type=MESH)

    @pl.when(jnp.logical_not(home))
    def _():
        pl.semaphore_signal(barrier, inc=1, device_id=swap, device_id_type=MESH)

    def exchange(lane, sizes, view, span):
        return ChipExchange(w, lane, x, across(x + 1), across(x - 1), mate, sizes, view, span)

    def token_view(xx, row, rows):
        return xs.at[pl.ds(pl.multiple_of((xx * 2 + c) * TD + row, 16), rows), :]

    def block_view(buf):
        return lambda xx, row, rows: buf.at[xx * 2 + c, pl.ds(row, rows)]

    def block_span(buf):
        return lambda blocks, rows: buf.at[0, pl.ds(0, rows)] if rows else buf.at[pl.ds(0, blocks)]

    token_ring = exchange(
        1, ((32, 16), (32, 16)), token_view, lambda blocks, rows: xs.at[pl.ds(0, blocks * TD + rows), :]
    )
    conv_ring = exchange(2, ((192, 192), (192, 208)), block_view(mc), block_span(mc))
    rec_ring = exchange(3, ((192, 192), (192, 192)), block_view(mr), block_span(mr))

    def along_y(part):
        return (y, at(z, y + 1), at(z, y - 1), part)

    def along_z(part):
        return (z, at(z + 1, y), at(z - 1, y), part)

    p1, p2 = [], []
    for g in range(6):
        a, b = 2 * g, 2 * g + 1
        rings = [
            along_y(lambda p, h, b=a: wb.at[b, z, p, pl.ds(64 * h, 64)]),
            along_z(lambda p, h, b=b: wb.at[b, p, y, pl.ds(64 * h, 64)]),
        ]
        p1.append(Exchange(w, 0, rings, lambda n, b=a: wb.at[b, 0, pl.ds(0, n)]))
        rings = [
            along_z(lambda p, h, b=a: wb.at[b, p, pl.ds(2 * h, 2)]),
            along_y(lambda p, h, b=b: wb.at[b, pl.ds(2 * h, 2), p]),
        ]
        p2.append(Exchange(w, 8, rings, lambda n, b=a: wb.at[b, pl.ds(0, n)]))

    stz[...] = jnp.zeros_like(stz)
    own.wait()
    pl.semaphore_wait(barrier, len(partners) + jnp.where(home, 0, 1))
    for g in range(3):
        p1[g].start()
    swap_k = w.new()

    def place(i):
        return wb.at[10 + i, swap[0] // 4, lax.rem(swap[0], 4)]

    @pl.when(jnp.logical_not(home))
    def _():
        for i in range(2):
            w.start(4, swap_k, stage.at[i], place(i), swap)

    @pl.when(home)
    def _():
        for i in range(2):
            pltpu.make_async_copy(stage.at[i], wb.at[10 + i, z, y], recv_sem.at[swap_k]).start()

    def swapped():
        @pl.when(jnp.logical_not(home))
        def _():
            w.arrive(swap_k, stage, swap)
            w.left(4, stage, swap)

        @pl.when(home)
        def _():
            pltpu.make_async_copy(stage, stage, recv_sem.at[swap_k]).wait()

    for copy in first:
        copy.wait()
    base = pl.multiple_of(t * TD, 16)

    def normalize(r, _):
        wide = tok[pl.ds(pl.multiple_of(r * 16, 16), 16), :].astype(F32)
        scale = lax.rsqrt(jnp.mean(wide * wide, axis=-1, keepdims=True) + EPS)
        xs[pl.ds(pl.multiple_of(base + r * 16, 16), 16), :] = (wide * scale * gainv[...]).astype(BF16)
        return 0

    lax.fori_loop(0, TD // 16, normalize, 0, unroll=TD // 16)
    token_ring.start()

    def whole(b):
        return wb[b].reshape(2048, 128)

    def project(group, finish, size, starts):
        weight = jnp.concatenate([whole(2 * group), whole(2 * group + 1)], axis=1)

        def tile(r, _):
            start = pl.multiple_of(starts(r), 32)
            rows = pl.ds(start, size)
            finish(start, rows, dot(xs[rows, :], weight))
            return 0

        return lambda low, high: lax.fori_loop(low, high, tile, 0)

    def project_all(group, finish):
        project(group, finish, PT, lambda r: r * PT)(0, T // PT)

    def by_ring(r):
        return lax.rem(x + jnp.where(r == 1, 3, jnp.where(r == 2, 1, jnp.where(r == 3, 2, 0))), 4) * XT

    def finish_fi(start, rows, v):
        gate = (1.0 - lbv[...]) * jax.nn.sigmoid(-rounded(v[:, :128]))
        kgb[rows, :] = gate
        cb[rows, :] = jnp.log1p(-gate) + shv[rows, :]
        vb[rows, :] = v[:, 128:].astype(BF16)

    def finish_vg(start, rows, v):
        gated = (rounded(v[:, :128]) * jax.nn.sigmoid(rounded(v[:, 128:]))).astype(BF16)
        ext[pl.ds(pl.multiple_of(start + HALO, 8), XT), :] = gated.astype(F32)

    def finish_qo(start, rows, v):
        raw = rounded(v[:, :128])
        qb[rows, :] = raw * jax.nn.sigmoid(raw)
        raw = rounded(v[:, 128:])
        ogb[rows, :] = raw * jax.nn.sigmoid(raw)

    def finish_gate(buf):
        def finish(start, rows, v):
            buf[rows, :] = jax.nn.sigmoid(rounded(v))

        return finish

    at_or_after = lax.broadcasted_iota(jnp.int32, (L, L), 0) >= lax.broadcasted_iota(jnp.int32, (L, L), 1)
    ones_below = jnp.where(at_or_after, 1.0, 0.0).astype(BF16)

    def pack_block(buf, i, decay, state):
        buf[i, pl.ds(0, HEAD), :] = state.astype(BF16)
        extra = jnp.concatenate([a.astype(F32) for a in two(decay)] + [jnp.zeros((14, HEAD), F32)], axis=0)
        buf[i, pl.ds(HEAD, 16), :] = extra.astype(BF16)

    def block_of(buf, i):
        both = buf[i, pl.ds(HEAD, 16), :].astype(F32)
        return both[0:1, :] + both[1:2, :], buf[i, pl.ds(0, HEAD), :].astype(F32)

    def local_states():
        for i in range(NC):
            rows = pl.ds(i * L, L)
            sides = dot(ones_below, jnp.concatenate(two(cb[rows, :]), axis=1))
            total = sides[:, :128] + sides[:, 128:]
            cb[rows, :] = total
            ending = (kgb[rows, :] * jnp.exp(total[L - 1 : L, :] - total)).astype(BF16)
            kv[i] = dot_first(vb[rows, :], ending)
        state = jnp.zeros((HEAD, HEAD), F32)
        before = jnp.zeros((1, HEAD), F32)
        for i in range(NC):
            last = cb[pl.ds(i * L + L - 1, 1), :]
            stb[i] = state.astype(BF16)
            rbuf[pl.ds(i, 1), :] = before
            state = jnp.exp(last) * state + kv[i]
            before = before + last
        pack_block(sty, y, jnp.exp(before), state)

    def local_outputs():
        for i in range(NC):
            rows = pl.ds(i * L, L)
            total, q = cb[rows, :], qb[rows, :]
            middle = 0.5 * total[L - 1 : L, :]
            left = (q * jnp.exp(total - middle)).astype(BF16)
            right = (kgb[rows, :] * jnp.exp(middle - total)).astype(BF16)
            scores = jnp.where(at_or_after, dot_last(left, right), 0.0).astype(BF16)
            o = dot(scores, vb[rows, :])
            o = o + dot_last((q * jnp.exp(total)).astype(BF16), stb[i])
            head[rows, :] = o
            qd[rows, :] = (q * jnp.exp(total + rbuf[pl.ds(i, 1), :])).astype(BF16)

    def convolve(low, high):
        for i in range(low, high):
            acc = jnp.zeros((128, HEAD), F32)
            for j in range(KW):
                acc = acc + ckv[pl.ds(j, 1), :] * ext[pl.ds(i * 128 + HALO - KW + 1 + j, 128), :]
            mc[t, pl.ds(i * 128, 128), :] = acc.astype(BF16)

    def out_weight(b):
        sides = [
            jnp.concatenate([wb[b, k // 2, (k % 2) * 2 + j] for k in range(8)], axis=0) for j in range(2)
        ]
        return jnp.concatenate(sides, axis=1)

    p1[0].relay()
    p1[1].relay()
    p1[3].start()
    p1[4].start()
    p1[2].relay()
    p1[0].rest()
    p2[0].start()
    p1[1].rest()
    p2[1].first()
    token_ring.relay(0)
    token_ring.relay(1)
    p2[0].relay()
    p2[1].second()
    token_ring.near()
    p1[2].rest()
    p2[1].relay()
    p2[2].first()
    p1[3].relay()
    p1[4].relay()
    swapped()
    p1[5].start()
    for copy in rest:
        copy.wait()
    token_ring.far(0)
    token_ring.far(1)
    p2[0].rest()
    p2[2].second()
    token_ring.mate_near()
    project_vg = project(0, finish_vg, XT, by_ring)
    project_vg(0, 3)
    token_ring.mate_far()
    project_vg(3, 4)
    hsend[...] = ext[pl.ds(T, HALO), :].astype(BF16)
    h_k = w.new()
    w.start(5, h_k, hsend, hrecv, following)
    p2[1].rest()
    project_all(1, finish_fi)
    local_states()
    y_k, z_k = w.new(), w.new()
    for i in (2, 1, 3):
        w.start(6, y_k, sty.at[y], sty.at[y], at(z, y + i))

    p2[2].relay()
    p1[3].rest()
    p1[5].relay()
    p2[3].start()
    convolve(1, T // 128)
    extra = [a.astype(F32) for v in (cgv[...], cbv[...]) for a in two(v)]
    mc[t, pl.ds(T, 16), :] = jnp.concatenate(extra + [jnp.zeros((12, HEAD), F32)], axis=0).astype(BF16)
    w.arrive(h_k, hrecv, preceding)
    ext[pl.ds(0, HALO), :] = jnp.where(s > 0, hrecv[...].astype(F32), 0.0)
    convolve(0, 1)
    conv_ring.start()
    w.arrive(y_k, sty.at[pl.ds(0, 3)], at(z, y + 1))
    row_decay, row_state = jnp.ones((1, HEAD), F32), jnp.zeros((HEAD, HEAD), F32)
    my_decay, my_state = row_decay, row_state
    for i in range(4):
        d, v = block_of(sty, i)
        row_decay, row_state = row_decay * d, d * row_state + v
        if i < 3:
            take = i < y
            my_decay = jnp.where(take, row_decay, my_decay)
            my_state = jnp.where(take, row_state, my_state)
    pack_block(stz, z, row_decay, row_state)
    for i in (2, 1, 3):

        @pl.when(z + i < 4)
        def _(i=i):
            w.start(7, z_k, stz.at[z], stz.at[z], at(z + i, y))


    p1[4].rest()
    p2[4].first()
    p2[2].rest()
    project_all(2, finish_qo)
    conv_ring.relay(0)
    conv_ring.relay(1)
    p2[3].relay()
    p2[4].second()
    local_outputs()
    p1[5].rest()
    p2[5].start()
    for i in (1, 2, 3):

        @pl.when(z == i)
        def _(i=i):
            w.arrive(z_k, stz.at[pl.ds(0, i)], at(z + 1, y))

    entering = siv[...].T
    for i in range(3):
        d, v = block_of(stz, i)
        entering = jnp.where(i < z, d * entering + v, entering)
    entering = (my_decay * entering + my_state).astype(BF16)

    def finish_head(low, high):
        for r in range(low, high):
            rows = pl.ds(r * 128, 128)
            h = head[rows, :] + dot_last(qd[rows, :], entering)
            h = h * lax.rsqrt(jnp.mean(h * h, axis=-1, keepdims=True) + EPS) * hgv[...]
            mr[t, rows, :] = (h * ogb[rows, :]).astype(BF16)

    finish_head(0, T // 128)
    rec_ring.start()
    conv_ring.near()
    p2[4].relay()
    p2[3].rest()
    project_all(3, finish_gate(sgr))
    conv_ring.far(0)
    conv_ring.far(1)
    rec_ring.relay(0)
    p2[5].relay()
    conv_ring.mate_near()
    conv_ring.mate_far()
    rec_ring.relay(1)

    gains, biases = [], []
    for k in range(8):
        four = mc[k, pl.ds(T, 16), :].astype(F32)
        gains.append(0.5 * (four[0:1, :] + four[1:2, :]))
        biases.append(0.5 * (four[2:3, :] + four[3:4, :]))

    def conv_scale(r, _):
        rows = pl.ds(pl.multiple_of(r * 64, 64), 64)
        squares = sum(v * v for v in (mc[k, rows, :].astype(F32) for k in range(8)))
        scale = lax.rsqrt(jnp.sum(squares, axis=-1, keepdims=True) * (1.0 / CONV) + EPS)
        scales[rows, :] = jnp.broadcast_to(scale, (64, 128))
        return 0

    def normalize_conv(r, _):
        rows = pl.ds(pl.multiple_of(r * 64, 64), 64)
        scale = scales[rows, :]
        for k in range(8):
            half = mc[k, rows, :].astype(F32) * scale * gains[k] + biases[k]
            mcn[rows, pl.ds(k * 128, 128)] = (half + half * jnp.tanh(half)).astype(BF16)
        return 0

    lax.fori_loop(0, T // 64, conv_scale, 0, unroll=4)
    lax.fori_loop(0, T // 64, normalize_conv, 0, unroll=2)
    rec_ring.near()
    p2[4].rest()
    project_all(4, finish_gate(sgc))
    rec_ring.far(0)
    rec_ring.far(1)
    p2[5].rest()
    w_rec, w_conv = out_weight(10), out_weight(11)

    def conv_tile(r, _):
        rows = pl.ds(pl.multiple_of(r * RT, RT), RT)
        sgc[rows, :] = sgc[rows, :] * rounded(dot(mcn[rows, :], w_conv))
        return 0

    lax.fori_loop(0, T // RT, conv_tile, 0)
    rec_ring.mate_near()
    rec_ring.mate_far()

    def last_tile(r, _):
        rows = pl.ds(pl.multiple_of(r * RT, RT), RT)
        mixed = jnp.concatenate([mr[k, rows, :] for k in range(8)], axis=1)
        out[rows, :] = (sgr[rows, :] * rounded(dot(mixed, w_rec)) + sgc[rows, :]).astype(BF16)
        return 0

    lax.fori_loop(0, T // RT, last_tile, 0)
    w.left(0, wb.at[pl.ds(0, 3), pl.ds(0, 3)], mate)
    w.left(8, wb.at[pl.ds(0, 9)], mate)
    w.left(1, xs.at[pl.ds(0, 7 * TD), :], mate)
    w.left(2, mc.at[pl.ds(0, 7)], mate)
    w.left(3, mr.at[pl.ds(0, 7)], mate)
    w.left(5, hsend, following)
    w.left(6, sty.at[pl.ds(0, 3)], mate)
    for i in (1, 2, 3):

        @pl.when(z == 3 - i)
        def _(i=i):
            w.left(7, stz.at[pl.ds(0, i)], mate)


def local(
    tokens, norm_gain, w_query, w_forget, w_input, w_outgate, w_conv_value, w_conv_gate, w_gate_rec, w_gate_conv,
    lower_bound, decay_shift, state_init, head_gain, conv_kernel, channel_gain, channel_bias, w_out_rec, w_out_conv,
):
    line = lambda v: v.reshape(1, -1)
    args = (
        tokens, line(norm_gain), w_forget, w_input, w_query, w_outgate, w_conv_value, w_conv_gate, w_gate_rec,
        w_gate_conv, line(lower_bound), decay_shift, state_init, line(head_gain), conv_kernel, line(channel_gain),
        line(channel_bias), w_out_rec, w_out_conv,
    )
    v = pltpu.VMEM
    scratch = [
        v((TD, 2048), BF16), v((1, 2048), F32), v((T, 2048), BF16), v((12, 4, 4, 128, 128), BF16),
        v((2, 128, 128), BF16), v((1, 128), F32), v((T, 128), F32), v((128, 128), F32), v((1, 128), F32),
        v((KW, 128), F32), v((1, 128), F32), v((1, 128), F32),
        v((T, 128), F32), v((T, 128), F32), v((T, 128), BF16), v((T, 128), F32), v((T, 128), F32),
        v((T + HALO, 128), F32), v((HALO, 128), BF16), v((HALO, 128), BF16), v((T, 256), F32), v((T, 256), F32),
        v((8, T + 16, 128), BF16), v((T, CONV), BF16), v((8, T, 128), BF16), v((T, 128), F32), v((T, 128), BF16),
        v((NC, 128, 128), BF16), v((16, 128), F32), v((4, 144, 128), BF16), v((4, 144, 128), BF16), v((NC, 128, 128), F32), v((T, 128), F32),
        pltpu.SemaphoreType.DMA((10,)), pltpu.SemaphoreType.DMA((9,)), pltpu.SemaphoreType.DMA((49,)),
    ]
    return pl.pallas_call(
        kernel,
        out_shape=jax.ShapeDtypeStruct((T, 256), BF16),
        in_specs=[pl.BlockSpec(memory_space=pltpu.HBM)] * len(args),
        out_specs=pl.BlockSpec(memory_space=pltpu.VMEM),
        scratch_shapes=scratch,
        compiler_params=pltpu.CompilerParams(
            collective_id=0, has_side_effects=True, vmem_limit_bytes=40 * 1024 * 1024
        ),
    )(*[pltpu.with_memory_space_constraint(a, pltpu.HBM) for a in args])


def solution(mesh):
    both = P("sp", "tp")
    in_specs = (
        P(("sp", "tp"), None), P(), both, both, both, both, both, both, both, both, P("tp"), both,
        P("tp", None, None), P("tp"), P(None, "tp"), P("tp"), P("tp"), P("tp", "sp"), P("tp", "sp"),
    )
    return jax.shard_map(local, mesh=mesh, in_specs=in_specs, out_specs=both, check_vma=False)
```

```python
import functools

import jax
import jax.numpy as jnp
from jax import lax
from jax.experimental import pallas as pl
from jax.experimental.pallas import tpu as pltpu
from jax.sharding import PartitionSpec as P

MESH = pl.DeviceIdType.MESH
F32 = jnp.float32
BF16 = jnp.bfloat16
HEAD = 128
CONV = 1024
KW = 31
EPS = 1e-06
L = 64
T = 768
NC = T // L
TD = 96
RT = 256
XT = 192
PT = 384
HALO = 32


class Wires:
    def __init__(self, send_sem, recv_sem):
        self.send_sem, self.recv_sem = send_sem, recv_sem
        self.count = 0

    def new(self):
        self.count += 1
        return self.count - 1

    def make(self, lane, k, src, dst, dev):
        return pltpu.make_async_remote_copy(
            src_ref=src,
            dst_ref=dst,
            send_sem=self.send_sem.at[lane],
            recv_sem=self.recv_sem.at[k],
            device_id=dev,
            device_id_type=MESH,
        )

    def start(self, lane, k, src, dst, dev):
        self.make(lane, k, src, dst, dev).start()

    def arrive(self, k, span, dev):
        self.make(0, k, span, span, dev).wait_recv()

    def left(self, lane, span, dev):
        self.make(lane, 0, span, span, dev).wait_send()


class Exchange:
    def __init__(self, wires, lane, rings, span):
        self.w, self.lane, self.rings, self.span = wires, lane, rings, span
        self.k = {"relay": wires.new(), "rest": wires.new()}

    def go(self, sem, view, dev):
        self.w.start(self.lane, self.k[sem], view, view, dev)

    def await_blocks(self, sem, n):
        self.w.arrive(self.k[sem], self.span(n * len(self.rings)), self.rings[0][1])

    def first(self):
        for pos, plus, minus, part in self.rings:
            self.go("relay", part(pos, 0), plus)
            self.go("relay", part(pos, 1), minus)

    def second(self):
        for pos, plus, minus, part in self.rings:
            self.go("rest", part(pos, 1), plus)
            self.go("rest", part(pos, 0), minus)

    def start(self):
        self.first()
        self.second()

    def relay(self):
        self.await_blocks("relay", 1)
        for pos, plus, minus, part in self.rings:
            self.go("rest", part(lax.rem(pos + 3, 4), 0), plus)
            self.go("rest", part(lax.rem(pos + 1, 4), 1), minus)

    def rest(self):
        self.await_blocks("rest", 2)


class ChipExchange:
    def __init__(self, wires, lane, pos, plus, minus, mate, sizes, view, span):
        self.w, self.lane, self.pos, self.plus, self.minus, self.mate = wires, lane, pos, plus, minus, mate
        self.sizes, self.view, self.span = sizes, view, span
        self.k = {n: wires.new() for n in ("relay0", "relay1", "near", "far0", "far1", "mate_near", "mate_far")}

    def piece(self, shift, half, i):
        row = sum(self.sizes[0]) * half + (self.sizes[half][0] if i else 0)
        return self.view(lax.rem(self.pos + shift, 4), row, self.sizes[half][i])

    def half(self, shift, half):
        return self.view(lax.rem(self.pos + shift, 4), sum(self.sizes[0]) * half, sum(self.sizes[half]))

    def go(self, sem, view, dev):
        self.w.start(self.lane, self.k[sem], view, view, dev)

    def take(self, sem, blocks, rows, dev):
        self.w.arrive(self.k[sem], self.span(blocks, rows), dev)

    def rows(self, i):
        return self.sizes[0][i] + self.sizes[1][i]

    def start(self):
        for i in range(2):
            self.go(f"relay{i}", self.piece(0, 0, i), self.plus)
            self.go(f"relay{i}", self.piece(0, 1, i), self.minus)
        self.go("near", self.half(0, 1), self.plus)
        self.go("near", self.half(0, 0), self.minus)
        for h in range(2):
            self.go("mate_near", self.half(0, h), self.mate)

    def relay(self, i):
        self.take(f"relay{i}", 0, self.rows(i), self.plus)
        left, right = self.piece(3, 0, i), self.piece(1, 1, i)
        self.go(f"far{i}", left, self.plus)
        self.go(f"far{i}", right, self.minus)
        self.go("mate_near", left, self.mate)
        self.go("mate_near", right, self.mate)

    def near(self):
        self.take("near", 1, 0, self.plus)
        self.go("mate_near", self.half(3, 1), self.mate)
        self.go("mate_near", self.half(1, 0), self.mate)

    def far(self, i):
        self.take(f"far{i}", 0, self.rows(i), self.plus)
        self.go("mate_far", self.piece(2, 0, i), self.mate)
        self.go("mate_far", self.piece(2, 1, i), self.mate)

    def mate_near(self):
        self.take("mate_near", 3, 0, self.mate)

    def mate_far(self):
        self.take("mate_far", 1, 0, self.mate)


def dot(a, b):
    return jnp.dot(a, b, preferred_element_type=F32)


def dot_last(a, b):
    return lax.dot_general(a, b, (((1,), (1,)), ((), ())), preferred_element_type=F32)


def dot_first(a, b):
    return lax.dot_general(a, b, (((0,), (0,)), ((), ())), preferred_element_type=F32)


def rounded(v):
    return v.astype(BF16).astype(F32)


def two(v):
    high = v.astype(BF16)
    return high, (v - high.astype(F32)).astype(BF16)


def kernel(
    tokens, gain, w_f, w_i, w_q, w_o, w_v, w_g, w_gr, w_gc, lb, shift, sinit, hgain, ck, cgain, cbias, w_or, w_oc,
    out,
    tok, gainv, xs, wb, stage, lbv, shv, siv, hgv, ckv, cgv, cbv,
    kgb, cb, vb, qb, ogb, ext, hsend, hrecv, sgr, sgc, mc, mcn, mr, head, qd, stb, rbuf, sty, stz, kv, scales, acc,
    load_sem, send_sem, recv_sem,
):
    s, t = lax.axis_index("sp"), lax.axis_index("tp")
    z, y, x, c = s // 4, lax.rem(s, 4), t // 2, lax.rem(t, 2)
    w = Wires(send_sem, recv_sem)

    def at(zz, yy):
        return (lax.rem(zz + 4, 4) * 4 + lax.rem(yy + 4, 4), t)

    def across(xx):
        return (s, lax.rem(xx + 4, 4) * 2 + c)

    mate = (s, 1 - c + 2 * x)
    swap = (2 * t + lax.rem(s, 2), s // 2)
    home = s // 2 == t
    following, preceding = (lax.rem(s + 1, 16), t), (lax.rem(s + 15, 16), t)

    def load(k, src, dst):
        copy = pltpu.make_async_copy(src, dst, load_sem.at[k])
        copy.start()
        return copy

    first = [load(0, tokens, tok), load(1, gain, gainv)]
    for b, src in enumerate(
        (
            w_v, w_g, w_f, w_i, w_q, w_o,
            w_gr.at[:, pl.ds(0, 128)], w_gr.at[:, pl.ds(128, 128)],
            w_gc.at[:, pl.ds(0, 128)], w_gc.at[:, pl.ds(128, 128)],
        )
    ):
        load(2, src, wb.at[b, z, y])
    load(2, w_or, stage.at[0])
    load(2, w_oc, stage.at[1])
    twelve = wb.at[0, pl.ds(0, 3)]
    own = pltpu.make_async_copy(twelve, twelve, load_sem.at[2])
    rest = [
        load(k + 3, a, b)
        for k, (a, b) in enumerate(
            (
                (shift, shv), (lb, lbv), (sinit.at[0], siv), (hgain, hgv), (ck, ckv), (cgain, cgv), (cbias, cbv),
            )
        )
    ]

    barrier = pltpu.get_barrier_semaphore()
    partners = [at(z, y + 1), at(z, y - 1), at(z, y + 2), at(z + 1, y), at(z - 1, y), at(z + 2, y)]
    partners += [across(x + 1), across(x - 1), mate, following, preceding]
    for dev in partners:
        pl.semaphore_signal(barrier, inc=1, device_id=dev, device_id_type=MESH)

    @pl.when(jnp.logical_not(home))
    def _():
        pl.semaphore_signal(barrier, inc=1, device_id=swap, device_id_type=MESH)

    def exchange(lane, sizes, view, span):
        return ChipExchange(w, lane, x, across(x + 1), across(x - 1), mate, sizes, view, span)

    def token_view(xx, row, rows):
        return xs.at[pl.ds(pl.multiple_of((xx * 2 + c) * TD + row, 16), rows), :]

    def block_view(buf):
        return lambda xx, row, rows: buf.at[xx * 2 + c, pl.ds(row, rows)]

    def block_span(buf):
        return lambda blocks, rows: buf.at[0, pl.ds(0, rows)] if rows else buf.at[pl.ds(0, blocks)]

    token_ring = exchange(
        1, ((32, 16), (32, 16)), token_view, lambda blocks, rows: xs.at[pl.ds(0, blocks * TD + rows), :]
    )
    conv_ring = exchange(2, ((192, 192), (192, 208)), block_view(mc), block_span(mc))
    rec_ring = exchange(3, ((192, 192), (192, 192)), block_view(mr), block_span(mr))

    def along_y(part):
        return (y, at(z, y + 1), at(z, y - 1), part)

    def along_z(part):
        return (z, at(z + 1, y), at(z - 1, y), part)

    p1, p2 = [], []
    for g in range(6):
        a, b = 2 * g, 2 * g + 1
        rings = [
            along_y(lambda p, h, b=a: wb.at[b, z, p, pl.ds(64 * h, 64)]),
            along_z(lambda p, h, b=b: wb.at[b, p, y, pl.ds(64 * h, 64)]),
        ]
        p1.append(Exchange(w, 0, rings, lambda n, b=a: wb.at[b, 0, pl.ds(0, n)]))
        rings = [
            along_z(lambda p, h, b=a: wb.at[b, p, pl.ds(2 * h, 2)]),
            along_y(lambda p, h, b=b: wb.at[b, pl.ds(2 * h, 2), p]),
        ]
        p2.append(Exchange(w, 8, rings, lambda n, b=a: wb.at[b, pl.ds(0, n)]))

    stz[...] = jnp.zeros_like(stz)
    own.wait()
    pl.semaphore_wait(barrier, len(partners) + jnp.where(home, 0, 1))
    for g in range(3):
        p1[g].start()
    swap_k, y_k, z_k, h_k = (w.new() for _ in range(4))

    def place(i):
        return wb.at[10 + i, swap[0] // 4, lax.rem(swap[0], 4)]

    @pl.when(jnp.logical_not(home))
    def _():
        for i in range(2):
            w.start(4, swap_k, stage.at[i], place(i), swap)

    @pl.when(home)
    def _():
        for i in range(2):
            pltpu.make_async_copy(stage.at[i], wb.at[10 + i, z, y], recv_sem.at[swap_k]).start()

    def swapped():
        @pl.when(jnp.logical_not(home))
        def _():
            w.arrive(swap_k, stage, swap)
            w.left(4, stage, swap)

        @pl.when(home)
        def _():
            pltpu.make_async_copy(stage, stage, recv_sem.at[swap_k]).wait()

    for copy in first:
        copy.wait()
    base = pl.multiple_of(t * TD, 16)

    def normalize(r, _):
        wide = tok[pl.ds(pl.multiple_of(r * 16, 16), 16), :].astype(F32)
        scale = lax.rsqrt(jnp.mean(wide * wide, axis=-1, keepdims=True) + EPS)
        xs[pl.ds(pl.multiple_of(base + r * 16, 16), 16), :] = (wide * scale * gainv[...]).astype(BF16)
        return 0

    lax.fori_loop(0, TD // 16, normalize, 0, unroll=TD // 16)
    token_ring.start()

    def whole(b):
        return wb[b].reshape(2048, 128)

    def project(group, finish, size, starts):
        weight = jnp.concatenate([whole(2 * group), whole(2 * group + 1)], axis=1)

        def tile(r, _):
            start = pl.multiple_of(starts(r), 32)
            rows = pl.ds(start, size)
            finish(start, rows, dot(xs[rows, :], weight))
            return 0

        return lambda low, high: lax.fori_loop(low, high, tile, 0)

    def project_all(group, finish):
        project(group, finish, PT, lambda r: r * PT)(0, T // PT)

    def by_ring(r):
        return lax.rem(x + jnp.where(r == 1, 3, jnp.where(r == 2, 1, jnp.where(r == 3, 2, 0))), 4) * XT

    def finish_fi(start, rows, v):
        gate = (1.0 - lbv[...]) * jax.nn.sigmoid(-rounded(v[:, :128]))
        kgb[rows, :] = gate
        cb[rows, :] = jnp.log1p(-gate) + shv[rows, :]
        vb[rows, :] = v[:, 128:].astype(BF16)

    def finish_vg(start, rows, v):
        gated = (rounded(v[:, :128]) * jax.nn.sigmoid(rounded(v[:, 128:]))).astype(BF16)
        ext[pl.ds(pl.multiple_of(start + HALO, 8), XT), :] = gated.astype(F32)

    def finish_qo(start, rows, v):
        raw = rounded(v[:, :128])
        qb[rows, :] = raw * jax.nn.sigmoid(raw)
        raw = rounded(v[:, 128:])
        ogb[rows, :] = raw * jax.nn.sigmoid(raw)

    def finish_gate(buf):
        def finish(start, rows, v):
            buf[rows, :] = jax.nn.sigmoid(rounded(v))

        return finish

    at_or_after = lax.broadcasted_iota(jnp.int32, (L, L), 0) >= lax.broadcasted_iota(jnp.int32, (L, L), 1)
    ones_below = jnp.where(at_or_after, 1.0, 0.0).astype(BF16)

    def pack_block(buf, i, decay, state):
        buf[i, pl.ds(0, HEAD), :] = state.astype(BF16)
        extra = jnp.concatenate([a.astype(F32) for a in two(decay)] + [jnp.zeros((14, HEAD), F32)], axis=0)
        buf[i, pl.ds(HEAD, 16), :] = extra.astype(BF16)

    def block_of(buf, i):
        both = buf[i, pl.ds(HEAD, 16), :].astype(F32)
        return both[0:1, :] + both[1:2, :], buf[i, pl.ds(0, HEAD), :].astype(F32)

    def local_states():
        for i in range(NC):
            rows = pl.ds(i * L, L)
            sides = dot(ones_below, jnp.concatenate(two(cb[rows, :]), axis=1))
            total = sides[:, :128] + sides[:, 128:]
            cb[rows, :] = total
            ending = (kgb[rows, :] * jnp.exp(total[L - 1 : L, :] - total)).astype(BF16)
            kv[i] = dot_first(vb[rows, :], ending)
        state = jnp.zeros((HEAD, HEAD), F32)
        before = jnp.zeros((1, HEAD), F32)
        for i in range(NC):
            last = cb[pl.ds(i * L + L - 1, 1), :]
            stb[i] = state.astype(BF16)
            rbuf[pl.ds(i, 1), :] = before
            state = jnp.exp(last) * state + kv[i]
            before = before + last
        pack_block(sty, y, jnp.exp(before), state)

    def local_outputs():
        for i in range(NC):
            rows = pl.ds(i * L, L)
            total, q = cb[rows, :], qb[rows, :]
            middle = 0.5 * total[L - 1 : L, :]
            left = (q * jnp.exp(total - middle)).astype(BF16)
            right = (kgb[rows, :] * jnp.exp(middle - total)).astype(BF16)
            scores = jnp.where(at_or_after, dot_last(left, right), 0.0).astype(BF16)
            o = dot(scores, vb[rows, :])
            o = o + dot_last((q * jnp.exp(total)).astype(BF16), stb[i])
            head[rows, :] = o
            qd[rows, :] = (q * jnp.exp(total + rbuf[pl.ds(i, 1), :])).astype(BF16)

    def convolve(low, high):
        for i in range(low, high):
            acc = jnp.zeros((128, HEAD), F32)
            for j in range(KW):
                acc = acc + ckv[pl.ds(j, 1), :] * ext[pl.ds(i * 128 + HALO - KW + 1 + j, 128), :]
            mc[t, pl.ds(i * 128, 128), :] = acc.astype(BF16)

    def take_z():
        for i in (1, 2, 3):

            @pl.when(z == i)
            def _(i=i):
                w.arrive(z_k, stz.at[pl.ds(0, i)], at(z + 1, y))

    def chip_weight(b, xx):
        top, low = ([wb[b, xx, 2 * k + j] for j in range(2)] for k in range(2))
        return jnp.concatenate([jnp.concatenate(top, axis=1), jnp.concatenate(low, axis=1)], axis=0)

    def chip_blocks(rows, xx):
        return jnp.concatenate([mr[2 * xx, rows, :], mr[2 * xx + 1, rows, :]], axis=1)

    p1[0].relay()
    p1[1].relay()
    p1[3].start()
    p1[4].start()
    p1[2].relay()
    p1[0].rest()
    p2[0].start()
    p1[1].rest()
    p2[1].first()
    token_ring.relay(0)
    token_ring.relay(1)
    p2[0].relay()
    p2[1].second()
    token_ring.near()
    p1[2].rest()
    p2[1].relay()
    p2[2].first()
    p1[3].relay()
    p1[4].relay()
    swapped()
    p1[5].start()
    for copy in rest:
        copy.wait()
    token_ring.far(0)
    token_ring.far(1)
    p2[0].rest()
    p2[2].second()
    token_ring.mate_near()
    project_vg = project(0, finish_vg, XT, by_ring)
    project_vg(0, 3)
    token_ring.mate_far()
    project_vg(3, 4)
    hsend[...] = ext[pl.ds(T, HALO), :].astype(BF16)
    w.start(5, h_k, hsend, hrecv, following)
    p2[1].rest()
    project_all(1, finish_fi)
    local_states()
    for i in (2, 1, 3):
        w.start(6, y_k, sty.at[y], sty.at[y], at(z, y + i))

    p2[2].relay()
    p1[3].rest()
    p1[5].relay()
    p2[3].start()
    convolve(1, T // 128)
    extra = [a.astype(F32) for v in (cgv[...], cbv[...]) for a in two(v)]
    mc[t, pl.ds(T, 16), :] = jnp.concatenate(extra + [jnp.zeros((12, HEAD), F32)], axis=0).astype(BF16)
    w.arrive(h_k, hrecv, preceding)
    ext[pl.ds(0, HALO), :] = jnp.where(s > 0, hrecv[...].astype(F32), 0.0)
    convolve(0, 1)
    conv_ring.start()
    w.arrive(y_k, sty.at[pl.ds(0, 3)], at(z, y + 1))
    row_decay, row_state = jnp.ones((1, HEAD), F32), jnp.zeros((HEAD, HEAD), F32)
    my_decay, my_state = row_decay, row_state
    for i in range(4):
        d, v = block_of(sty, i)
        row_decay, row_state = row_decay * d, d * row_state + v
        if i < 3:
            take = i < y
            my_decay = jnp.where(take, row_decay, my_decay)
            my_state = jnp.where(take, row_state, my_state)
    pack_block(stz, z, row_decay, row_state)
    for i in (2, 1, 3):

        @pl.when(z + i < 4)
        def _(i=i):
            w.start(7, z_k, stz.at[z], stz.at[z], at(z + i, y))


    p1[4].rest()
    p2[4].first()
    p2[2].rest()
    project_all(2, finish_qo)
    conv_ring.relay(0)
    conv_ring.relay(1)
    p2[3].relay()
    p2[4].second()
    local_outputs()
    p1[5].rest()
    p2[5].start()
    take_z()
    entering = siv[...].T
    for i in range(3):
        d, v = block_of(stz, i)
        entering = jnp.where(i < z, d * entering + v, entering)
    entering = (my_decay * entering + my_state).astype(BF16)

    def finish_head(low, high):
        for r in range(low, high):
            rows = pl.ds(r * 128, 128)
            h = head[rows, :] + dot_last(qd[rows, :], entering)
            h = h * lax.rsqrt(jnp.mean(h * h, axis=-1, keepdims=True) + EPS) * hgv[...]
            mr[t, rows, :] = (h * ogb[rows, :]).astype(BF16)

    finish_head(0, T // 128)
    rec_ring.start()
    conv_ring.near()
    p2[4].relay()
    p2[3].rest()
    project_all(3, finish_gate(sgr))
    conv_ring.far(0)
    conv_ring.far(1)
    rec_ring.relay(0)
    rec_ring.relay(1)
    p2[5].relay()
    conv_ring.mate_near()
    conv_ring.mate_far()

    gains, biases = [], []
    for k in range(8):
        four = mc[k, pl.ds(T, 16), :].astype(F32)
        gains.append(0.5 * (four[0:1, :] + four[1:2, :]))
        biases.append(0.5 * (four[2:3, :] + four[3:4, :]))

    def conv_scale(r, _):
        rows = pl.ds(pl.multiple_of(r * 64, 64), 64)
        squares = sum(v * v for v in (mc[k, rows, :].astype(F32) for k in range(8)))
        scale = lax.rsqrt(jnp.sum(squares, axis=-1, keepdims=True) * (1.0 / CONV) + EPS)
        scales[rows, :] = jnp.broadcast_to(scale, (64, 128))
        return 0

    def normalize_conv(r, _):
        rows = pl.ds(pl.multiple_of(r * 64, 64), 64)
        scale = scales[rows, :]
        for k in range(8):
            half = mc[k, rows, :].astype(F32) * scale * gains[k] + biases[k]
            mcn[rows, pl.ds(k * 128, 128)] = (half + half * jnp.tanh(half)).astype(BF16)
        return 0

    lax.fori_loop(0, T // 64, conv_scale, 0, unroll=4)
    lax.fori_loop(0, T // 64, normalize_conv, 0, unroll=2)
    rec_ring.near()
    p2[4].rest()
    project_all(4, finish_gate(sgc))
    rec_ring.far(0)
    rec_ring.far(1)
    p2[5].rest()
    w_conv = jnp.concatenate([chip_weight(11, xx) for xx in range(4)], axis=0)

    def conv_tile(r, _):
        rows = pl.ds(pl.multiple_of(r * PT, PT), PT)
        sgc[rows, :] = sgc[rows, :] * rounded(dot(mcn[rows, :], w_conv))
        return 0

    lax.fori_loop(0, T // PT, conv_tile, 0)
    rec_ring.mate_near()
    near = [x, lax.rem(x + 1, 4), lax.rem(x + 3, 4)]
    w_near = jnp.concatenate([chip_weight(10, xx) for xx in near], axis=0)

    def near_tile(r, _):
        rows = pl.ds(pl.multiple_of(r * PT, PT), PT)
        acc[rows, :] = dot(jnp.concatenate([chip_blocks(rows, xx) for xx in near], axis=1), w_near)
        return 0

    lax.fori_loop(0, T // PT, near_tile, 0)
    rec_ring.mate_far()
    opposite = lax.rem(x + 2, 4)
    w_far = chip_weight(10, opposite)

    def last_tile(r, _):
        rows = pl.ds(pl.multiple_of(r * RT, RT), RT)
        y_rec = rounded(acc[rows, :] + dot(chip_blocks(rows, opposite), w_far))
        out[rows, :] = (sgr[rows, :] * y_rec + sgc[rows, :]).astype(BF16)
        return 0

    lax.fori_loop(0, T // RT, last_tile, 0)
    w.left(0, wb.at[pl.ds(0, 3), pl.ds(0, 3)], mate)
    w.left(8, wb.at[pl.ds(0, 9)], mate)
    w.left(1, xs.at[pl.ds(0, 7 * TD), :], mate)
    w.left(2, mc.at[pl.ds(0, 7)], mate)
    w.left(3, mr.at[pl.ds(0, 7)], mate)
    w.left(5, hsend, following)
    w.left(6, sty.at[pl.ds(0, 3)], mate)
    for i in (1, 2, 3):

        @pl.when(z == 3 - i)
        def _(i=i):
            w.left(7, stz.at[pl.ds(0, i)], mate)


def local(
    tokens, norm_gain, w_query, w_forget, w_input, w_outgate, w_conv_value, w_conv_gate, w_gate_rec, w_gate_conv,
    lower_bound, decay_shift, state_init, head_gain, conv_kernel, channel_gain, channel_bias, w_out_rec, w_out_conv,
):
    line = lambda v: v.reshape(1, -1)
    args = (
        tokens, line(norm_gain), w_forget, w_input, w_query, w_outgate, w_conv_value, w_conv_gate, w_gate_rec,
        w_gate_conv, line(lower_bound), decay_shift, state_init, line(head_gain), conv_kernel, line(channel_gain),
        line(channel_bias), w_out_rec, w_out_conv,
    )
    v = pltpu.VMEM
    scratch = [
        v((TD, 2048), BF16), v((1, 2048), F32), v((T, 2048), BF16), v((12, 4, 4, 128, 128), BF16),
        v((2, 128, 128), BF16), v((1, 128), F32), v((T, 128), F32), v((128, 128), F32), v((1, 128), F32),
        v((KW, 128), F32), v((1, 128), F32), v((1, 128), F32),
        v((T, 128), F32), v((T, 128), F32), v((T, 128), BF16), v((T, 128), F32), v((T, 128), F32),
        v((T + HALO, 128), F32), v((HALO, 128), BF16), v((HALO, 128), BF16), v((T, 256), F32), v((T, 256), F32),
        v((8, T + 16, 128), BF16), v((T, CONV), BF16), v((8, T, 128), BF16), v((T, 128), F32), v((T, 128), BF16),
        v((NC, 128, 128), BF16), v((16, 128), F32), v((4, 144, 128), BF16), v((4, 144, 128), BF16), v((NC, 128, 128), F32), v((T, 128), F32), v((T, 256), F32),
        pltpu.SemaphoreType.DMA((10,)), pltpu.SemaphoreType.DMA((9,)), pltpu.SemaphoreType.DMA((49,)),
    ]
    return pl.pallas_call(
        kernel,
        out_shape=jax.ShapeDtypeStruct((T, 256), BF16),
        in_specs=[pl.BlockSpec(memory_space=pltpu.HBM)] * len(args),
        out_specs=pl.BlockSpec(memory_space=pltpu.VMEM),
        scratch_shapes=scratch,
        compiler_params=pltpu.CompilerParams(
            collective_id=0, has_side_effects=True, vmem_limit_bytes=40 * 1024 * 1024
        ),
    )(*[pltpu.with_memory_space_constraint(a, pltpu.HBM) for a in args])


def solution(mesh):
    both = P("sp", "tp")
    in_specs = (
        P(("sp", "tp"), None), P(), both, both, both, both, both, both, both, both, P("tp"), both,
        P("tp", None, None), P("tp"), P(None, "tp"), P("tp"), P("tp"), P("tp", "sp"), P("tp", "sp"),
    )
    return jax.shard_map(local, mesh=mesh, in_specs=in_specs, out_specs=both, check_vma=False)
```

```python
import functools

import jax
import jax.numpy as jnp
from jax import lax
from jax.experimental import pallas as pl
from jax.experimental.pallas import tpu as pltpu
from jax.sharding import PartitionSpec as P

MESH = pl.DeviceIdType.MESH
F32 = jnp.float32
BF16 = jnp.bfloat16
HEAD = 128
CONV = 1024
KW = 31
EPS = 1e-06
L = 64
T = 768
NC = T // L
TD = 96
RT = 256
XT = 192
PT = 384
HALO = 32


class Wires:
    def __init__(self, send_sem, recv_sem):
        self.send_sem, self.recv_sem = send_sem, recv_sem
        self.count = 0

    def new(self):
        self.count += 1
        return self.count - 1

    def make(self, lane, k, src, dst, dev):
        return pltpu.make_async_remote_copy(
            src_ref=src,
            dst_ref=dst,
            send_sem=self.send_sem.at[lane],
            recv_sem=self.recv_sem.at[k],
            device_id=dev,
            device_id_type=MESH,
        )

    def start(self, lane, k, src, dst, dev):
        self.make(lane, k, src, dst, dev).start()

    def arrive(self, k, span, dev):
        self.make(0, k, span, span, dev).wait_recv()

    def left(self, lane, span, dev):
        self.make(lane, 0, span, span, dev).wait_send()


class Exchange:
    def __init__(self, wires, lane, rings, span):
        self.w, self.lane, self.rings, self.span = wires, lane, rings, span
        self.k = {"relay": wires.new(), "rest": wires.new()}

    def go(self, sem, view, dev):
        self.w.start(self.lane, self.k[sem], view, view, dev)

    def await_blocks(self, sem, n):
        self.w.arrive(self.k[sem], self.span(n * len(self.rings)), self.rings[0][1])

    def first(self):
        for pos, plus, minus, part in self.rings:
            self.go("relay", part(pos, 0), plus)
            self.go("relay", part(pos, 1), minus)

    def second(self):
        for pos, plus, minus, part in self.rings:
            self.go("rest", part(pos, 1), plus)
            self.go("rest", part(pos, 0), minus)

    def start(self):
        self.first()
        self.second()

    def relay(self):
        self.await_blocks("relay", 1)
        for pos, plus, minus, part in self.rings:
            self.go("rest", part(lax.rem(pos + 3, 4), 0), plus)
            self.go("rest", part(lax.rem(pos + 1, 4), 1), minus)

    def rest(self):
        self.await_blocks("rest", 2)


class ChipExchange:
    def __init__(self, wires, lane, pos, plus, minus, mate, sizes, view, span):
        self.w, self.lane, self.pos, self.plus, self.minus, self.mate = wires, lane, pos, plus, minus, mate
        self.sizes, self.view, self.span = sizes, view, span
        self.k = {n: wires.new() for n in ("relay0", "relay1", "near", "far0", "far1", "mate_near", "mate_far")}

    def piece(self, shift, half, i):
        row = sum(self.sizes[0]) * half + (self.sizes[half][0] if i else 0)
        return self.view(lax.rem(self.pos + shift, 4), row, self.sizes[half][i])

    def half(self, shift, half):
        return self.view(lax.rem(self.pos + shift, 4), sum(self.sizes[0]) * half, sum(self.sizes[half]))

    def go(self, sem, view, dev):
        self.w.start(self.lane, self.k[sem], view, view, dev)

    def take(self, sem, blocks, rows, dev):
        self.w.arrive(self.k[sem], self.span(blocks, rows), dev)

    def rows(self, i):
        return self.sizes[0][i] + self.sizes[1][i]

    def start(self):
        for i in range(2):
            self.go(f"relay{i}", self.piece(0, 0, i), self.plus)
            self.go(f"relay{i}", self.piece(0, 1, i), self.minus)
        self.go("near", self.half(0, 1), self.plus)
        self.go("near", self.half(0, 0), self.minus)
        for h in range(2):
            self.go("mate_near", self.half(0, h), self.mate)

    def relay(self, i):
        self.take(f"relay{i}", 0, self.rows(i), self.plus)
        left, right = self.piece(3, 0, i), self.piece(1, 1, i)
        self.go(f"far{i}", left, self.plus)
        self.go(f"far{i}", right, self.minus)
        self.go("mate_near", left, self.mate)
        self.go("mate_near", right, self.mate)

    def near(self):
        self.take("near", 1, 0, self.plus)
        self.go("mate_near", self.half(3, 1), self.mate)
        self.go("mate_near", self.half(1, 0), self.mate)

    def far(self, i):
        self.take(f"far{i}", 0, self.rows(i), self.plus)
        self.go("mate_far", self.piece(2, 0, i), self.mate)
        self.go("mate_far", self.piece(2, 1, i), self.mate)

    def mate_near(self):
        self.take("mate_near", 3, 0, self.mate)

    def mate_far(self):
        self.take("mate_far", 1, 0, self.mate)


def dot(a, b):
    return jnp.dot(a, b, preferred_element_type=F32)


def dot_last(a, b):
    return lax.dot_general(a, b, (((1,), (1,)), ((), ())), preferred_element_type=F32)


def dot_first(a, b):
    return lax.dot_general(a, b, (((0,), (0,)), ((), ())), preferred_element_type=F32)


def rounded(v):
    return v.astype(BF16).astype(F32)


def two(v):
    high = v.astype(BF16)
    return high, (v - high.astype(F32)).astype(BF16)


def kernel(
    tokens, gain, w_f, w_i, w_q, w_o, w_v, w_g, w_gr, w_gc, lb, shift, sinit, hgain, ck, cgain, cbias, w_or, w_oc,
    out,
    tok, gainv, xs, wb, stage, lbv, shv, siv, hgv, ckv, cgv, cbv,
    kgb, cb, vb, qb, ogb, ext, hsend, hrecv, sgr, sgc, mc, mcn, mr, head, qd, stb, rbuf, sty, stz, kv, scales, acc,
    load_sem, send_sem, recv_sem,
):
    s, t = lax.axis_index("sp"), lax.axis_index("tp")
    z, y, x, c = s // 4, lax.rem(s, 4), t // 2, lax.rem(t, 2)
    w = Wires(send_sem, recv_sem)

    def at(zz, yy):
        return (lax.rem(zz + 4, 4) * 4 + lax.rem(yy + 4, 4), t)

    def across(xx):
        return (s, lax.rem(xx + 4, 4) * 2 + c)

    mate = (s, 1 - c + 2 * x)
    swap = (2 * t + lax.rem(s, 2), s // 2)
    home = s // 2 == t
    following, preceding = (lax.rem(s + 1, 16), t), (lax.rem(s + 15, 16), t)

    def load(k, src, dst):
        copy = pltpu.make_async_copy(src, dst, load_sem.at[k])
        copy.start()
        return copy

    first = [load(0, tokens, tok), load(1, gain, gainv)]
    for b, src in enumerate(
        (
            w_v, w_g, w_f, w_i, w_q, w_o,
            w_gr.at[:, pl.ds(0, 128)], w_gr.at[:, pl.ds(128, 128)],
            w_gc.at[:, pl.ds(0, 128)], w_gc.at[:, pl.ds(128, 128)],
        )
    ):
        load(2, src, wb.at[b, z, y])
    load(2, w_or, stage.at[0])
    load(2, w_oc, stage.at[1])
    twelve = wb.at[0, pl.ds(0, 3)]
    own = pltpu.make_async_copy(twelve, twelve, load_sem.at[2])
    rest = [
        load(k + 3, a, b)
        for k, (a, b) in enumerate(
            (
                (shift, shv), (lb, lbv), (sinit.at[0], siv), (hgain, hgv), (ck, ckv), (cgain, cgv), (cbias, cbv),
            )
        )
    ]

    barrier = pltpu.get_barrier_semaphore()
    partners = [at(z, y + 1), at(z, y - 1), at(z, y + 2), at(z + 1, y), at(z - 1, y), at(z + 2, y)]
    partners += [across(x + 1), across(x - 1), mate, following, preceding]
    for dev in partners:
        pl.semaphore_signal(barrier, inc=1, device_id=dev, device_id_type=MESH)

    @pl.when(jnp.logical_not(home))
    def _():
        pl.semaphore_signal(barrier, inc=1, device_id=swap, device_id_type=MESH)

    def exchange(lane, sizes, view, span):
        return ChipExchange(w, lane, x, across(x + 1), across(x - 1), mate, sizes, view, span)

    def token_view(xx, row, rows):
        return xs.at[pl.ds(pl.multiple_of((xx * 2 + c) * TD + row, 16), rows), :]

    def block_view(buf):
        return lambda xx, row, rows: buf.at[xx * 2 + c, pl.ds(row, rows)]

    def block_span(buf):
        return lambda blocks, rows: buf.at[0, pl.ds(0, rows)] if rows else buf.at[pl.ds(0, blocks)]

    token_ring = exchange(
        1, ((32, 16), (32, 16)), token_view, lambda blocks, rows: xs.at[pl.ds(0, blocks * TD + rows), :]
    )
    conv_ring = exchange(2, ((192, 192), (192, 208)), block_view(mc), block_span(mc))
    rec_ring = exchange(3, ((192, 192), (192, 192)), block_view(mr), block_span(mr))

    def along_y(part):
        return (y, at(z, y + 1), at(z, y - 1), part)

    def along_z(part):
        return (z, at(z + 1, y), at(z - 1, y), part)

    p1, p2 = [], []
    for g in range(6):
        a, b = 2 * g, 2 * g + 1
        rings = [
            along_y(lambda p, h, b=a: wb.at[b, z, p, pl.ds(64 * h, 64)]),
            along_z(lambda p, h, b=b: wb.at[b, p, y, pl.ds(64 * h, 64)]),
        ]
        p1.append(Exchange(w, 0, rings, lambda n, b=a: wb.at[b, 0, pl.ds(0, n)]))
        rings = [
            along_z(lambda p, h, b=a: wb.at[b, p, pl.ds(2 * h, 2)]),
            along_y(lambda p, h, b=b: wb.at[b, pl.ds(2 * h, 2), p]),
        ]
        p2.append(Exchange(w, 8, rings, lambda n, b=a: wb.at[b, pl.ds(0, n)]))

    stz[...] = jnp.zeros_like(stz)
    own.wait()
    pl.semaphore_wait(barrier, len(partners) + jnp.where(home, 0, 1))
    for g in range(3):
        p1[g].start()
    swap_k, y_k, z_k, h_k = (w.new() for _ in range(4))

    def place(i):
        return wb.at[10 + i, swap[0] // 4, lax.rem(swap[0], 4)]

    @pl.when(jnp.logical_not(home))
    def _():
        for i in range(2):
            w.start(4, swap_k, stage.at[i], place(i), swap)

    @pl.when(home)
    def _():
        for i in range(2):
            pltpu.make_async_copy(stage.at[i], wb.at[10 + i, z, y], recv_sem.at[swap_k]).start()

    def swapped():
        @pl.when(jnp.logical_not(home))
        def _():
            w.arrive(swap_k, stage, swap)
            w.left(4, stage, swap)

        @pl.when(home)
        def _():
            pltpu.make_async_copy(stage, stage, recv_sem.at[swap_k]).wait()

    for copy in first:
        copy.wait()
    base = pl.multiple_of(t * TD, 16)

    def normalize(r, _):
        wide = tok[pl.ds(pl.multiple_of(r * 16, 16), 16), :].astype(F32)
        scale = lax.rsqrt(jnp.mean(wide * wide, axis=-1, keepdims=True) + EPS)
        xs[pl.ds(pl.multiple_of(base + r * 16, 16), 16), :] = (wide * scale * gainv[...]).astype(BF16)
        return 0

    lax.fori_loop(0, TD // 16, normalize, 0, unroll=TD // 16)
    token_ring.start()

    def whole(b):
        return wb[b].reshape(2048, 128)

    def project(group, finish, size, starts):
        weight = jnp.concatenate([whole(2 * group), whole(2 * group + 1)], axis=1)

        def tile(r, _):
            start = pl.multiple_of(starts(r), 32)
            rows = pl.ds(start, size)
            finish(start, rows, dot(xs[rows, :], weight))
            return 0

        def run(low, high):
            lax.fori_loop(low, high, tile, 0, unroll=high - low if high - low > 1 else None)

        return run

    def project_all(group, finish):
        project(group, finish, PT, lambda r: r * PT)(0, T // PT)

    def by_ring(r):
        return lax.rem(x + jnp.where(r == 1, 3, jnp.where(r == 2, 1, jnp.where(r == 3, 2, 0))), 4) * XT

    def finish_fi(start, rows, v):
        gate = (1.0 - lbv[...]) * jax.nn.sigmoid(-rounded(v[:, :128]))
        kgb[rows, :] = gate
        cb[rows, :] = jnp.log1p(-gate) + shv[rows, :]
        vb[rows, :] = v[:, 128:].astype(BF16)

    def finish_vg(start, rows, v):
        gated = (rounded(v[:, :128]) * jax.nn.sigmoid(rounded(v[:, 128:]))).astype(BF16)
        ext[pl.ds(pl.multiple_of(start + HALO, 8), XT), :] = gated.astype(F32)

    def finish_qo(start, rows, v):
        raw = rounded(v[:, :128])
        qb[rows, :] = raw * jax.nn.sigmoid(raw)
        raw = rounded(v[:, 128:])
        ogb[rows, :] = raw * jax.nn.sigmoid(raw)

    def finish_gate(buf):
        def finish(start, rows, v):
            buf[rows, :] = jax.nn.sigmoid(rounded(v))

        return finish

    at_or_after = lax.broadcasted_iota(jnp.int32, (L, L), 0) >= lax.broadcasted_iota(jnp.int32, (L, L), 1)
    ones_below = jnp.where(at_or_after, 1.0, 0.0).astype(BF16)

    def pack_block(buf, i, decay, state):
        buf[i, pl.ds(0, HEAD), :] = state.astype(BF16)
        extra = jnp.concatenate([a.astype(F32) for a in two(decay)] + [jnp.zeros((14, HEAD), F32)], axis=0)
        buf[i, pl.ds(HEAD, 16), :] = extra.astype(BF16)

    def block_of(buf, i):
        both = buf[i, pl.ds(HEAD, 16), :].astype(F32)
        return both[0:1, :] + both[1:2, :], buf[i, pl.ds(0, HEAD), :].astype(F32)

    def local_states():
        for i in range(NC):
            rows = pl.ds(i * L, L)
            sides = dot(ones_below, jnp.concatenate(two(cb[rows, :]), axis=1))
            total = sides[:, :128] + sides[:, 128:]
            cb[rows, :] = total
            ending = (kgb[rows, :] * jnp.exp(total[L - 1 : L, :] - total)).astype(BF16)
            kv[i] = dot_first(vb[rows, :], ending)
        state = jnp.zeros((HEAD, HEAD), F32)
        before = jnp.zeros((1, HEAD), F32)
        for i in range(NC):
            last = cb[pl.ds(i * L + L - 1, 1), :]
            stb[i] = state.astype(BF16)
            rbuf[pl.ds(i, 1), :] = before
            state = jnp.exp(last) * state + kv[i]
            before = before + last
        pack_block(sty, y, jnp.exp(before), state)

    def local_outputs():
        for i in range(NC):
            rows = pl.ds(i * L, L)
            total, q = cb[rows, :], qb[rows, :]
            middle = 0.5 * total[L - 1 : L, :]
            left = (q * jnp.exp(total - middle)).astype(BF16)
            right = (kgb[rows, :] * jnp.exp(middle - total)).astype(BF16)
            scores = jnp.where(at_or_after, dot_last(left, right), 0.0).astype(BF16)
            o = dot(scores, vb[rows, :])
            o = o + dot_last((q * jnp.exp(total)).astype(BF16), stb[i])
            head[rows, :] = o
            qd[rows, :] = (q * jnp.exp(total + rbuf[pl.ds(i, 1), :])).astype(BF16)

    def convolve(low, high):
        for i in range(low, high):
            acc = jnp.zeros((128, HEAD), F32)
            for j in range(KW):
                acc = acc + ckv[pl.ds(j, 1), :] * ext[pl.ds(i * 128 + HALO - KW + 1 + j, 128), :]
            mc[t, pl.ds(i * 128, 128), :] = acc.astype(BF16)

    def take_z():
        for i in (1, 2, 3):

            @pl.when(z == i)
            def _(i=i):
                w.arrive(z_k, stz.at[pl.ds(0, i)], at(z + 1, y))

    def chip_weight(b, xx):
        top, low = ([wb[b, xx, 2 * k + j] for j in range(2)] for k in range(2))
        return jnp.concatenate([jnp.concatenate(top, axis=1), jnp.concatenate(low, axis=1)], axis=0)

    def chip_blocks(rows, xx):
        return jnp.concatenate([mr[2 * xx, rows, :], mr[2 * xx + 1, rows, :]], axis=1)

    p1[0].relay()
    p1[1].relay()
    p1[3].start()
    p1[4].start()
    p1[2].relay()
    p1[0].rest()
    p2[0].start()
    p1[1].rest()
    p2[1].first()
    token_ring.relay(0)
    token_ring.relay(1)
    p2[0].relay()
    p2[1].second()
    token_ring.near()
    p1[2].rest()
    p2[1].relay()
    p2[2].first()
    p1[3].relay()
    p1[4].relay()
    swapped()
    p1[5].start()
    for copy in rest:
        copy.wait()
    token_ring.far(0)
    token_ring.far(1)
    p2[0].rest()
    p2[2].second()
    token_ring.mate_near()
    project_vg = project(0, finish_vg, XT, by_ring)
    project_vg(0, 3)
    token_ring.mate_far()
    project_vg(3, 4)
    hsend[...] = ext[pl.ds(T, HALO), :].astype(BF16)
    w.start(5, h_k, hsend, hrecv, following)
    p2[1].rest()
    project_all(1, finish_fi)
    local_states()
    for i in (2, 1, 3):
        w.start(6, y_k, sty.at[y], sty.at[y], at(z, y + i))

    p2[2].relay()
    p1[3].rest()
    p1[5].relay()
    p2[3].start()
    convolve(1, T // 128)
    extra = [a.astype(F32) for v in (cgv[...], cbv[...]) for a in two(v)]
    mc[t, pl.ds(T, 16), :] = jnp.concatenate(extra + [jnp.zeros((12, HEAD), F32)], axis=0).astype(BF16)
    w.arrive(h_k, hrecv, preceding)
    ext[pl.ds(0, HALO), :] = jnp.where(s > 0, hrecv[...].astype(F32), 0.0)
    convolve(0, 1)
    conv_ring.start()
    w.arrive(y_k, sty.at[pl.ds(0, 3)], at(z, y + 1))
    row_decay, row_state = jnp.ones((1, HEAD), F32), jnp.zeros((HEAD, HEAD), F32)
    my_decay, my_state = row_decay, row_state
    for i in range(4):
        d, v = block_of(sty, i)
        row_decay, row_state = row_decay * d, d * row_state + v
        if i < 3:
            take = i < y
            my_decay = jnp.where(take, row_decay, my_decay)
            my_state = jnp.where(take, row_state, my_state)
    pack_block(stz, z, row_decay, row_state)
    for i in (2, 1, 3):

        @pl.when(z + i < 4)
        def _(i=i):
            w.start(7, z_k, stz.at[z], stz.at[z], at(z + i, y))


    p1[4].rest()
    p2[4].first()
    p2[2].rest()
    project_all(2, finish_qo)
    conv_ring.relay(0)
    conv_ring.relay(1)
    p2[3].relay()
    p2[4].second()
    local_outputs()
    p1[5].rest()
    p2[5].start()
    take_z()
    entering = siv[...].T
    for i in range(3):
        d, v = block_of(stz, i)
        entering = jnp.where(i < z, d * entering + v, entering)
    entering = (my_decay * entering + my_state).astype(BF16)

    def finish_head(low, high):
        for r in range(low, high):
            rows = pl.ds(r * 128, 128)
            h = head[rows, :] + dot_last(qd[rows, :], entering)
            h = h * lax.rsqrt(jnp.mean(h * h, axis=-1, keepdims=True) + EPS) * hgv[...]
            mr[t, rows, :] = (h * ogb[rows, :]).astype(BF16)

    finish_head(0, T // 128)
    rec_ring.start()
    conv_ring.near()
    p2[4].relay()
    conv_ring.far(0)
    conv_ring.far(1)
    p2[3].rest()
    project_gr = project(3, finish_gate(sgr), PT, lambda r: r * PT)
    project_gr(0, 1)
    rec_ring.relay(0)
    conv_ring.mate_near()
    conv_ring.mate_far()

    def conv_scale(r, _):
        rows = pl.ds(pl.multiple_of(r * 64, 64), 64)
        squares = sum(v * v for v in (mc[k, rows, :].astype(F32) for k in range(8)))
        scale = lax.rsqrt(jnp.sum(squares, axis=-1, keepdims=True) * (1.0 / CONV) + EPS)
        scales[rows, :] = jnp.broadcast_to(scale, (64, 128))
        return 0

    gains, biases = [], []
    for k in range(8):
        four = mc[k, pl.ds(T, 16), :].astype(F32)
        gains.append(0.5 * (four[0:1, :] + four[1:2, :]))
        biases.append(0.5 * (four[2:3, :] + four[3:4, :]))

    def normalize_conv(r, _):
        rows = pl.ds(pl.multiple_of(r * 64, 64), 64)
        scale = scales[rows, :]
        for k in range(8):
            half = mc[k, rows, :].astype(F32) * scale * gains[k] + biases[k]
            mcn[rows, pl.ds(k * 128, 128)] = (half + half * jnp.tanh(half)).astype(BF16)
        return 0

    lax.fori_loop(0, T // 64, conv_scale, 0, unroll=4)
    rec_ring.relay(1)
    p2[5].relay()
    project_gr(1, 2)
    lax.fori_loop(0, T // 64, normalize_conv, 0, unroll=2)
    rec_ring.near()
    p2[4].rest()
    project_all(4, finish_gate(sgc))
    rec_ring.far(0)
    rec_ring.far(1)
    p2[5].rest()
    w_conv = jnp.concatenate([chip_weight(11, xx) for xx in range(4)], axis=0)

    def conv_tile(r, _):
        rows = pl.ds(pl.multiple_of(r * PT, PT), PT)
        sgc[rows, :] = sgc[rows, :] * rounded(dot(mcn[rows, :], w_conv))
        return 0

    lax.fori_loop(0, T // PT, conv_tile, 0, unroll=2)
    rec_ring.mate_near()
    near = [x, lax.rem(x + 1, 4), lax.rem(x + 3, 4)]
    w_near = jnp.concatenate([chip_weight(10, xx) for xx in near], axis=0)

    def near_tile(r, _):
        rows = pl.ds(pl.multiple_of(r * PT, PT), PT)
        acc[rows, :] = dot(jnp.concatenate([chip_blocks(rows, xx) for xx in near], axis=1), w_near)
        return 0

    lax.fori_loop(0, T // PT, near_tile, 0, unroll=2)
    rec_ring.mate_far()
    opposite = lax.rem(x + 2, 4)
    w_far = chip_weight(10, opposite)

    def last_tile(r, _):
        rows = pl.ds(pl.multiple_of(r * RT, RT), RT)
        y_rec = rounded(acc[rows, :] + dot(chip_blocks(rows, opposite), w_far))
        out[rows, :] = (sgr[rows, :] * y_rec + sgc[rows, :]).astype(BF16)
        return 0

    lax.fori_loop(0, T // RT, last_tile, 0, unroll=3)
    w.left(0, wb.at[pl.ds(0, 3), pl.ds(0, 3)], mate)
    w.left(8, wb.at[pl.ds(0, 9)], mate)
    w.left(1, xs.at[pl.ds(0, 7 * TD), :], mate)
    w.left(2, mc.at[pl.ds(0, 7)], mate)
    w.left(3, mr.at[pl.ds(0, 7)], mate)
    w.left(5, hsend, following)
    w.left(6, sty.at[pl.ds(0, 3)], mate)
    for i in (1, 2, 3):

        @pl.when(z == 3 - i)
        def _(i=i):
            w.left(7, stz.at[pl.ds(0, i)], mate)


def local(
    tokens, norm_gain, w_query, w_forget, w_input, w_outgate, w_conv_value, w_conv_gate, w_gate_rec, w_gate_conv,
    lower_bound, decay_shift, state_init, head_gain, conv_kernel, channel_gain, channel_bias, w_out_rec, w_out_conv,
):
    line = lambda v: v.reshape(1, -1)
    args = (
        tokens, line(norm_gain), w_forget, w_input, w_query, w_outgate, w_conv_value, w_conv_gate, w_gate_rec,
        w_gate_conv, line(lower_bound), decay_shift, state_init, line(head_gain), conv_kernel, line(channel_gain),
        line(channel_bias), w_out_rec, w_out_conv,
    )
    v = pltpu.VMEM
    scratch = [
        v((TD, 2048), BF16), v((1, 2048), F32), v((T, 2048), BF16), v((12, 4, 4, 128, 128), BF16),
        v((2, 128, 128), BF16), v((1, 128), F32), v((T, 128), F32), v((128, 128), F32), v((1, 128), F32),
        v((KW, 128), F32), v((1, 128), F32), v((1, 128), F32),
        v((T, 128), F32), v((T, 128), F32), v((T, 128), BF16), v((T, 128), F32), v((T, 128), F32),
        v((T + HALO, 128), F32), v((HALO, 128), BF16), v((HALO, 128), BF16), v((T, 256), F32), v((T, 256), F32),
        v((8, T + 16, 128), BF16), v((T, CONV), BF16), v((8, T, 128), BF16), v((T, 128), F32), v((T, 128), BF16),
        v((NC, 128, 128), BF16), v((16, 128), F32), v((4, 144, 128), BF16), v((4, 144, 128), BF16), v((NC, 128, 128), F32), v((T, 128), F32), v((T, 256), F32),
        pltpu.SemaphoreType.DMA((10,)), pltpu.SemaphoreType.DMA((9,)), pltpu.SemaphoreType.DMA((49,)),
    ]
    return pl.pallas_call(
        kernel,
        out_shape=jax.ShapeDtypeStruct((T, 256), BF16),
        in_specs=[pl.BlockSpec(memory_space=pltpu.HBM)] * len(args),
        out_specs=pl.BlockSpec(memory_space=pltpu.VMEM),
        scratch_shapes=scratch,
        compiler_params=pltpu.CompilerParams(
            collective_id=0, has_side_effects=True, vmem_limit_bytes=40 * 1024 * 1024
        ),
    )(*[pltpu.with_memory_space_constraint(a, pltpu.HBM) for a in args])


def solution(mesh):
    both = P("sp", "tp")
    in_specs = (
        P(("sp", "tp"), None), P(), both, both, both, both, both, both, both, both, P("tp"), both,
        P("tp", None, None), P("tp"), P(None, "tp"), P("tp"), P("tp"), P("tp", "sp"), P("tp", "sp"),
    )
    return jax.shard_map(local, mesh=mesh, in_specs=in_specs, out_specs=both, check_vma=False)
```

```python
import functools

import jax
import jax.numpy as jnp
from jax import lax
from jax.experimental import pallas as pl
from jax.experimental.pallas import tpu as pltpu
from jax.sharding import PartitionSpec as P

MESH = pl.DeviceIdType.MESH
F32 = jnp.float32
BF16 = jnp.bfloat16
HEAD = 128
CONV = 1024
KW = 31
EPS = 1e-06
L = 64
T = 768
NC = T // L
TD = 96
RT = 256
XT = 192
PT = 384
HALO = 32


class Wires:
    def __init__(self, send_sem, recv_sem):
        self.send_sem, self.recv_sem = send_sem, recv_sem
        self.count = 0

    def new(self):
        self.count += 1
        return self.count - 1

    def make(self, lane, k, src, dst, dev):
        return pltpu.make_async_remote_copy(
            src_ref=src,
            dst_ref=dst,
            send_sem=self.send_sem.at[lane],
            recv_sem=self.recv_sem.at[k],
            device_id=dev,
            device_id_type=MESH,
        )

    def start(self, lane, k, src, dst, dev):
        self.make(lane, k, src, dst, dev).start()

    def arrive(self, k, span, dev):
        self.make(0, k, span, span, dev).wait_recv()

    def left(self, lane, span, dev):
        self.make(lane, 0, span, span, dev).wait_send()


class Exchange:
    def __init__(self, wires, lane, rings, span):
        self.w, self.lane, self.rings, self.span = wires, lane, rings, span
        self.k = {"relay": wires.new(), "rest": wires.new()}

    def go(self, sem, view, dev):
        self.w.start(self.lane, self.k[sem], view, view, dev)

    def await_blocks(self, sem, n):
        self.w.arrive(self.k[sem], self.span(n * len(self.rings)), self.rings[0][1])

    def first(self):
        for pos, plus, minus, part in self.rings:
            self.go("relay", part(pos, 0), plus)
            self.go("relay", part(pos, 1), minus)

    def second(self):
        for pos, plus, minus, part in self.rings:
            self.go("rest", part(pos, 1), plus)
            self.go("rest", part(pos, 0), minus)

    def start(self):
        self.first()
        self.second()

    def relay(self):
        self.await_blocks("relay", 1)
        for pos, plus, minus, part in self.rings:
            self.go("rest", part(lax.rem(pos + 3, 4), 0), plus)
            self.go("rest", part(lax.rem(pos + 1, 4), 1), minus)

    def rest(self):
        self.await_blocks("rest", 2)


class ChipExchange:
    def __init__(self, wires, lane, pos, plus, minus, mate, sizes, view, span):
        self.w, self.lane, self.pos, self.plus, self.minus, self.mate = wires, lane, pos, plus, minus, mate
        self.sizes, self.view, self.span = sizes, view, span
        self.k = {n: wires.new() for n in ("relay0", "relay1", "near", "far0", "far1", "mate_near", "mate_far")}

    def piece(self, shift, half, i):
        row = sum(self.sizes[0]) * half + (self.sizes[half][0] if i else 0)
        return self.view(lax.rem(self.pos + shift, 4), row, self.sizes[half][i])

    def half(self, shift, half):
        return self.view(lax.rem(self.pos + shift, 4), sum(self.sizes[0]) * half, sum(self.sizes[half]))

    def go(self, sem, view, dev):
        self.w.start(self.lane, self.k[sem], view, view, dev)

    def take(self, sem, blocks, rows, dev):
        self.w.arrive(self.k[sem], self.span(blocks, rows), dev)

    def rows(self, i):
        return self.sizes[0][i] + self.sizes[1][i]

    def start(self):
        for i in range(2):
            self.go(f"relay{i}", self.piece(0, 0, i), self.plus)
            self.go(f"relay{i}", self.piece(0, 1, i), self.minus)
        self.go("near", self.half(0, 1), self.plus)
        self.go("near", self.half(0, 0), self.minus)
        for h in range(2):
            self.go("mate_near", self.half(0, h), self.mate)

    def relay(self, i):
        self.take(f"relay{i}", 0, self.rows(i), self.plus)
        left, right = self.piece(3, 0, i), self.piece(1, 1, i)
        self.go(f"far{i}", left, self.plus)
        self.go(f"far{i}", right, self.minus)
        self.go("mate_near", left, self.mate)
        self.go("mate_near", right, self.mate)

    def near(self):
        self.take("near", 1, 0, self.plus)
        self.go("mate_near", self.half(3, 1), self.mate)
        self.go("mate_near", self.half(1, 0), self.mate)

    def far(self, i):
        self.take(f"far{i}", 0, self.rows(i), self.plus)
        self.go("mate_far", self.piece(2, 0, i), self.mate)
        self.go("mate_far", self.piece(2, 1, i), self.mate)

    def mate_near(self):
        self.take("mate_near", 3, 0, self.mate)

    def mate_far(self):
        self.take("mate_far", 1, 0, self.mate)


def dot(a, b):
    return jnp.dot(a, b, preferred_element_type=F32)


def dot_last(a, b):
    return lax.dot_general(a, b, (((1,), (1,)), ((), ())), preferred_element_type=F32)


def dot_first(a, b):
    return lax.dot_general(a, b, (((0,), (0,)), ((), ())), preferred_element_type=F32)


def rounded(v):
    return v.astype(BF16).astype(F32)


def two(v):
    high = v.astype(BF16)
    return high, (v - high.astype(F32)).astype(BF16)


def kernel(
    tokens, gain, w_f, w_i, w_q, w_o, w_v, w_g, w_gr, w_gc, lb, shift, sinit, hgain, ck, cgain, cbias, w_or, w_oc,
    out,
    tok, gainv, xs, wb, stage, lbv, shv, siv, hgv, ckv, cgv, cbv,
    kgb, cb, vb, qb, ogb, ext, hsend, hrecv, sgr, sgc, mc, mcn, mr, head, qd, stb, rbuf, sty, stz, kv, scales, acc,
    load_sem, send_sem, recv_sem,
):
    s, t = lax.axis_index("sp"), lax.axis_index("tp")
    z, y, x, c = s // 4, lax.rem(s, 4), t // 2, lax.rem(t, 2)
    w = Wires(send_sem, recv_sem)

    def at(zz, yy):
        return (lax.rem(zz + 4, 4) * 4 + lax.rem(yy + 4, 4), t)

    def across(xx):
        return (s, lax.rem(xx + 4, 4) * 2 + c)

    mate = (s, 1 - c + 2 * x)
    swap = (2 * t + lax.rem(s, 2), s // 2)
    home = s // 2 == t
    following, preceding = (lax.rem(s + 1, 16), t), (lax.rem(s + 15, 16), t)

    def load(k, src, dst):
        copy = pltpu.make_async_copy(src, dst, load_sem.at[k])
        copy.start()
        return copy

    first = [load(0, tokens, tok), load(1, gain, gainv)]
    for b, src in enumerate(
        (
            w_v, w_g, w_f, w_i, w_q, w_o,
            w_gr.at[:, pl.ds(0, 128)], w_gr.at[:, pl.ds(128, 128)],
            w_gc.at[:, pl.ds(0, 128)], w_gc.at[:, pl.ds(128, 128)],
        )
    ):
        load(2, src, wb.at[b, z, y])
    load(2, w_or, stage.at[0])
    load(2, w_oc, stage.at[1])
    twelve = wb.at[0, pl.ds(0, 3)]
    own = pltpu.make_async_copy(twelve, twelve, load_sem.at[2])
    rest = [
        load(k + 3, a, b)
        for k, (a, b) in enumerate(
            (
                (shift, shv), (lb, lbv), (sinit.at[0], siv), (hgain, hgv), (ck, ckv), (cgain, cgv), (cbias, cbv),
            )
        )
    ]

    barrier = pltpu.get_barrier_semaphore()
    partners = [at(z, y + 1), at(z, y - 1), at(z + 1, y), at(z - 1, y), across(x + 1), across(x - 1), mate]
    for dev in partners:
        pl.semaphore_signal(barrier, inc=1, device_id=dev, device_id_type=MESH)

    for there, dev in ((s < 15, following), (s > 0, preceding)):

        @pl.when(there)
        def _(dev=dev):
            pl.semaphore_signal(barrier, inc=1, device_id=dev, device_id_type=MESH)

    @pl.when(jnp.logical_not(home))
    def _():
        pl.semaphore_signal(barrier, inc=1, device_id=swap, device_id_type=MESH)

    def exchange(lane, sizes, view, span):
        return ChipExchange(w, lane, x, across(x + 1), across(x - 1), mate, sizes, view, span)

    def token_view(xx, row, rows):
        return xs.at[pl.ds(pl.multiple_of((xx * 2 + c) * TD + row, 16), rows), :]

    def block_view(buf):
        return lambda xx, row, rows: buf.at[xx * 2 + c, pl.ds(row, rows)]

    def block_span(buf):
        return lambda blocks, rows: buf.at[0, pl.ds(0, rows)] if rows else buf.at[pl.ds(0, blocks)]

    token_ring = exchange(
        1, ((32, 16), (32, 16)), token_view, lambda blocks, rows: xs.at[pl.ds(0, blocks * TD + rows), :]
    )
    conv_ring = exchange(2, ((192, 192), (192, 208)), block_view(mc), block_span(mc))
    rec_ring = exchange(3, ((192, 192), (192, 192)), block_view(mr), block_span(mr))

    def along_y(part):
        return (y, at(z, y + 1), at(z, y - 1), part)

    def along_z(part):
        return (z, at(z + 1, y), at(z - 1, y), part)

    p1, p2 = [], []
    for g in range(6):
        a, b = 2 * g, 2 * g + 1
        rings = [
            along_y(lambda p, h, b=a: wb.at[b, z, p, pl.ds(64 * h, 64)]),
            along_z(lambda p, h, b=b: wb.at[b, p, y, pl.ds(64 * h, 64)]),
        ]
        p1.append(Exchange(w, 0, rings, lambda n, b=a: wb.at[b, 0, pl.ds(0, n)]))
        rings = [
            along_z(lambda p, h, b=a: wb.at[b, p, pl.ds(2 * h, 2)]),
            along_y(lambda p, h, b=b: wb.at[b, pl.ds(2 * h, 2), p]),
        ]
        p2.append(Exchange(w, 8, rings, lambda n, b=a: wb.at[b, pl.ds(0, n)]))

    stz[...] = jnp.zeros_like(stz)
    own.wait()
    count = len(partners) + jnp.where(home, 0, 1) + jnp.where(s < 15, 1, 0) + jnp.where(s > 0, 1, 0)
    pl.semaphore_wait(barrier, count)
    for g in range(3):
        p1[g].start()
    swap_k, y_k, z_k, h_k = (w.new() for _ in range(4))

    def place(i):
        return wb.at[10 + i, swap[0] // 4, lax.rem(swap[0], 4)]

    @pl.when(jnp.logical_not(home))
    def _():
        for i in range(2):
            w.start(4, swap_k, stage.at[i], place(i), swap)

    @pl.when(home)
    def _():
        for i in range(2):
            pltpu.make_async_copy(stage.at[i], wb.at[10 + i, z, y], recv_sem.at[swap_k]).start()

    def swapped():
        @pl.when(jnp.logical_not(home))
        def _():
            w.arrive(swap_k, stage, swap)
            w.left(4, stage, swap)

        @pl.when(home)
        def _():
            pltpu.make_async_copy(stage, stage, recv_sem.at[swap_k]).wait()

    for copy in first:
        copy.wait()
    base = pl.multiple_of(t * TD, 16)

    def normalize(r, _):
        wide = tok[pl.ds(pl.multiple_of(r * 16, 16), 16), :].astype(F32)
        scale = lax.rsqrt(jnp.mean(wide * wide, axis=-1, keepdims=True) + EPS)
        xs[pl.ds(pl.multiple_of(base + r * 16, 16), 16), :] = (wide * scale * gainv[...]).astype(BF16)
        return 0

    lax.fori_loop(0, TD // 16, normalize, 0, unroll=TD // 16)
    token_ring.start()

    def whole(b):
        return wb[b].reshape(2048, 128)

    def project(group, finish, size, starts):
        weight = jnp.concatenate([whole(2 * group), whole(2 * group + 1)], axis=1)

        def tile(r, _):
            start = pl.multiple_of(starts(r), 32)
            rows = pl.ds(start, size)
            finish(start, rows, dot(xs[rows, :], weight))
            return 0

        def run(low, high):
            lax.fori_loop(low, high, tile, 0, unroll=high - low if high - low > 1 else None)

        return run

    def project_all(group, finish):
        project(group, finish, PT, lambda r: r * PT)(0, T // PT)

    def by_ring(r):
        return lax.rem(x + jnp.where(r == 1, 3, jnp.where(r == 2, 1, jnp.where(r == 3, 2, 0))), 4) * XT

    def finish_fi(start, rows, v):
        gate = (1.0 - lbv[...]) * jax.nn.sigmoid(-rounded(v[:, :128]))
        kgb[rows, :] = gate
        cb[rows, :] = jnp.log1p(-gate) + shv[rows, :]
        vb[rows, :] = v[:, 128:].astype(BF16)

    def finish_vg(start, rows, v):
        gated = (rounded(v[:, :128]) * jax.nn.sigmoid(rounded(v[:, 128:]))).astype(BF16)
        ext[pl.ds(pl.multiple_of(start + HALO, 8), XT), :] = gated.astype(F32)

    def finish_qo(start, rows, v):
        raw = rounded(v[:, :128])
        qb[rows, :] = raw * jax.nn.sigmoid(raw)
        raw = rounded(v[:, 128:])
        ogb[rows, :] = raw * jax.nn.sigmoid(raw)

    def finish_gate(buf):
        def finish(start, rows, v):
            buf[rows, :] = jax.nn.sigmoid(rounded(v))

        return finish

    at_or_after = lax.broadcasted_iota(jnp.int32, (L, L), 0) >= lax.broadcasted_iota(jnp.int32, (L, L), 1)
    ones_below = jnp.where(at_or_after, 1.0, 0.0).astype(BF16)

    def pack_block(buf, i, decay, state):
        buf[i, pl.ds(0, HEAD), :] = state.astype(BF16)
        extra = jnp.concatenate([a.astype(F32) for a in two(decay)] + [jnp.zeros((14, HEAD), F32)], axis=0)
        buf[i, pl.ds(HEAD, 16), :] = extra.astype(BF16)

    def block_of(buf, i):
        both = buf[i, pl.ds(HEAD, 16), :].astype(F32)
        return both[0:1, :] + both[1:2, :], buf[i, pl.ds(0, HEAD), :].astype(F32)

    def local_states():
        for i in range(NC):
            rows = pl.ds(i * L, L)
            sides = dot(ones_below, jnp.concatenate(two(cb[rows, :]), axis=1))
            total = sides[:, :128] + sides[:, 128:]
            cb[rows, :] = total
            ending = (kgb[rows, :] * jnp.exp(total[L - 1 : L, :] - total)).astype(BF16)
            kv[i] = dot_first(vb[rows, :], ending)
        state = jnp.zeros((HEAD, HEAD), F32)
        before = jnp.zeros((1, HEAD), F32)
        for i in range(NC):
            last = cb[pl.ds(i * L + L - 1, 1), :]
            stb[i] = state.astype(BF16)
            rbuf[pl.ds(i, 1), :] = before
            state = jnp.exp(last) * state + kv[i]
            before = before + last
        pack_block(sty, y, jnp.exp(before), state)

    def local_outputs():
        for i in range(NC):
            rows = pl.ds(i * L, L)
            total, q = cb[rows, :], qb[rows, :]
            middle = 0.5 * total[L - 1 : L, :]
            left = (q * jnp.exp(total - middle)).astype(BF16)
            right = (kgb[rows, :] * jnp.exp(middle - total)).astype(BF16)
            scores = jnp.where(at_or_after, dot_last(left, right), 0.0).astype(BF16)
            o = dot(scores, vb[rows, :])
            o = o + dot_last((q * jnp.exp(total)).astype(BF16), stb[i])
            head[rows, :] = o
            qd[rows, :] = (q * jnp.exp(total + rbuf[pl.ds(i, 1), :])).astype(BF16)

    def convolve(low, high):
        for i in range(low, high):
            acc = jnp.zeros((128, HEAD), F32)
            for j in range(KW):
                acc = acc + ckv[pl.ds(j, 1), :] * ext[pl.ds(i * 128 + HALO - KW + 1 + j, 128), :]
            mc[t, pl.ds(i * 128, 128), :] = acc.astype(BF16)

    def take_halo():
        @pl.when(s > 0)
        def _():
            w.arrive(h_k, hrecv, preceding)
            ext[pl.ds(0, HALO), :] = hrecv[...].astype(F32)

        @pl.when(s == 0)
        def _():
            ext[pl.ds(0, HALO), :] = jnp.zeros((HALO, HEAD), F32)

    def take_z():
        for i in (1, 2, 3):

            @pl.when(z == i)
            def _(i=i):
                w.arrive(z_k, stz.at[pl.ds(0, i)], at(z + 1, y))

    def chip_weight(b, xx):
        top, low = ([wb[b, xx, 2 * k + j] for j in range(2)] for k in range(2))
        return jnp.concatenate([jnp.concatenate(top, axis=1), jnp.concatenate(low, axis=1)], axis=0)

    def chip_blocks(rows, xx):
        return jnp.concatenate([mr[2 * xx, rows, :], mr[2 * xx + 1, rows, :]], axis=1)

    p1[0].relay()
    p1[1].relay()
    p1[3].start()
    p1[4].start()
    p1[2].relay()
    p1[0].rest()
    p2[0].start()
    p1[1].rest()
    p2[1].first()
    token_ring.relay(0)
    token_ring.relay(1)
    p2[0].relay()
    p2[1].second()
    token_ring.near()
    p1[2].rest()
    p2[1].relay()
    p2[2].first()
    p1[3].relay()
    p1[4].relay()
    swapped()
    p1[5].start()
    for copy in rest:
        copy.wait()
    token_ring.far(0)
    token_ring.far(1)
    p2[0].rest()
    p2[2].second()
    token_ring.mate_near()
    project_vg = project(0, finish_vg, XT, by_ring)
    project_vg(0, 3)
    token_ring.mate_far()
    project_vg(3, 4)
    hsend[...] = ext[pl.ds(T, HALO), :].astype(BF16)

    @pl.when(s < 15)
    def _():
        w.start(5, h_k, hsend, hrecv, following)

    p2[1].rest()
    project_all(1, finish_fi)
    local_states()
    for i in (2, 1, 3):
        w.start(6, y_k, sty.at[y], sty.at[y], at(z, y + i))

    p2[2].relay()
    p1[3].rest()
    p1[5].relay()
    p2[3].start()
    convolve(1, T // 128)
    extra = [a.astype(F32) for v in (cgv[...], cbv[...]) for a in two(v)]
    mc[t, pl.ds(T, 16), :] = jnp.concatenate(extra + [jnp.zeros((12, HEAD), F32)], axis=0).astype(BF16)
    take_halo()
    convolve(0, 1)
    conv_ring.start()
    w.arrive(y_k, sty.at[pl.ds(0, 3)], at(z, y + 1))
    row_decay, row_state = jnp.ones((1, HEAD), F32), jnp.zeros((HEAD, HEAD), F32)
    my_decay, my_state = row_decay, row_state
    for i in range(4):
        d, v = block_of(sty, i)
        row_decay, row_state = row_decay * d, d * row_state + v
        if i < 3:
            take = i < y
            my_decay = jnp.where(take, row_decay, my_decay)
            my_state = jnp.where(take, row_state, my_state)
    pack_block(stz, z, row_decay, row_state)
    for i in (2, 1, 3):

        @pl.when(z + i < 4)
        def _(i=i):
            w.start(7, z_k, stz.at[z], stz.at[z], at(z + i, y))


    p1[5].rest()
    p2[5].first()
    p2[2].rest()
    project_all(2, finish_qo)
    conv_ring.relay(0)
    conv_ring.relay(1)
    p2[3].relay()
    p2[5].second()
    local_outputs()
    p1[4].rest()
    p2[4].start()
    take_z()
    entering = siv[...].T
    for i in range(3):
        d, v = block_of(stz, i)
        entering = jnp.where(i < z, d * entering + v, entering)
    entering = (my_decay * entering + my_state).astype(BF16)

    def finish_head(low, high):
        for r in range(low, high):
            rows = pl.ds(r * 128, 128)
            h = head[rows, :] + dot_last(qd[rows, :], entering)
            h = h * lax.rsqrt(jnp.mean(h * h, axis=-1, keepdims=True) + EPS) * hgv[...]
            mr[t, rows, :] = (h * ogb[rows, :]).astype(BF16)

    finish_head(0, T // 128)
    rec_ring.start()
    conv_ring.near()
    p2[5].relay()
    conv_ring.far(0)
    conv_ring.far(1)
    rec_ring.relay(0)
    conv_ring.mate_near()
    conv_ring.mate_far()

    def conv_scale(r, _):
        rows = pl.ds(pl.multiple_of(r * 64, 64), 64)
        squares = sum(v * v for v in (mc[k, rows, :].astype(F32) for k in range(8)))
        scale = lax.rsqrt(jnp.sum(squares, axis=-1, keepdims=True) * (1.0 / CONV) + EPS)
        scales[rows, :] = jnp.broadcast_to(scale, (64, 128))
        return 0

    gains, biases = [], []
    for k in range(8):
        four = mc[k, pl.ds(T, 16), :].astype(F32)
        gains.append(0.5 * (four[0:1, :] + four[1:2, :]))
        biases.append(0.5 * (four[2:3, :] + four[3:4, :]))

    def normalize_conv(r, _):
        rows = pl.ds(pl.multiple_of(r * 64, 64), 64)
        scale = scales[rows, :]
        for k in range(8):
            half = mc[k, rows, :].astype(F32) * scale * gains[k] + biases[k]
            mcn[rows, pl.ds(k * 128, 128)] = (half + half * jnp.tanh(half)).astype(BF16)
        return 0

    lax.fori_loop(0, T // 64, conv_scale, 0, unroll=4)
    rec_ring.relay(1)
    p2[4].relay()
    p2[3].rest()
    project_all(3, finish_gate(sgr))
    rec_ring.near()
    lax.fori_loop(0, T // 64, normalize_conv, 0, unroll=2)
    p2[5].rest()
    w_conv = jnp.concatenate([chip_weight(11, xx) for xx in range(4)], axis=0)

    def conv_tile(r, _):
        rows = pl.ds(pl.multiple_of(r * PT, PT), PT)
        sgc[rows, :] = rounded(dot(mcn[rows, :], w_conv))
        return 0

    lax.fori_loop(0, T // PT, conv_tile, 0, unroll=2)
    rec_ring.far(0)
    rec_ring.far(1)
    rec_ring.mate_near()
    near = [x, lax.rem(x + 1, 4), lax.rem(x + 3, 4)]
    w_near = jnp.concatenate([chip_weight(10, xx) for xx in near], axis=0)

    def near_tile(r, _):
        rows = pl.ds(pl.multiple_of(r * PT, PT), PT)
        acc[rows, :] = dot(jnp.concatenate([chip_blocks(rows, xx) for xx in near], axis=1), w_near)
        return 0

    lax.fori_loop(0, T // PT, near_tile, 0, unroll=2)
    p2[4].rest()

    def finish_gc(start, rows, v):
        sgc[rows, :] = jax.nn.sigmoid(rounded(v)) * sgc[rows, :]

    project_all(4, finish_gc)
    rec_ring.mate_far()
    opposite = lax.rem(x + 2, 4)
    w_far = chip_weight(10, opposite)

    def last_tile(r, _):
        rows = pl.ds(pl.multiple_of(r * RT, RT), RT)
        y_rec = rounded(acc[rows, :] + dot(chip_blocks(rows, opposite), w_far))
        out[rows, :] = (sgr[rows, :] * y_rec + sgc[rows, :]).astype(BF16)
        return 0

    lax.fori_loop(0, T // RT, last_tile, 0, unroll=3)
    w.left(0, wb.at[pl.ds(0, 3), pl.ds(0, 3)], mate)
    w.left(8, wb.at[pl.ds(0, 9)], mate)
    w.left(1, xs.at[pl.ds(0, 7 * TD), :], mate)
    w.left(2, mc.at[pl.ds(0, 7)], mate)
    w.left(3, mr.at[pl.ds(0, 7)], mate)

    @pl.when(s < 15)
    def _():
        w.left(5, hsend, following)

    w.left(6, sty.at[pl.ds(0, 3)], mate)
    for i in (1, 2, 3):

        @pl.when(z == 3 - i)
        def _(i=i):
            w.left(7, stz.at[pl.ds(0, i)], mate)


def local(
    tokens, norm_gain, w_query, w_forget, w_input, w_outgate, w_conv_value, w_conv_gate, w_gate_rec, w_gate_conv,
    lower_bound, decay_shift, state_init, head_gain, conv_kernel, channel_gain, channel_bias, w_out_rec, w_out_conv,
):
    line = lambda v: v.reshape(1, -1)
    args = (
        tokens, line(norm_gain), w_forget, w_input, w_query, w_outgate, w_conv_value, w_conv_gate, w_gate_rec,
        w_gate_conv, line(lower_bound), decay_shift, state_init, line(head_gain), conv_kernel, line(channel_gain),
        line(channel_bias), w_out_rec, w_out_conv,
    )
    v = pltpu.VMEM
    scratch = [
        v((TD, 2048), BF16), v((1, 2048), F32), v((T, 2048), BF16), v((12, 4, 4, 128, 128), BF16),
        v((2, 128, 128), BF16), v((1, 128), F32), v((T, 128), F32), v((128, 128), F32), v((1, 128), F32),
        v((KW, 128), F32), v((1, 128), F32), v((1, 128), F32),
        v((T, 128), F32), v((T, 128), F32), v((T, 128), BF16), v((T, 128), F32), v((T, 128), F32),
        v((T + HALO, 128), F32), v((HALO, 128), BF16), v((HALO, 128), BF16), v((T, 256), F32), v((T, 256), F32),
        v((8, T + 16, 128), BF16), v((T, CONV), BF16), v((8, T, 128), BF16), v((T, 128), F32), v((T, 128), BF16),
        v((NC, 128, 128), BF16), v((16, 128), F32), v((4, 144, 128), BF16), v((4, 144, 128), BF16), v((NC, 128, 128), F32), v((T, 128), F32), v((T, 256), F32),
        pltpu.SemaphoreType.DMA((10,)), pltpu.SemaphoreType.DMA((9,)), pltpu.SemaphoreType.DMA((49,)),
    ]
    return pl.pallas_call(
        kernel,
        out_shape=jax.ShapeDtypeStruct((T, 256), BF16),
        in_specs=[pl.BlockSpec(memory_space=pltpu.HBM)] * len(args),
        out_specs=pl.BlockSpec(memory_space=pltpu.VMEM),
        scratch_shapes=scratch,
        compiler_params=pltpu.CompilerParams(
            collective_id=0, has_side_effects=True, vmem_limit_bytes=40 * 1024 * 1024
        ),
    )(*[pltpu.with_memory_space_constraint(a, pltpu.HBM) for a in args])


def solution(mesh):
    both = P("sp", "tp")
    in_specs = (
        P(("sp", "tp"), None), P(), both, both, both, both, both, both, both, both, P("tp"), both,
        P("tp", None, None), P("tp"), P(None, "tp"), P("tp"), P("tp"), P("tp", "sp"), P("tp", "sp"),
    )
    return jax.shard_map(local, mesh=mesh, in_specs=in_specs, out_specs=both, check_vma=False)
```

```python
import functools

import jax
import jax.numpy as jnp
from jax import lax
from jax.experimental import pallas as pl
from jax.experimental.pallas import tpu as pltpu
from jax.sharding import PartitionSpec as P

MESH = pl.DeviceIdType.MESH
F32 = jnp.float32
BF16 = jnp.bfloat16
HEAD = 128
CONV = 1024
KW = 31
EPS = 1e-06
L = 64
T = 768
NC = T // L
TD = 96
RT = 256
XT = 192
PT = 384
HALO = 32


class Wires:
    def __init__(self, send_sem, recv_sem):
        self.send_sem, self.recv_sem = send_sem, recv_sem
        self.count = 0

    def new(self):
        self.count += 1
        return self.count - 1

    def make(self, lane, k, src, dst, dev):
        return pltpu.make_async_remote_copy(
            src_ref=src,
            dst_ref=dst,
            send_sem=self.send_sem.at[lane],
            recv_sem=self.recv_sem.at[k],
            device_id=dev,
            device_id_type=MESH,
        )

    def start(self, lane, k, src, dst, dev):
        self.make(lane, k, src, dst, dev).start()

    def arrive(self, k, span, dev):
        self.make(0, k, span, span, dev).wait_recv()

    def left(self, lane, span, dev):
        self.make(lane, 0, span, span, dev).wait_send()


class Exchange:
    def __init__(self, wires, lane, rings, span, k=None):
        self.w, self.lane, self.rings, self.span = wires, lane, rings, span
        self.k = k or {"relay": wires.new(), "rest": wires.new()}

    def go(self, sem, view, dev):
        self.w.start(self.lane, self.k[sem], view, view, dev)

    def await_blocks(self, sem, n):
        self.w.arrive(self.k[sem], self.span(n * len(self.rings)), self.rings[0][1])

    def first(self):
        for pos, plus, minus, part in self.rings:
            self.go("relay", part(pos, 0), plus)
            self.go("relay", part(pos, 1), minus)

    def second(self):
        for pos, plus, minus, part in self.rings:
            self.go("rest", part(pos, 1), plus)
            self.go("rest", part(pos, 0), minus)

    def start(self):
        self.first()
        self.second()

    def relay(self):
        self.await_blocks("relay", 1)
        for pos, plus, minus, part in self.rings:
            self.go("rest", part(lax.rem(pos + 3, 4), 0), plus)
            self.go("rest", part(lax.rem(pos + 1, 4), 1), minus)

    def rest(self):
        self.await_blocks("rest", 2)


class ChipExchange:
    def __init__(self, wires, lane, pos, plus, minus, mate, sizes, view, span, k=None):
        self.w, self.lane, self.pos, self.plus, self.minus, self.mate = wires, lane, pos, plus, minus, mate
        self.sizes, self.view, self.span = sizes, view, span
        names = ("relay0", "relay1", "near", "far0", "far1")
        self.k = {n: k[n] if k else wires.new() for n in names}
        self.k.update({n: wires.new() for n in ("mate_near", "mate_far")})

    def piece(self, shift, half, i):
        row = sum(self.sizes[0]) * half + (self.sizes[half][0] if i else 0)
        return self.view(lax.rem(self.pos + shift, 4), row, self.sizes[half][i])

    def half(self, shift, half):
        return self.view(lax.rem(self.pos + shift, 4), sum(self.sizes[0]) * half, sum(self.sizes[half]))

    def go(self, sem, view, dev):
        self.w.start(self.lane, self.k[sem], view, view, dev)

    def take(self, sem, blocks, rows, dev):
        self.w.arrive(self.k[sem], self.span(blocks, rows), dev)

    def rows(self, i):
        return self.sizes[0][i] + self.sizes[1][i]

    def start(self):
        for i in range(2):
            self.go(f"relay{i}", self.piece(0, 0, i), self.plus)
            self.go(f"relay{i}", self.piece(0, 1, i), self.minus)
        self.go("near", self.half(0, 1), self.plus)
        self.go("near", self.half(0, 0), self.minus)
        for h in range(2):
            self.go("mate_near", self.half(0, h), self.mate)

    def relay(self, i):
        self.take(f"relay{i}", 0, self.rows(i), self.plus)
        left, right = self.piece(3, 0, i), self.piece(1, 1, i)
        self.go(f"far{i}", left, self.plus)
        self.go(f"far{i}", right, self.minus)
        self.go("mate_near", left, self.mate)
        self.go("mate_near", right, self.mate)

    def near(self):
        self.take("near", 1, 0, self.plus)
        self.go("mate_near", self.half(3, 1), self.mate)
        self.go("mate_near", self.half(1, 0), self.mate)

    def far(self, i):
        self.take(f"far{i}", 0, self.rows(i), self.plus)
        self.go("mate_far", self.piece(2, 0, i), self.mate)
        self.go("mate_far", self.piece(2, 1, i), self.mate)

    def mate_near(self):
        self.take("mate_near", 3, 0, self.mate)

    def mate_far(self):
        self.take("mate_far", 1, 0, self.mate)


def dot(a, b):
    return jnp.dot(a, b, preferred_element_type=F32)


def dot_last(a, b):
    return lax.dot_general(a, b, (((1,), (1,)), ((), ())), preferred_element_type=F32)


def dot_first(a, b):
    return lax.dot_general(a, b, (((0,), (0,)), ((), ())), preferred_element_type=F32)


def rounded(v):
    return v.astype(BF16).astype(F32)


def two(v):
    high = v.astype(BF16)
    return high, (v - high.astype(F32)).astype(BF16)


def kernel(
    tokens, gain, w_f, w_i, w_q, w_o, w_v, w_g, w_gr, w_gc, lb, shift, sinit, hgain, ck, cgain, cbias, w_or, w_oc,
    out,
    tok, gainv, xs, wb, stage, lbv, shv, siv, hgv, ckv, cgv, cbv,
    kgb, cb, vb, qb, ogb, ext, hsend, hrecv, sgr, sgc, mc, mcn, mr, head, qd, stb, rbuf, sty, stz, kv, scales, acc,
    load_sem, send_sem, recv_sem,
):
    s, t = lax.axis_index("sp"), lax.axis_index("tp")
    z, y, x, c = s // 4, lax.rem(s, 4), t // 2, lax.rem(t, 2)
    w = Wires(send_sem, recv_sem)

    def at(zz, yy):
        return (lax.rem(zz + 4, 4) * 4 + lax.rem(yy + 4, 4), t)

    def across(xx):
        return (s, lax.rem(xx + 4, 4) * 2 + c)

    mate = (s, 1 - c + 2 * x)
    swap = (2 * t + lax.rem(s, 2), s // 2)
    home = s // 2 == t
    following, preceding = (lax.rem(s + 1, 16), t), (lax.rem(s + 15, 16), t)

    def load(k, src, dst):
        copy = pltpu.make_async_copy(src, dst, load_sem.at[k])
        copy.start()
        return copy

    first = [load(0, tokens, tok), load(1, gain, gainv)]
    for b, src in enumerate(
        (
            w_v, w_g, w_f, w_i, w_q, w_o,
            w_gr.at[:, pl.ds(0, 128)], w_gr.at[:, pl.ds(128, 128)],
            w_gc.at[:, pl.ds(0, 128)], w_gc.at[:, pl.ds(128, 128)],
        )
    ):
        load(2, src, wb.at[b, z, y])
    load(2, w_or, stage.at[0])
    load(2, w_oc, stage.at[1])
    twelve = wb.at[0, pl.ds(0, 3)]
    own = pltpu.make_async_copy(twelve, twelve, load_sem.at[2])
    rest = [
        load(k + 3, a, b)
        for k, (a, b) in enumerate(
            (
                (shift, shv), (lb, lbv), (sinit.at[0], siv), (hgain, hgv), (ck, ckv), (cgain, cgv), (cbias, cbv),
            )
        )
    ]

    barrier = pltpu.get_barrier_semaphore()
    partners = [at(z, y + 1), at(z, y - 1), at(z + 1, y), at(z - 1, y), across(x + 1), across(x - 1), mate]
    for dev in partners:
        pl.semaphore_signal(barrier, inc=1, device_id=dev, device_id_type=MESH)

    for there, dev in ((s > 0, preceding),):

        @pl.when(there)
        def _(dev=dev):
            pl.semaphore_signal(barrier, inc=1, device_id=dev, device_id_type=MESH)

    @pl.when(jnp.logical_not(home))
    def _():
        pl.semaphore_signal(barrier, inc=1, device_id=swap, device_id_type=MESH)

    def exchange(lane, sizes, view, span, k=None):
        return ChipExchange(w, lane, x, across(x + 1), across(x - 1), mate, sizes, view, span, k)

    def token_view(xx, row, rows):
        return xs.at[pl.ds(pl.multiple_of((xx * 2 + c) * TD + row, 16), rows), :]

    def block_view(buf):
        return lambda xx, row, rows: buf.at[xx * 2 + c, pl.ds(row, rows)]

    def block_span(buf):
        return lambda blocks, rows: buf.at[0, pl.ds(0, rows)] if rows else buf.at[pl.ds(0, blocks)]

    token_ring = exchange(
        1, ((32, 16), (32, 16)), token_view, lambda blocks, rows: xs.at[pl.ds(0, blocks * TD + rows), :]
    )
    conv_ring = exchange(2, ((192, 192), (192, 208)), block_view(mc), block_span(mc))
    rec_ring = exchange(3, ((192, 192), (192, 192)), block_view(mr), block_span(mr), token_ring.k)

    def along_y(part):
        return (y, at(z, y + 1), at(z, y - 1), part)

    def along_z(part):
        return (z, at(z + 1, y), at(z - 1, y), part)

    p1, p2 = [], []
    for g in range(6):
        a, b = 2 * g, 2 * g + 1
        rings = [
            along_y(lambda p, h, b=a: wb.at[b, z, p, pl.ds(64 * h, 64)]),
            along_z(lambda p, h, b=b: wb.at[b, p, y, pl.ds(64 * h, 64)]),
        ]
        p1.append(Exchange(w, 0, rings, lambda n, b=a: wb.at[b, 0, pl.ds(0, n)]))
        rings = [
            along_z(lambda p, h, b=a: wb.at[b, p, pl.ds(2 * h, 2)]),
            along_y(lambda p, h, b=b: wb.at[b, pl.ds(2 * h, 2), p]),
        ]
        p2.append(Exchange(w, 8, rings, lambda n, b=a: wb.at[b, pl.ds(0, n)], p1[g - 3].k if g > 2 else None))

    stz[...] = jnp.zeros_like(stz)
    own.wait()
    count = len(partners) + jnp.where(home, 0, 1) + jnp.where(s < 15, 1, 0)
    pl.semaphore_wait(barrier, count)
    for g in range(3):
        p1[g].start()
    swap_k, y_k, z_k, h_k = (w.new() for _ in range(4))

    def place(i):
        return wb.at[10 + i, swap[0] // 4, lax.rem(swap[0], 4)]

    @pl.when(jnp.logical_not(home))
    def _():
        for i in range(2):
            w.start(4, swap_k, stage.at[i], place(i), swap)

    @pl.when(home)
    def _():
        for i in range(2):
            pltpu.make_async_copy(stage.at[i], wb.at[10 + i, z, y], recv_sem.at[swap_k]).start()

    def swapped():
        @pl.when(jnp.logical_not(home))
        def _():
            w.arrive(swap_k, stage, swap)
            w.left(4, stage, swap)

        @pl.when(home)
        def _():
            pltpu.make_async_copy(stage, stage, recv_sem.at[swap_k]).wait()

    for copy in first:
        copy.wait()
    base = pl.multiple_of(t * TD, 16)

    def normalize(r, _):
        wide = tok[pl.ds(pl.multiple_of(r * 16, 16), 16), :].astype(F32)
        scale = lax.rsqrt(jnp.mean(wide * wide, axis=-1, keepdims=True) + EPS)
        xs[pl.ds(pl.multiple_of(base + r * 16, 16), 16), :] = (wide * scale * gainv[...]).astype(BF16)
        return 0

    lax.fori_loop(0, TD // 16, normalize, 0, unroll=TD // 16)
    token_ring.start()

    def whole(b):
        return wb[b].reshape(2048, 128)

    def project(group, finish, size, starts):
        weight = jnp.concatenate([whole(2 * group), whole(2 * group + 1)], axis=1)

        def tile(r, _):
            start = pl.multiple_of(starts(r), 32)
            rows = pl.ds(start, size)
            finish(start, rows, dot(xs[rows, :], weight))
            return 0

        def run(low, high):
            lax.fori_loop(low, high, tile, 0, unroll=high - low if high - low > 1 else None)

        return run

    def project_all(group, finish):
        project(group, finish, PT, lambda r: r * PT)(0, T // PT)

    def by_ring(r):
        return lax.rem(x + jnp.where(r == 1, 3, jnp.where(r == 2, 1, jnp.where(r == 3, 2, 0))), 4) * XT

    def finish_fi(start, rows, v):
        gate = (1.0 - lbv[...]) * jax.nn.sigmoid(-rounded(v[:, :128]))
        kgb[rows, :] = gate
        cb[rows, :] = jnp.log1p(-gate) + shv[rows, :]
        vb[rows, :] = v[:, 128:].astype(BF16)

    def finish_vg(start, rows, v):
        gated = (rounded(v[:, :128]) * jax.nn.sigmoid(rounded(v[:, 128:]))).astype(BF16)
        ext[pl.ds(pl.multiple_of(start + HALO, 8), XT), :] = gated.astype(F32)

    def finish_qo(start, rows, v):
        raw = rounded(v[:, :128])
        qb[rows, :] = raw * jax.nn.sigmoid(raw)
        raw = rounded(v[:, 128:])
        ogb[rows, :] = raw * jax.nn.sigmoid(raw)

    def finish_gate(buf):
        def finish(start, rows, v):
            buf[rows, :] = jax.nn.sigmoid(rounded(v))

        return finish

    at_or_after = lax.broadcasted_iota(jnp.int32, (L, L), 0) >= lax.broadcasted_iota(jnp.int32, (L, L), 1)
    ones_below = jnp.where(at_or_after, 1.0, 0.0).astype(BF16)

    def pack_block(buf, i, decay, state):
        buf[i, pl.ds(0, HEAD), :] = state.astype(BF16)
        extra = jnp.concatenate([a.astype(F32) for a in two(decay)] + [jnp.zeros((14, HEAD), F32)], axis=0)
        buf[i, pl.ds(HEAD, 16), :] = extra.astype(BF16)

    def block_of(buf, i):
        both = buf[i, pl.ds(HEAD, 16), :].astype(F32)
        return both[0:1, :] + both[1:2, :], buf[i, pl.ds(0, HEAD), :].astype(F32)

    def local_states():
        for i in range(NC):
            rows = pl.ds(i * L, L)
            sides = dot(ones_below, jnp.concatenate(two(cb[rows, :]), axis=1))
            total = sides[:, :128] + sides[:, 128:]
            cb[rows, :] = total
            ending = (kgb[rows, :] * jnp.exp(total[L - 1 : L, :] - total)).astype(BF16)
            kv[i] = dot_first(vb[rows, :], ending)
        state = jnp.zeros((HEAD, HEAD), F32)
        before = jnp.zeros((1, HEAD), F32)
        for i in range(NC):
            last = cb[pl.ds(i * L + L - 1, 1), :]
            stb[i] = state.astype(BF16)
            rbuf[pl.ds(i, 1), :] = before
            state = jnp.exp(last) * state + kv[i]
            before = before + last
        pack_block(sty, y, jnp.exp(before), state)

    def local_outputs():
        for i in range(NC):
            rows = pl.ds(i * L, L)
            total, q = cb[rows, :], qb[rows, :]
            middle = 0.5 * total[L - 1 : L, :]
            left = (q * jnp.exp(total - middle)).astype(BF16)
            right = (kgb[rows, :] * jnp.exp(middle - total)).astype(BF16)
            scores = jnp.where(at_or_after, dot_last(left, right), 0.0).astype(BF16)
            o = dot(scores, vb[rows, :])
            o = o + dot_last((q * jnp.exp(total)).astype(BF16), stb[i])
            head[rows, :] = o
            qd[rows, :] = (q * jnp.exp(total + rbuf[pl.ds(i, 1), :])).astype(BF16)

    def convolve(low, high):
        for i in range(low, high):
            acc = jnp.zeros((128, HEAD), F32)
            for j in range(KW):
                acc = acc + ckv[pl.ds(j, 1), :] * ext[pl.ds(i * 128 + HALO - KW + 1 + j, 128), :]
            mc[t, pl.ds(i * 128, 128), :] = acc.astype(BF16)

    def take_halo():
        @pl.when(s > 0)
        def _():
            w.arrive(h_k, hrecv, preceding)
            ext[pl.ds(0, HALO), :] = hrecv[...].astype(F32)

        @pl.when(s == 0)
        def _():
            ext[pl.ds(0, HALO), :] = jnp.zeros((HALO, HEAD), F32)

    def take_z():
        for i in (1, 2, 3):

            @pl.when(z == i)
            def _(i=i):
                w.arrive(z_k, stz.at[pl.ds(0, i)], at(z + 1, y))

    def chip_weight(b, xx):
        top, low = ([wb[b, xx, 2 * k + j] for j in range(2)] for k in range(2))
        return jnp.concatenate([jnp.concatenate(top, axis=1), jnp.concatenate(low, axis=1)], axis=0)

    def chip_blocks(rows, xx):
        return jnp.concatenate([mr[2 * xx, rows, :], mr[2 * xx + 1, rows, :]], axis=1)

    p1[0].relay()
    p1[1].relay()
    p1[3].start()
    p1[4].start()
    p1[2].relay()
    p1[0].rest()
    p2[0].start()
    p1[1].rest()
    p2[1].first()
    token_ring.relay(0)
    token_ring.relay(1)
    p2[0].relay()
    p2[1].second()
    token_ring.near()
    p1[2].rest()
    p2[1].relay()
    p2[2].first()
    p1[3].relay()
    p1[4].relay()
    swapped()
    p1[5].start()
    for copy in rest:
        copy.wait()
    token_ring.far(0)
    token_ring.far(1)
    p2[0].rest()
    p2[2].second()
    token_ring.mate_near()
    project_vg = project(0, finish_vg, XT, by_ring)
    project_vg(0, 3)
    token_ring.mate_far()
    project_vg(3, 4)
    hsend[...] = ext[pl.ds(T, HALO), :].astype(BF16)

    @pl.when(s < 15)
    def _():
        w.start(5, h_k, hsend, hrecv, following)

    p2[1].rest()
    project_all(1, finish_fi)
    local_states()
    for i in (2, 1, 3):
        w.start(6, y_k, sty.at[y], sty.at[y], at(z, y + i))

    p2[2].relay()
    p1[3].rest()
    p1[5].relay()
    p2[3].start()
    convolve(1, T // 128)
    extra = [a.astype(F32) for v in (cgv[...], cbv[...]) for a in two(v)]
    mc[t, pl.ds(T, 16), :] = jnp.concatenate(extra + [jnp.zeros((12, HEAD), F32)], axis=0).astype(BF16)
    take_halo()
    convolve(0, 1)
    conv_ring.start()
    w.arrive(y_k, sty.at[pl.ds(0, 3)], at(z, y + 1))
    row_decay, row_state = jnp.ones((1, HEAD), F32), jnp.zeros((HEAD, HEAD), F32)
    my_decay, my_state = row_decay, row_state
    for i in range(4):
        d, v = block_of(sty, i)
        row_decay, row_state = row_decay * d, d * row_state + v
        if i < 3:
            take = i < y
            my_decay = jnp.where(take, row_decay, my_decay)
            my_state = jnp.where(take, row_state, my_state)
    pack_block(stz, z, row_decay, row_state)
    for i in (2, 1, 3):

        @pl.when(z + i < 4)
        def _(i=i):
            w.start(7, z_k, stz.at[z], stz.at[z], at(z + i, y))


    p1[5].rest()
    p2[5].first()
    p2[2].rest()
    project_all(2, finish_qo)
    conv_ring.relay(0)
    conv_ring.relay(1)
    p2[3].relay()
    p2[5].second()
    local_outputs()
    p1[4].rest()
    p2[4].start()
    take_z()
    entering = siv[...].T
    for i in range(3):
        d, v = block_of(stz, i)
        entering = jnp.where(i < z, d * entering + v, entering)
    entering = (my_decay * entering + my_state).astype(BF16)

    def finish_head(low, high):
        for r in range(low, high):
            rows = pl.ds(r * 128, 128)
            h = head[rows, :] + dot_last(qd[rows, :], entering)
            h = h * lax.rsqrt(jnp.mean(h * h, axis=-1, keepdims=True) + EPS) * hgv[...]
            mr[t, rows, :] = (h * ogb[rows, :]).astype(BF16)

    finish_head(0, T // 128)
    rec_ring.start()
    conv_ring.near()
    p2[5].relay()
    conv_ring.far(0)
    conv_ring.far(1)
    rec_ring.relay(0)
    conv_ring.mate_near()
    conv_ring.mate_far()

    def conv_scale(r, _):
        rows = pl.ds(pl.multiple_of(r * 64, 64), 64)
        squares = sum(v * v for v in (mc[k, rows, :].astype(F32) for k in range(8)))
        scale = lax.rsqrt(jnp.sum(squares, axis=-1, keepdims=True) * (1.0 / CONV) + EPS)
        scales[rows, :] = jnp.broadcast_to(scale, (64, 128))
        return 0

    gains, biases = [], []
    for k in range(8):
        four = mc[k, pl.ds(T, 16), :].astype(F32)
        gains.append(0.5 * (four[0:1, :] + four[1:2, :]))
        biases.append(0.5 * (four[2:3, :] + four[3:4, :]))

    def normalize_conv(r, _):
        rows = pl.ds(pl.multiple_of(r * 64, 64), 64)
        scale = scales[rows, :]
        for k in range(8):
            half = mc[k, rows, :].astype(F32) * scale * gains[k] + biases[k]
            mcn[rows, pl.ds(k * 128, 128)] = (half + half * jnp.tanh(half)).astype(BF16)
        return 0

    lax.fori_loop(0, T // 64, conv_scale, 0, unroll=4)
    rec_ring.relay(1)
    p2[4].relay()
    p2[3].rest()
    project_all(3, finish_gate(sgr))
    rec_ring.near()
    lax.fori_loop(0, T // 64, normalize_conv, 0, unroll=2)
    p2[5].rest()
    w_conv = jnp.concatenate([chip_weight(11, xx) for xx in range(4)], axis=0)

    def conv_tile(r, _):
        rows = pl.ds(pl.multiple_of(r * PT, PT), PT)
        sgc[rows, :] = rounded(dot(mcn[rows, :], w_conv))
        return 0

    lax.fori_loop(0, T // PT, conv_tile, 0, unroll=2)
    rec_ring.far(0)
    rec_ring.far(1)
    rec_ring.mate_near()
    near = [x, lax.rem(x + 1, 4), lax.rem(x + 3, 4)]
    w_near = jnp.concatenate([chip_weight(10, xx) for xx in near], axis=0)

    def near_tile(r, _):
        rows = pl.ds(pl.multiple_of(r * PT, PT), PT)
        acc[rows, :] = dot(jnp.concatenate([chip_blocks(rows, xx) for xx in near], axis=1), w_near)
        return 0

    lax.fori_loop(0, T // PT, near_tile, 0, unroll=2)
    p2[4].rest()

    def finish_gc(start, rows, v):
        sgc[rows, :] = jax.nn.sigmoid(rounded(v)) * sgc[rows, :]

    project_all(4, finish_gc)
    rec_ring.mate_far()
    opposite = lax.rem(x + 2, 4)
    w_far = chip_weight(10, opposite)

    def last_tile(r, _):
        rows = pl.ds(pl.multiple_of(r * RT, RT), RT)
        y_rec = rounded(acc[rows, :] + dot(chip_blocks(rows, opposite), w_far))
        out[rows, :] = (sgr[rows, :] * y_rec + sgc[rows, :]).astype(BF16)
        return 0

    lax.fori_loop(0, T // RT, last_tile, 0, unroll=3)
    w.left(0, wb.at[pl.ds(0, 3), pl.ds(0, 3)], mate)
    w.left(8, wb.at[pl.ds(0, 9)], mate)
    w.left(1, xs.at[pl.ds(0, 7 * TD), :], mate)
    w.left(2, mc.at[pl.ds(0, 7)], mate)
    w.left(3, mr.at[pl.ds(0, 7)], mate)

    @pl.when(s < 15)
    def _():
        w.left(5, hsend, following)

    w.left(6, sty.at[pl.ds(0, 3)], mate)
    for i in (1, 2, 3):

        @pl.when(z == 3 - i)
        def _(i=i):
            w.left(7, stz.at[pl.ds(0, i)], mate)


def local(
    tokens, norm_gain, w_query, w_forget, w_input, w_outgate, w_conv_value, w_conv_gate, w_gate_rec, w_gate_conv,
    lower_bound, decay_shift, state_init, head_gain, conv_kernel, channel_gain, channel_bias, w_out_rec, w_out_conv,
):
    line = lambda v: v.reshape(1, -1)
    args = (
        tokens, line(norm_gain), w_forget, w_input, w_query, w_outgate, w_conv_value, w_conv_gate, w_gate_rec,
        w_gate_conv, line(lower_bound), decay_shift, state_init, line(head_gain), conv_kernel, line(channel_gain),
        line(channel_bias), w_out_rec, w_out_conv,
    )
    v = pltpu.VMEM
    scratch = [
        v((TD, 2048), BF16), v((1, 2048), F32), v((T, 2048), BF16), v((12, 4, 4, 128, 128), BF16),
        v((2, 128, 128), BF16), v((1, 128), F32), v((T, 128), F32), v((128, 128), F32), v((1, 128), F32),
        v((KW, 128), F32), v((1, 128), F32), v((1, 128), F32),
        v((T, 128), F32), v((T, 128), F32), v((T, 128), BF16), v((T, 128), F32), v((T, 128), F32),
        v((T + HALO, 128), F32), v((HALO, 128), BF16), v((HALO, 128), BF16), v((T, 256), F32), v((T, 256), F32),
        v((8, T + 16, 128), BF16), v((T, CONV), BF16), v((8, T, 128), BF16), v((T, 128), F32), v((T, 128), BF16),
        v((NC, 128, 128), BF16), v((16, 128), F32), v((4, 144, 128), BF16), v((4, 144, 128), BF16), v((NC, 128, 128), F32), v((T, 128), F32), v((T, 256), F32),
        pltpu.SemaphoreType.DMA((10,)), pltpu.SemaphoreType.DMA((9,)), pltpu.SemaphoreType.DMA((38,)),
    ]
    return pl.pallas_call(
        kernel,
        out_shape=jax.ShapeDtypeStruct((T, 256), BF16),
        in_specs=[pl.BlockSpec(memory_space=pltpu.HBM)] * len(args),
        out_specs=pl.BlockSpec(memory_space=pltpu.VMEM),
        scratch_shapes=scratch,
        compiler_params=pltpu.CompilerParams(
            collective_id=0, has_side_effects=True, vmem_limit_bytes=40 * 1024 * 1024
        ),
    )(*[pltpu.with_memory_space_constraint(a, pltpu.HBM) for a in args])


def solution(mesh):
    both = P("sp", "tp")
    in_specs = (
        P(("sp", "tp"), None), P(), both, both, both, both, both, both, both, both, P("tp"), both,
        P("tp", None, None), P("tp"), P(None, "tp"), P("tp"), P("tp"), P("tp", "sp"), P("tp", "sp"),
    )
    return jax.shard_map(local, mesh=mesh, in_specs=in_specs, out_specs=both, check_vma=False)
```

```python
import functools

import jax
import jax.numpy as jnp
from jax import lax
from jax.experimental import pallas as pl
from jax.experimental.pallas import tpu as pltpu
from jax.sharding import PartitionSpec as P

MESH = pl.DeviceIdType.MESH
F32 = jnp.float32
BF16 = jnp.bfloat16
HEAD = 128
CONV = 1024
KW = 31
EPS = 1e-06
L = 64
T = 768
NC = T // L
TD = 96
RT = 256
XT = 192
PT = 384
HALO = 32


class Wires:
    def __init__(self, send_sem, recv_sem):
        self.send_sem, self.recv_sem = send_sem, recv_sem
        self.count = 0

    def new(self):
        self.count += 1
        return self.count - 1

    def make(self, lane, k, src, dst, dev):
        return pltpu.make_async_remote_copy(
            src_ref=src,
            dst_ref=dst,
            send_sem=self.send_sem.at[lane],
            recv_sem=self.recv_sem.at[k],
            device_id=dev,
            device_id_type=MESH,
        )

    def start(self, lane, k, src, dst, dev):
        self.make(lane, k, src, dst, dev).start()

    def arrive(self, k, span, dev):
        self.make(0, k, span, span, dev).wait_recv()

    def left(self, lane, span, dev):
        self.make(lane, 0, span, span, dev).wait_send()


class Exchange:
    def __init__(self, wires, lane, rings, span, k=None):
        self.w, self.lane, self.rings, self.span = wires, lane, rings, span
        self.k = k or {"relay": wires.new(), "rest": wires.new()}

    def go(self, sem, view, dev):
        self.w.start(self.lane, self.k[sem], view, view, dev)

    def await_blocks(self, sem, n):
        self.w.arrive(self.k[sem], self.span(n * len(self.rings)), self.rings[0][1])

    def first(self):
        for pos, plus, minus, part in self.rings:
            self.go("relay", part(pos, 0), plus)
            self.go("relay", part(pos, 1), minus)

    def second(self):
        for pos, plus, minus, part in self.rings:
            self.go("rest", part(pos, 1), plus)
            self.go("rest", part(pos, 0), minus)

    def start(self):
        self.first()
        self.second()

    def relay(self):
        self.await_blocks("relay", 1)
        for pos, plus, minus, part in self.rings:
            self.go("rest", part(lax.rem(pos + 3, 4), 0), plus)
            self.go("rest", part(lax.rem(pos + 1, 4), 1), minus)

    def rest(self):
        self.await_blocks("rest", 2)


class ChipExchange:
    def __init__(self, wires, lane, pos, plus, minus, mate, sizes, view, span, k=None):
        self.w, self.lane, self.pos, self.plus, self.minus, self.mate = wires, lane, pos, plus, minus, mate
        self.sizes, self.view, self.span = sizes, view, span
        names = ("relay0", "relay1", "near", "far0", "far1")
        self.k = {n: k[n] if k else wires.new() for n in names}
        self.k.update({n: wires.new() for n in ("mate_near", "mate_far")})

    def piece(self, shift, half, i):
        row = sum(self.sizes[0]) * half + (self.sizes[half][0] if i else 0)
        return self.view(lax.rem(self.pos + shift, 4), row, self.sizes[half][i])

    def half(self, shift, half):
        return self.view(lax.rem(self.pos + shift, 4), sum(self.sizes[0]) * half, sum(self.sizes[half]))

    def go(self, sem, view, dev):
        self.w.start(self.lane, self.k[sem], view, view, dev)

    def take(self, sem, blocks, rows, dev):
        self.w.arrive(self.k[sem], self.span(blocks, rows), dev)

    def rows(self, i):
        return self.sizes[0][i] + self.sizes[1][i]

    def start(self):
        self.start_piece(0)
        self.start_piece(1)
        self.start_rest()

    def start_piece(self, i):
        self.go(f"relay{i}", self.piece(0, 0, i), self.plus)
        self.go(f"relay{i}", self.piece(0, 1, i), self.minus)

    def start_rest(self):
        self.go("near", self.half(0, 1), self.plus)
        self.go("near", self.half(0, 0), self.minus)
        for h in range(2):
            self.go("mate_near", self.half(0, h), self.mate)

    def relay(self, i):
        self.take(f"relay{i}", 0, self.rows(i), self.plus)
        left, right = self.piece(3, 0, i), self.piece(1, 1, i)
        self.go(f"far{i}", left, self.plus)
        self.go(f"far{i}", right, self.minus)
        self.go("mate_near", left, self.mate)
        self.go("mate_near", right, self.mate)

    def near(self):
        self.take("near", 1, 0, self.plus)
        self.go("mate_near", self.half(3, 1), self.mate)
        self.go("mate_near", self.half(1, 0), self.mate)

    def far(self, i):
        self.take(f"far{i}", 0, self.rows(i), self.plus)
        self.go("mate_far", self.piece(2, 0, i), self.mate)
        self.go("mate_far", self.piece(2, 1, i), self.mate)

    def mate_near(self):
        self.take("mate_near", 3, 0, self.mate)

    def mate_far(self):
        self.take("mate_far", 1, 0, self.mate)


def dot(a, b):
    return jnp.dot(a, b, preferred_element_type=F32)


def dot_last(a, b):
    return lax.dot_general(a, b, (((1,), (1,)), ((), ())), preferred_element_type=F32)


def dot_first(a, b):
    return lax.dot_general(a, b, (((0,), (0,)), ((), ())), preferred_element_type=F32)


def rounded(v):
    return v.astype(BF16).astype(F32)


def two(v):
    high = v.astype(BF16)
    return high, (v - high.astype(F32)).astype(BF16)


def kernel(
    tokens, gain, w_f, w_i, w_q, w_o, w_v, w_g, w_gr, w_gc, lb, shift, sinit, hgain, ck, cgain, cbias, w_or, w_oc,
    out,
    tok, gainv, xs, wb, stage, lbv, shv, siv, hgv, ckv, cgv, cbv,
    kgb, cb, vb, qb, ogb, ext, hsend, hrecv, sgr, sgc, mc, mcn, mr, head, qd, stb, rbuf, sty, stz, kv, scales, acc,
    load_sem, send_sem, recv_sem,
):
    s, t = lax.axis_index("sp"), lax.axis_index("tp")
    z, y, x, c = s // 4, lax.rem(s, 4), t // 2, lax.rem(t, 2)
    w = Wires(send_sem, recv_sem)

    def at(zz, yy):
        return (lax.rem(zz + 4, 4) * 4 + lax.rem(yy + 4, 4), t)

    def across(xx):
        return (s, lax.rem(xx + 4, 4) * 2 + c)

    mate = (s, 1 - c + 2 * x)
    swap = (2 * t + lax.rem(s, 2), s // 2)
    home = s // 2 == t
    following, preceding = (lax.rem(s + 1, 16), t), (lax.rem(s + 15, 16), t)

    def load(k, src, dst):
        copy = pltpu.make_async_copy(src, dst, load_sem.at[k])
        copy.start()
        return copy

    first = [load(0, tokens, tok), load(1, gain, gainv)]
    for b, src in enumerate(
        (
            w_v, w_g, w_f, w_i, w_q, w_o,
            w_gr.at[:, pl.ds(0, 128)], w_gr.at[:, pl.ds(128, 128)],
            w_gc.at[:, pl.ds(0, 128)], w_gc.at[:, pl.ds(128, 128)],
        )
    ):
        load(2, src, wb.at[b, z, y])
    load(2, w_or, stage.at[0])
    load(2, w_oc, stage.at[1])
    twelve = wb.at[0, pl.ds(0, 3)]
    own = pltpu.make_async_copy(twelve, twelve, load_sem.at[2])
    rest = [
        load(k + 3, a, b)
        for k, (a, b) in enumerate(
            (
                (shift, shv), (lb, lbv), (sinit.at[0], siv), (hgain, hgv), (ck, ckv), (cgain, cgv), (cbias, cbv),
            )
        )
    ]

    barrier = pltpu.get_barrier_semaphore()
    partners = [at(z, y + 1), at(z, y - 1), at(z + 1, y), at(z - 1, y), across(x + 1), across(x - 1), mate]
    for dev in partners:
        pl.semaphore_signal(barrier, inc=1, device_id=dev, device_id_type=MESH)

    for there, dev in ((s > 0, preceding),):

        @pl.when(there)
        def _(dev=dev):
            pl.semaphore_signal(barrier, inc=1, device_id=dev, device_id_type=MESH)

    @pl.when(jnp.logical_not(home))
    def _():
        pl.semaphore_signal(barrier, inc=1, device_id=swap, device_id_type=MESH)

    def exchange(lane, sizes, view, span, k=None):
        return ChipExchange(w, lane, x, across(x + 1), across(x - 1), mate, sizes, view, span, k)

    def token_view(xx, row, rows):
        return xs.at[pl.ds(pl.multiple_of((xx * 2 + c) * TD + row, 16), rows), :]

    def block_view(buf):
        return lambda xx, row, rows: buf.at[xx * 2 + c, pl.ds(row, rows)]

    def block_span(buf):
        return lambda blocks, rows: buf.at[0, pl.ds(0, rows)] if rows else buf.at[pl.ds(0, blocks)]

    token_ring = exchange(
        1, ((32, 16), (32, 16)), token_view, lambda blocks, rows: xs.at[pl.ds(0, blocks * TD + rows), :]
    )
    conv_ring = exchange(2, ((192, 192), (192, 208)), block_view(mc), block_span(mc))
    rec_ring = exchange(3, ((192, 192), (192, 192)), block_view(mr), block_span(mr), token_ring.k)

    def along_y(part):
        return (y, at(z, y + 1), at(z, y - 1), part)

    def along_z(part):
        return (z, at(z + 1, y), at(z - 1, y), part)

    p1, p2 = [], []
    for g in range(6):
        a, b = 2 * g, 2 * g + 1
        rings = [
            along_y(lambda p, h, b=a: wb.at[b, z, p, pl.ds(64 * h, 64)]),
            along_z(lambda p, h, b=b: wb.at[b, p, y, pl.ds(64 * h, 64)]),
        ]
        p1.append(Exchange(w, 0, rings, lambda n, b=a: wb.at[b, 0, pl.ds(0, n)]))
        rings = [
            along_z(lambda p, h, b=a: wb.at[b, p, pl.ds(2 * h, 2)]),
            along_y(lambda p, h, b=b: wb.at[b, pl.ds(2 * h, 2), p]),
        ]
        p2.append(Exchange(w, 8, rings, lambda n, b=a: wb.at[b, pl.ds(0, n)], p1[g - 3].k if g > 2 else None))

    stz[...] = jnp.zeros_like(stz)
    own.wait()
    count = len(partners) + jnp.where(home, 0, 1) + jnp.where(s < 15, 1, 0)
    pl.semaphore_wait(barrier, count)
    for g in range(3):
        p1[g].start()
    swap_k, y_k, z_k, h_k = (w.new() for _ in range(4))

    def place(i):
        return wb.at[10 + i, swap[0] // 4, lax.rem(swap[0], 4)]

    @pl.when(jnp.logical_not(home))
    def _():
        for i in range(2):
            w.start(4, swap_k, stage.at[i], place(i), swap)

    @pl.when(home)
    def _():
        for i in range(2):
            pltpu.make_async_copy(stage.at[i], wb.at[10 + i, z, y], recv_sem.at[swap_k]).start()

    def swapped():
        @pl.when(jnp.logical_not(home))
        def _():
            w.arrive(swap_k, stage, swap)
            w.left(4, stage, swap)

        @pl.when(home)
        def _():
            pltpu.make_async_copy(stage, stage, recv_sem.at[swap_k]).wait()

    for copy in first:
        copy.wait()
    base = pl.multiple_of(t * TD, 16)

    def normalize(r, _):
        wide = tok[pl.ds(pl.multiple_of(r * 16, 16), 16), :].astype(F32)
        scale = lax.rsqrt(jnp.mean(wide * wide, axis=-1, keepdims=True) + EPS)
        xs[pl.ds(pl.multiple_of(base + r * 16, 16), 16), :] = (wide * scale * gainv[...]).astype(BF16)
        return 0

    lax.fori_loop(0, TD // 16, normalize, 0, unroll=TD // 16)
    token_ring.start()

    def whole(b):
        return wb[b].reshape(2048, 128)

    def project(group, finish, size, starts):
        weight = jnp.concatenate([whole(2 * group), whole(2 * group + 1)], axis=1)

        def tile(r, _):
            start = pl.multiple_of(starts(r), 32)
            rows = pl.ds(start, size)
            finish(start, rows, dot(xs[rows, :], weight))
            return 0

        def run(low, high):
            lax.fori_loop(low, high, tile, 0, unroll=high - low if high - low > 1 else None)

        return run

    def project_all(group, finish):
        project(group, finish, PT, lambda r: r * PT)(0, T // PT)

    def by_ring(r):
        return lax.rem(x + jnp.where(r == 1, 3, jnp.where(r == 2, 1, jnp.where(r == 3, 2, 0))), 4) * XT

    def finish_fi(start, rows, v):
        gate = (1.0 - lbv[...]) * jax.nn.sigmoid(-rounded(v[:, :128]))
        kgb[rows, :] = gate
        cb[rows, :] = jnp.log1p(-gate) + shv[rows, :]
        vb[rows, :] = v[:, 128:].astype(BF16)

    def finish_vg(start, rows, v):
        gated = (rounded(v[:, :128]) * jax.nn.sigmoid(rounded(v[:, 128:]))).astype(BF16)
        ext[pl.ds(pl.multiple_of(start + HALO, 8), XT), :] = gated.astype(F32)

    def finish_qo(start, rows, v):
        raw = rounded(v[:, :128])
        qb[rows, :] = raw * jax.nn.sigmoid(raw)
        raw = rounded(v[:, 128:])
        ogb[rows, :] = raw * jax.nn.sigmoid(raw)

    def finish_gate(buf):
        def finish(start, rows, v):
            buf[rows, :] = jax.nn.sigmoid(rounded(v))

        return finish

    at_or_after = lax.broadcasted_iota(jnp.int32, (L, L), 0) >= lax.broadcasted_iota(jnp.int32, (L, L), 1)
    ones_below = jnp.where(at_or_after, 1.0, 0.0).astype(BF16)

    def pack_block(buf, i, decay, state):
        buf[i, pl.ds(0, HEAD), :] = state.astype(BF16)
        extra = jnp.concatenate([a.astype(F32) for a in two(decay)] + [jnp.zeros((14, HEAD), F32)], axis=0)
        buf[i, pl.ds(HEAD, 16), :] = extra.astype(BF16)

    def block_of(buf, i):
        both = buf[i, pl.ds(HEAD, 16), :].astype(F32)
        return both[0:1, :] + both[1:2, :], buf[i, pl.ds(0, HEAD), :].astype(F32)

    def local_states():
        for i in range(NC):
            rows = pl.ds(i * L, L)
            sides = dot(ones_below, jnp.concatenate(two(cb[rows, :]), axis=1))
            total = sides[:, :128] + sides[:, 128:]
            cb[rows, :] = total
            ending = (kgb[rows, :] * jnp.exp(total[L - 1 : L, :] - total)).astype(BF16)
            kv[i] = dot_first(vb[rows, :], ending)
        state = jnp.zeros((HEAD, HEAD), F32)
        before = jnp.zeros((1, HEAD), F32)
        for i in range(NC):
            last = cb[pl.ds(i * L + L - 1, 1), :]
            stb[i] = state.astype(BF16)
            rbuf[pl.ds(i, 1), :] = before
            state = jnp.exp(last) * state + kv[i]
            before = before + last
        pack_block(sty, y, jnp.exp(before), state)

    def local_outputs():
        for i in range(NC):
            rows = pl.ds(i * L, L)
            total, q = cb[rows, :], qb[rows, :]
            middle = 0.5 * total[L - 1 : L, :]
            left = (q * jnp.exp(total - middle)).astype(BF16)
            right = (kgb[rows, :] * jnp.exp(middle - total)).astype(BF16)
            scores = jnp.where(at_or_after, dot_last(left, right), 0.0).astype(BF16)
            o = dot(scores, vb[rows, :])
            o = o + dot_last((q * jnp.exp(total)).astype(BF16), stb[i])
            head[rows, :] = o
            qd[rows, :] = (q * jnp.exp(total + rbuf[pl.ds(i, 1), :])).astype(BF16)

    def convolve(low, high):
        for i in range(low, high):
            acc = jnp.zeros((128, HEAD), F32)
            for j in range(KW):
                acc = acc + ckv[pl.ds(j, 1), :] * ext[pl.ds(i * 128 + HALO - KW + 1 + j, 128), :]
            mc[t, pl.ds(i * 128, 128), :] = acc.astype(BF16)

    def take_halo():
        @pl.when(s > 0)
        def _():
            w.arrive(h_k, hrecv, preceding)
            ext[pl.ds(0, HALO), :] = hrecv[...].astype(F32)

        @pl.when(s == 0)
        def _():
            ext[pl.ds(0, HALO), :] = jnp.zeros((HALO, HEAD), F32)

    def take_z():
        for i in (1, 2, 3):

            @pl.when(z == i)
            def _(i=i):
                w.arrive(z_k, stz.at[pl.ds(0, i)], at(z + 1, y))

    def chip_weight(b, xx):
        top, low = ([wb[b, xx, 2 * k + j] for j in range(2)] for k in range(2))
        return jnp.concatenate([jnp.concatenate(top, axis=1), jnp.concatenate(low, axis=1)], axis=0)

    def chip_blocks(rows, xx):
        return jnp.concatenate([mr[2 * xx, rows, :], mr[2 * xx + 1, rows, :]], axis=1)

    p1[0].relay()
    p1[1].relay()
    p1[3].start()
    p1[4].start()
    p1[2].relay()
    p1[0].rest()
    p2[0].start()
    p1[1].rest()
    p2[1].first()
    token_ring.relay(0)
    token_ring.relay(1)
    p2[0].relay()
    p2[1].second()
    token_ring.near()
    p1[2].rest()
    p2[1].relay()
    p2[2].first()
    p1[3].relay()
    p1[4].relay()
    swapped()
    p1[5].start()
    for copy in rest:
        copy.wait()
    token_ring.far(0)
    token_ring.far(1)
    p2[0].rest()
    p2[2].second()
    token_ring.mate_near()
    project_vg = project(0, finish_vg, XT, by_ring)
    project_vg(0, 3)
    token_ring.mate_far()
    project_vg(3, 4)
    hsend[...] = ext[pl.ds(T, HALO), :].astype(BF16)

    @pl.when(s < 15)
    def _():
        w.start(5, h_k, hsend, hrecv, following)

    p2[1].rest()
    project_all(1, finish_fi)
    local_states()
    for i in (2, 1, 3):
        w.start(6, y_k, sty.at[y], sty.at[y], at(z, y + i))

    p2[2].relay()
    p1[3].rest()
    p1[5].relay()
    p2[3].start()
    convolve(1, T // 128)
    extra = [a.astype(F32) for v in (cgv[...], cbv[...]) for a in two(v)]
    mc[t, pl.ds(T, 16), :] = jnp.concatenate(extra + [jnp.zeros((12, HEAD), F32)], axis=0).astype(BF16)
    take_halo()
    convolve(0, 1)
    conv_ring.start()
    w.arrive(y_k, sty.at[pl.ds(0, 3)], at(z, y + 1))
    row_decay, row_state = jnp.ones((1, HEAD), F32), jnp.zeros((HEAD, HEAD), F32)
    my_decay, my_state = row_decay, row_state
    for i in range(4):
        d, v = block_of(sty, i)
        row_decay, row_state = row_decay * d, d * row_state + v
        if i < 3:
            take = i < y
            my_decay = jnp.where(take, row_decay, my_decay)
            my_state = jnp.where(take, row_state, my_state)
    pack_block(stz, z, row_decay, row_state)
    for i in (2, 1, 3):

        @pl.when(z + i < 4)
        def _(i=i):
            w.start(7, z_k, stz.at[z], stz.at[z], at(z + i, y))


    p1[5].rest()
    p2[5].first()
    p2[2].rest()
    project_all(2, finish_qo)
    conv_ring.relay(0)
    conv_ring.relay(1)
    p2[3].relay()
    p2[5].second()
    local_outputs()
    p1[4].rest()
    p2[4].start()
    take_z()
    entering = siv[...].T
    for i in range(3):
        d, v = block_of(stz, i)
        entering = jnp.where(i < z, d * entering + v, entering)
    entering = (my_decay * entering + my_state).astype(BF16)

    def finish_head(*starts):
        for start in starts:
            rows = pl.ds(start, 192)
            h = head[rows, :] + dot_last(qd[rows, :], entering)
            h = h * lax.rsqrt(jnp.mean(h * h, axis=-1, keepdims=True) + EPS) * hgv[...]
            mr[t, rows, :] = (h * ogb[rows, :]).astype(BF16)

    finish_head(0, 384)
    rec_ring.start_piece(0)
    finish_head(192, 576)
    rec_ring.start_piece(1)
    rec_ring.start_rest()
    conv_ring.near()
    p2[5].relay()
    conv_ring.far(0)
    conv_ring.far(1)
    rec_ring.relay(0)
    conv_ring.mate_near()
    conv_ring.mate_far()

    def conv_scale(r, _):
        rows = pl.ds(pl.multiple_of(r * 64, 64), 64)
        squares = sum(v * v for v in (mc[k, rows, :].astype(F32) for k in range(8)))
        scale = lax.rsqrt(jnp.sum(squares, axis=-1, keepdims=True) * (1.0 / CONV) + EPS)
        scales[rows, :] = jnp.broadcast_to(scale, (64, 128))
        return 0

    gains, biases = [], []
    for k in range(8):
        four = mc[k, pl.ds(T, 16), :].astype(F32)
        gains.append(0.5 * (four[0:1, :] + four[1:2, :]))
        biases.append(0.5 * (four[2:3, :] + four[3:4, :]))

    def normalize_conv(r, _):
        rows = pl.ds(pl.multiple_of(r * 64, 64), 64)
        scale = scales[rows, :]
        for k in range(8):
            half = mc[k, rows, :].astype(F32) * scale * gains[k] + biases[k]
            mcn[rows, pl.ds(k * 128, 128)] = (half + half * jnp.tanh(half)).astype(BF16)
        return 0

    lax.fori_loop(0, T // 64, conv_scale, 0, unroll=4)
    rec_ring.relay(1)
    p2[4].relay()
    p2[3].rest()
    project_all(3, finish_gate(sgr))
    rec_ring.near()
    lax.fori_loop(0, T // 64, normalize_conv, 0, unroll=2)
    p2[5].rest()
    w_conv = jnp.concatenate([chip_weight(11, xx) for xx in range(4)], axis=0)

    def conv_tile(r, _):
        rows = pl.ds(pl.multiple_of(r * PT, PT), PT)
        sgc[rows, :] = rounded(dot(mcn[rows, :], w_conv))
        return 0

    lax.fori_loop(0, T // PT, conv_tile, 0, unroll=2)
    rec_ring.far(0)
    rec_ring.far(1)
    rec_ring.mate_near()
    near = [x, lax.rem(x + 1, 4), lax.rem(x + 3, 4)]
    w_near = jnp.concatenate([chip_weight(10, xx) for xx in near], axis=0)

    def near_tile(r, _):
        rows = pl.ds(pl.multiple_of(r * PT, PT), PT)
        acc[rows, :] = dot(jnp.concatenate([chip_blocks(rows, xx) for xx in near], axis=1), w_near)
        return 0

    lax.fori_loop(0, T // PT, near_tile, 0, unroll=2)
    p2[4].rest()

    def finish_gc(start, rows, v):
        sgc[rows, :] = jax.nn.sigmoid(rounded(v)) * sgc[rows, :]

    project_all(4, finish_gc)
    rec_ring.mate_far()
    opposite = lax.rem(x + 2, 4)
    w_far = chip_weight(10, opposite)

    def last_tile(r, _):
        rows = pl.ds(pl.multiple_of(r * RT, RT), RT)
        y_rec = rounded(acc[rows, :] + dot(chip_blocks(rows, opposite), w_far))
        out[rows, :] = (sgr[rows, :] * y_rec + sgc[rows, :]).astype(BF16)
        return 0

    lax.fori_loop(0, T // RT, last_tile, 0, unroll=3)
    w.left(0, wb.at[pl.ds(0, 3), pl.ds(0, 3)], mate)
    w.left(8, wb.at[pl.ds(0, 9)], mate)
    w.left(1, xs.at[pl.ds(0, 7 * TD), :], mate)
    w.left(2, mc.at[pl.ds(0, 7)], mate)
    w.left(3, mr.at[pl.ds(0, 7)], mate)

    @pl.when(s < 15)
    def _():
        w.left(5, hsend, following)

    w.left(6, sty.at[pl.ds(0, 3)], mate)
    for i in (1, 2, 3):

        @pl.when(z == 3 - i)
        def _(i=i):
            w.left(7, stz.at[pl.ds(0, i)], mate)


def local(
    tokens, norm_gain, w_query, w_forget, w_input, w_outgate, w_conv_value, w_conv_gate, w_gate_rec, w_gate_conv,
    lower_bound, decay_shift, state_init, head_gain, conv_kernel, channel_gain, channel_bias, w_out_rec, w_out_conv,
):
    line = lambda v: v.reshape(1, -1)
    args = (
        tokens, line(norm_gain), w_forget, w_input, w_query, w_outgate, w_conv_value, w_conv_gate, w_gate_rec,
        w_gate_conv, line(lower_bound), decay_shift, state_init, line(head_gain), conv_kernel, line(channel_gain),
        line(channel_bias), w_out_rec, w_out_conv,
    )
    v = pltpu.VMEM
    scratch = [
        v((TD, 2048), BF16), v((1, 2048), F32), v((T, 2048), BF16), v((12, 4, 4, 128, 128), BF16),
        v((2, 128, 128), BF16), v((1, 128), F32), v((T, 128), F32), v((128, 128), F32), v((1, 128), F32),
        v((KW, 128), F32), v((1, 128), F32), v((1, 128), F32),
        v((T, 128), F32), v((T, 128), F32), v((T, 128), BF16), v((T, 128), F32), v((T, 128), F32),
        v((T + HALO, 128), F32), v((HALO, 128), BF16), v((HALO, 128), BF16), v((T, 256), F32), v((T, 256), F32),
        v((8, T + 16, 128), BF16), v((T, CONV), BF16), v((8, T, 128), BF16), v((T, 128), F32), v((T, 128), BF16),
        v((NC, 128, 128), BF16), v((16, 128), F32), v((4, 144, 128), BF16), v((4, 144, 128), BF16), v((NC, 128, 128), F32), v((T, 128), F32), v((T, 256), F32),
        pltpu.SemaphoreType.DMA((10,)), pltpu.SemaphoreType.DMA((9,)), pltpu.SemaphoreType.DMA((38,)),
    ]
    return pl.pallas_call(
        kernel,
        out_shape=jax.ShapeDtypeStruct((T, 256), BF16),
        in_specs=[pl.BlockSpec(memory_space=pltpu.HBM)] * len(args),
        out_specs=pl.BlockSpec(memory_space=pltpu.VMEM),
        scratch_shapes=scratch,
        compiler_params=pltpu.CompilerParams(
            collective_id=0, has_side_effects=True, vmem_limit_bytes=40 * 1024 * 1024
        ),
    )(*[pltpu.with_memory_space_constraint(a, pltpu.HBM) for a in args])


def solution(mesh):
    both = P("sp", "tp")
    in_specs = (
        P(("sp", "tp"), None), P(), both, both, both, both, both, both, both, both, P("tp"), both,
        P("tp", None, None), P("tp"), P(None, "tp"), P("tp"), P("tp"), P("tp", "sp"), P("tp", "sp"),
    )
    return jax.shard_map(local, mesh=mesh, in_specs=in_specs, out_specs=both, check_vma=False)
```

```python
import functools

import jax
import jax.numpy as jnp
from jax import lax
from jax.experimental import pallas as pl
from jax.experimental.pallas import tpu as pltpu
from jax.sharding import PartitionSpec as P

MESH = pl.DeviceIdType.MESH
F32 = jnp.float32
BF16 = jnp.bfloat16
HEAD = 128
CONV = 1024
KW = 31
EPS = 1e-06
L = 64
T = 768
NC = T // L
TD = 96
RT = 256
XT = 192
PT = 384
HALO = 32


class Wires:
    def __init__(self, send_sem, recv_sem):
        self.send_sem, self.recv_sem = send_sem, recv_sem
        self.count = 0

    def new(self):
        self.count += 1
        return self.count - 1

    def make(self, lane, k, src, dst, dev):
        return pltpu.make_async_remote_copy(
            src_ref=src,
            dst_ref=dst,
            send_sem=self.send_sem.at[lane],
            recv_sem=self.recv_sem.at[k],
            device_id=dev,
            device_id_type=MESH,
        )

    def start(self, lane, k, src, dst, dev):
        self.make(lane, k, src, dst, dev).start()

    def arrive(self, k, span, dev):
        self.make(0, k, span, span, dev).wait_recv()

    def left(self, lane, span, dev):
        self.make(lane, 0, span, span, dev).wait_send()


class Exchange:
    def __init__(self, wires, lane, rings, span, k=None):
        self.w, self.lane, self.rings, self.span = wires, lane, rings, span
        self.k = k or {"relay": wires.new(), "rest": wires.new()}

    def go(self, sem, view, dev):
        self.w.start(self.lane, self.k[sem], view, view, dev)

    def await_blocks(self, sem, n):
        self.w.arrive(self.k[sem], self.span(n * len(self.rings)), self.rings[0][1])

    def first(self):
        for pos, plus, minus, part in self.rings:
            self.go("relay", part(pos, 0), plus)
            self.go("relay", part(pos, 1), minus)

    def second(self):
        for pos, plus, minus, part in self.rings:
            self.go("rest", part(pos, 1), plus)
            self.go("rest", part(pos, 0), minus)

    def start(self):
        self.first()
        self.second()

    def relay(self):
        self.await_blocks("relay", 1)
        for pos, plus, minus, part in self.rings:
            self.go("rest", part(lax.rem(pos + 3, 4), 0), plus)
            self.go("rest", part(lax.rem(pos + 1, 4), 1), minus)

    def rest(self):
        self.await_blocks("rest", 2)


class ChipExchange:
    def __init__(self, wires, lane, pos, plus, minus, mate, sizes, view, span, k=None):
        self.w, self.lane, self.pos, self.plus, self.minus, self.mate = wires, lane, pos, plus, minus, mate
        self.sizes, self.view, self.span = sizes, view, span
        names = ("relay0", "relay1", "near", "far0", "far1")
        self.k = {n: k[n] if k else wires.new() for n in names}
        self.k.update({n: wires.new() for n in ("mate_near", "mate_far")})

    def piece(self, shift, half, i):
        row = sum(self.sizes[0]) * half + (self.sizes[half][0] if i else 0)
        return self.view(lax.rem(self.pos + shift, 4), row, self.sizes[half][i])

    def half(self, shift, half):
        return self.view(lax.rem(self.pos + shift, 4), sum(self.sizes[0]) * half, sum(self.sizes[half]))

    def go(self, sem, view, dev):
        self.w.start(self.lane, self.k[sem], view, view, dev)

    def take(self, sem, blocks, rows, dev):
        self.w.arrive(self.k[sem], self.span(blocks, rows), dev)

    def rows(self, i):
        return self.sizes[0][i] + self.sizes[1][i]

    def start(self):
        for i in range(2):
            self.go(f"relay{i}", self.piece(0, 0, i), self.plus)
            self.go(f"relay{i}", self.piece(0, 1, i), self.minus)
        self.go("near", self.half(0, 1), self.plus)
        self.go("near", self.half(0, 0), self.minus)
        for h in range(2):
            self.go("mate_near", self.half(0, h), self.mate)

    def relay(self, i):
        self.take(f"relay{i}", 0, self.rows(i), self.plus)
        left, right = self.piece(3, 0, i), self.piece(1, 1, i)
        self.go(f"far{i}", left, self.plus)
        self.go(f"far{i}", right, self.minus)
        self.go("mate_near", left, self.mate)
        self.go("mate_near", right, self.mate)

    def near(self):
        self.take("near", 1, 0, self.plus)
        self.go("mate_near", self.half(3, 1), self.mate)
        self.go("mate_near", self.half(1, 0), self.mate)

    def far(self, i):
        self.take(f"far{i}", 0, self.rows(i), self.plus)
        self.go("mate_far", self.piece(2, 0, i), self.mate)
        self.go("mate_far", self.piece(2, 1, i), self.mate)

    def mate_near(self):
        self.take("mate_near", 3, 0, self.mate)

    def mate_far(self):
        self.take("mate_far", 1, 0, self.mate)


def dot(a, b):
    return jnp.dot(a, b, preferred_element_type=F32)


def dot_last(a, b):
    return lax.dot_general(a, b, (((1,), (1,)), ((), ())), preferred_element_type=F32)


def dot_first(a, b):
    return lax.dot_general(a, b, (((0,), (0,)), ((), ())), preferred_element_type=F32)


def rounded(v):
    return v.astype(BF16).astype(F32)


def two(v):
    high = v.astype(BF16)
    return high, (v - high.astype(F32)).astype(BF16)


def kernel(
    tokens, gain, w_f, w_i, w_q, w_o, w_v, w_g, w_gr, w_gc, lb, shift, sinit, hgain, ck, cgain, cbias, w_or, w_oc,
    out,
    tok, gainv, xs, wb, stage, lbv, shv, siv, hgv, ckv, cgv, cbv,
    kgb, cb, vb, qb, ogb, ext, hsend, hrecv, sgr, sgc, mc, mcn, mr, head, qd, stb, rbuf, sty, stz, kv, scales, acc,
    load_sem, send_sem, recv_sem,
):
    s, t = lax.axis_index("sp"), lax.axis_index("tp")
    z, y, x, c = s // 4, lax.rem(s, 4), t // 2, lax.rem(t, 2)
    w = Wires(send_sem, recv_sem)

    def at(zz, yy):
        return (lax.rem(zz + 4, 4) * 4 + lax.rem(yy + 4, 4), t)

    def across(xx):
        return (s, lax.rem(xx + 4, 4) * 2 + c)

    mate = (s, 1 - c + 2 * x)
    swap = (2 * t + lax.rem(s, 2), s // 2)
    home = s // 2 == t
    following, preceding = (lax.rem(s + 1, 16), t), (lax.rem(s + 15, 16), t)

    def load(k, src, dst):
        copy = pltpu.make_async_copy(src, dst, load_sem.at[k])
        copy.start()
        return copy

    first = [load(0, tokens, tok), load(1, gain, gainv)]
    for b, src in enumerate(
        (
            w_v, w_g, w_f, w_i, w_q, w_o,
            w_gr.at[:, pl.ds(0, 128)], w_gr.at[:, pl.ds(128, 128)],
            w_gc.at[:, pl.ds(0, 128)], w_gc.at[:, pl.ds(128, 128)],
        )
    ):
        load(2, src, wb.at[b, z, y])
    load(2, w_or, stage.at[0])
    load(2, w_oc, stage.at[1])
    twelve = wb.at[0, pl.ds(0, 3)]
    own = pltpu.make_async_copy(twelve, twelve, load_sem.at[2])
    rest = [
        load(k + 3, a, b)
        for k, (a, b) in enumerate(
            (
                (shift, shv), (lb, lbv), (sinit.at[0], siv), (hgain, hgv), (ck, ckv), (cgain, cgv), (cbias, cbv),
            )
        )
    ]

    barrier = pltpu.get_barrier_semaphore()
    partners = [at(z, y + 1), at(z, y - 1), at(z + 1, y), at(z - 1, y), across(x + 1), across(x - 1), mate]
    for dev in partners:
        pl.semaphore_signal(barrier, inc=1, device_id=dev, device_id_type=MESH)

    for there, dev in ((s > 0, preceding),):

        @pl.when(there)
        def _(dev=dev):
            pl.semaphore_signal(barrier, inc=1, device_id=dev, device_id_type=MESH)

    @pl.when(jnp.logical_not(home))
    def _():
        pl.semaphore_signal(barrier, inc=1, device_id=swap, device_id_type=MESH)

    def exchange(lane, sizes, view, span, k=None):
        return ChipExchange(w, lane, x, across(x + 1), across(x - 1), mate, sizes, view, span, k)

    def token_view(xx, row, rows):
        return xs.at[pl.ds(pl.multiple_of((xx * 2 + c) * TD + row, 16), rows), :]

    def block_view(buf):
        return lambda xx, row, rows: buf.at[xx * 2 + c, pl.ds(row, rows)]

    def block_span(buf):
        return lambda blocks, rows: buf.at[0, pl.ds(0, rows)] if rows else buf.at[pl.ds(0, blocks)]

    token_ring = exchange(
        1, ((32, 16), (32, 16)), token_view, lambda blocks, rows: xs.at[pl.ds(0, blocks * TD + rows), :]
    )
    conv_ring = exchange(2, ((192, 192), (192, 208)), block_view(mc), block_span(mc))
    rec_ring = exchange(3, ((192, 192), (192, 192)), block_view(mr), block_span(mr), token_ring.k)

    def along_y(part):
        return (y, at(z, y + 1), at(z, y - 1), part)

    def along_z(part):
        return (z, at(z + 1, y), at(z - 1, y), part)

    p1, p2 = [], []
    for g in range(6):
        a, b = 2 * g, 2 * g + 1
        rings = [
            along_y(lambda p, h, b=a: wb.at[b, z, p, pl.ds(64 * h, 64)]),
            along_z(lambda p, h, b=b: wb.at[b, p, y, pl.ds(64 * h, 64)]),
        ]
        p1.append(Exchange(w, 0, rings, lambda n, b=a: wb.at[b, 0, pl.ds(0, n)]))
        rings = [
            along_z(lambda p, h, b=a: wb.at[b, p, pl.ds(2 * h, 2)]),
            along_y(lambda p, h, b=b: wb.at[b, pl.ds(2 * h, 2), p]),
        ]
        p2.append(Exchange(w, 8, rings, lambda n, b=a: wb.at[b, pl.ds(0, n)], p1[g - 3].k if g > 2 else None))

    stz[...] = jnp.zeros_like(stz)
    sty[...] = jnp.zeros_like(sty)
    own.wait()
    count = len(partners) + jnp.where(home, 0, 1) + jnp.where(s < 15, 1, 0)
    pl.semaphore_wait(barrier, count)
    for g in range(3):
        p1[g].start()
    swap_k, y_k, z_k, h_k = (w.new() for _ in range(4))

    def place(i):
        return wb.at[10 + i, swap[0] // 4, lax.rem(swap[0], 4)]

    @pl.when(jnp.logical_not(home))
    def _():
        for i in range(2):
            w.start(4, swap_k, stage.at[i], place(i), swap)

    @pl.when(home)
    def _():
        for i in range(2):
            pltpu.make_async_copy(stage.at[i], wb.at[10 + i, z, y], recv_sem.at[swap_k]).start()

    def swapped():
        @pl.when(jnp.logical_not(home))
        def _():
            w.arrive(swap_k, stage, swap)
            w.left(4, stage, swap)

        @pl.when(home)
        def _():
            pltpu.make_async_copy(stage, stage, recv_sem.at[swap_k]).wait()

    for copy in first:
        copy.wait()
    base = pl.multiple_of(t * TD, 16)

    def normalize(r, _):
        wide = tok[pl.ds(pl.multiple_of(r * 16, 16), 16), :].astype(F32)
        scale = lax.rsqrt(jnp.mean(wide * wide, axis=-1, keepdims=True) + EPS)
        xs[pl.ds(pl.multiple_of(base + r * 16, 16), 16), :] = (wide * scale * gainv[...]).astype(BF16)
        return 0

    lax.fori_loop(0, TD // 16, normalize, 0, unroll=TD // 16)
    token_ring.start()

    def whole(b):
        return wb[b].reshape(2048, 128)

    def project(group, finish, size, starts):
        weight = jnp.concatenate([whole(2 * group), whole(2 * group + 1)], axis=1)

        def tile(r, _):
            start = pl.multiple_of(starts(r), 32)
            rows = pl.ds(start, size)
            finish(start, rows, dot(xs[rows, :], weight))
            return 0

        def run(low, high):
            lax.fori_loop(low, high, tile, 0, unroll=high - low if high - low > 1 else None)

        return run

    def project_all(group, finish):
        project(group, finish, PT, lambda r: r * PT)(0, T // PT)

    def by_ring(r):
        return lax.rem(x + jnp.where(r == 1, 3, jnp.where(r == 2, 1, jnp.where(r == 3, 2, 0))), 4) * XT

    def finish_fi(start, rows, v):
        gate = (1.0 - lbv[...]) * jax.nn.sigmoid(-rounded(v[:, :128]))
        kgb[rows, :] = gate
        cb[rows, :] = jnp.log1p(-gate) + shv[rows, :]
        vb[rows, :] = v[:, 128:].astype(BF16)

    def finish_vg(start, rows, v):
        gated = (rounded(v[:, :128]) * jax.nn.sigmoid(rounded(v[:, 128:]))).astype(BF16)
        ext[pl.ds(pl.multiple_of(start + HALO, 8), XT), :] = gated.astype(F32)

    def finish_qo(start, rows, v):
        raw = rounded(v[:, :128])
        qb[rows, :] = raw * jax.nn.sigmoid(raw)
        raw = rounded(v[:, 128:])
        ogb[rows, :] = raw * jax.nn.sigmoid(raw)

    def finish_gate(buf):
        def finish(start, rows, v):
            buf[rows, :] = jax.nn.sigmoid(rounded(v))

        return finish

    at_or_after = lax.broadcasted_iota(jnp.int32, (L, L), 0) >= lax.broadcasted_iota(jnp.int32, (L, L), 1)
    ones_below = jnp.where(at_or_after, 1.0, 0.0).astype(BF16)

    def pack_block(buf, i, decay, state):
        buf[i, pl.ds(0, HEAD), :] = state.astype(BF16)
        extra = jnp.concatenate([a.astype(F32) for a in two(decay)] + [jnp.zeros((14, HEAD), F32)], axis=0)
        buf[i, pl.ds(HEAD, 16), :] = extra.astype(BF16)

    def block_of(buf, i):
        both = buf[i, pl.ds(HEAD, 16), :].astype(F32)
        return both[0:1, :] + both[1:2, :], buf[i, pl.ds(0, HEAD), :].astype(F32)

    def local_states():
        for i in range(NC):
            rows = pl.ds(i * L, L)
            sides = dot(ones_below, jnp.concatenate(two(cb[rows, :]), axis=1))
            total = sides[:, :128] + sides[:, 128:]
            cb[rows, :] = total
            ending = (kgb[rows, :] * jnp.exp(total[L - 1 : L, :] - total)).astype(BF16)
            kv[i] = dot_first(vb[rows, :], ending)
        state = jnp.zeros((HEAD, HEAD), F32)
        before = jnp.zeros((1, HEAD), F32)
        for i in range(NC):
            last = cb[pl.ds(i * L + L - 1, 1), :]
            stb[i] = state.astype(BF16)
            rbuf[pl.ds(i, 1), :] = before
            state = jnp.exp(last) * state + kv[i]
            before = before + last
        pack_block(sty, y, jnp.exp(before), state)

    def local_outputs():
        for i in range(NC):
            rows = pl.ds(i * L, L)
            total, q = cb[rows, :], qb[rows, :]
            middle = 0.5 * total[L - 1 : L, :]
            left = (q * jnp.exp(total - middle)).astype(BF16)
            right = (kgb[rows, :] * jnp.exp(middle - total)).astype(BF16)
            scores = jnp.where(at_or_after, dot_last(left, right), 0.0).astype(BF16)
            o = dot(scores, vb[rows, :])
            o = o + dot_last((q * jnp.exp(total)).astype(BF16), stb[i])
            head[rows, :] = o
            qd[rows, :] = (q * jnp.exp(total + rbuf[pl.ds(i, 1), :])).astype(BF16)

    def convolve(low, high):
        for i in range(low, high):
            acc = jnp.zeros((128, HEAD), F32)
            for j in range(KW):
                acc = acc + ckv[pl.ds(j, 1), :] * ext[pl.ds(i * 128 + HALO - KW + 1 + j, 128), :]
            mc[t, pl.ds(i * 128, 128), :] = acc.astype(BF16)

    def take_halo():
        @pl.when(s > 0)
        def _():
            w.arrive(h_k, hrecv, preceding)
            ext[pl.ds(0, HALO), :] = hrecv[...].astype(F32)

        @pl.when(s == 0)
        def _():
            ext[pl.ds(0, HALO), :] = jnp.zeros((HALO, HEAD), F32)

    def take_z():
        for i in (1, 2, 3):

            @pl.when(z == i)
            def _(i=i):
                w.arrive(z_k, stz.at[pl.ds(0, i), pl.ds(0, 130)], at(z + 1, y))

    def chip_weight(b, xx):
        top, low = ([wb[b, xx, 2 * k + j] for j in range(2)] for k in range(2))
        return jnp.concatenate([jnp.concatenate(top, axis=1), jnp.concatenate(low, axis=1)], axis=0)

    def chip_blocks(rows, xx):
        return jnp.concatenate([mr[2 * xx, rows, :], mr[2 * xx + 1, rows, :]], axis=1)

    p1[0].relay()
    p1[1].relay()
    p1[3].start()
    p1[4].start()
    p1[2].relay()
    p1[0].rest()
    p2[0].start()
    p1[1].rest()
    p2[1].first()
    token_ring.relay(0)
    token_ring.relay(1)
    p2[0].relay()
    p2[1].second()
    token_ring.near()
    p1[2].rest()
    p2[1].relay()
    p2[2].first()
    p1[3].relay()
    p1[4].relay()
    swapped()
    p1[5].start()
    for copy in rest:
        copy.wait()
    token_ring.far(0)
    token_ring.far(1)
    p2[0].rest()
    p2[2].second()
    token_ring.mate_near()
    project_vg = project(0, finish_vg, XT, by_ring)
    project_vg(0, 3)
    token_ring.mate_far()
    project_vg(3, 4)
    hsend[...] = ext[pl.ds(T, HALO), :].astype(BF16)

    @pl.when(s < 15)
    def _():
        w.start(5, h_k, hsend, hrecv, following)

    p2[1].rest()
    project_all(1, finish_fi)
    local_states()
    for i in (2, 1, 3):
        w.start(6, y_k, sty.at[y, pl.ds(0, 130)], sty.at[y, pl.ds(0, 130)], at(z, y + i))

    p2[2].relay()
    p1[3].rest()
    p1[5].relay()
    p2[3].start()
    convolve(1, T // 128)
    extra = [a.astype(F32) for v in (cgv[...], cbv[...]) for a in two(v)]
    mc[t, pl.ds(T, 16), :] = jnp.concatenate(extra + [jnp.zeros((12, HEAD), F32)], axis=0).astype(BF16)
    take_halo()
    convolve(0, 1)
    conv_ring.start()
    w.arrive(y_k, sty.at[pl.ds(0, 3), pl.ds(0, 130)], at(z, y + 1))
    row_decay, row_state = jnp.ones((1, HEAD), F32), jnp.zeros((HEAD, HEAD), F32)
    my_decay, my_state = row_decay, row_state
    for i in range(4):
        d, v = block_of(sty, i)
        row_decay, row_state = row_decay * d, d * row_state + v
        if i < 3:
            take = i < y
            my_decay = jnp.where(take, row_decay, my_decay)
            my_state = jnp.where(take, row_state, my_state)
    pack_block(stz, z, row_decay, row_state)
    for i in (2, 1, 3):

        @pl.when(z + i < 4)
        def _(i=i):
            w.start(7, z_k, stz.at[z, pl.ds(0, 130)], stz.at[z, pl.ds(0, 130)], at(z + i, y))


    p1[5].rest()
    p2[5].first()
    p2[2].rest()
    project_all(2, finish_qo)
    conv_ring.relay(0)
    conv_ring.relay(1)
    p2[3].relay()
    p2[5].second()
    local_outputs()
    p1[4].rest()
    p2[4].start()
    take_z()
    entering = siv[...].T
    for i in range(3):
        d, v = block_of(stz, i)
        entering = jnp.where(i < z, d * entering + v, entering)
    entering = (my_decay * entering + my_state).astype(BF16)

    def finish_head(low, high):
        for r in range(low, high):
            rows = pl.ds(r * 128, 128)
            h = head[rows, :] + dot_last(qd[rows, :], entering)
            h = h * lax.rsqrt(jnp.mean(h * h, axis=-1, keepdims=True) + EPS) * hgv[...]
            mr[t, rows, :] = (h * ogb[rows, :]).astype(BF16)

    finish_head(0, T // 128)
    rec_ring.start()
    conv_ring.near()
    p2[5].relay()
    conv_ring.far(0)
    conv_ring.far(1)
    rec_ring.relay(0)
    conv_ring.mate_near()
    conv_ring.mate_far()

    def conv_scale(r, _):
        rows = pl.ds(pl.multiple_of(r * 64, 64), 64)
        squares = sum(v * v for v in (mc[k, rows, :].astype(F32) for k in range(8)))
        scale = lax.rsqrt(jnp.sum(squares, axis=-1, keepdims=True) * (1.0 / CONV) + EPS)
        scales[rows, :] = jnp.broadcast_to(scale, (64, 128))
        return 0

    gains, biases = [], []
    for k in range(8):
        four = mc[k, pl.ds(T, 16), :].astype(F32)
        gains.append(0.5 * (four[0:1, :] + four[1:2, :]))
        biases.append(0.5 * (four[2:3, :] + four[3:4, :]))

    def normalize_conv(r, _):
        rows = pl.ds(pl.multiple_of(r * 64, 64), 64)
        scale = scales[rows, :]
        for k in range(8):
            half = mc[k, rows, :].astype(F32) * scale * gains[k] + biases[k]
            mcn[rows, pl.ds(k * 128, 128)] = (half + half * jnp.tanh(half)).astype(BF16)
        return 0

    lax.fori_loop(0, T // 64, conv_scale, 0, unroll=4)
    rec_ring.relay(1)
    p2[4].relay()
    p2[3].rest()
    project_all(3, finish_gate(sgr))
    rec_ring.near()
    lax.fori_loop(0, T // 64, normalize_conv, 0, unroll=2)
    p2[5].rest()
    w_conv = jnp.concatenate([chip_weight(11, xx) for xx in range(4)], axis=0)

    def conv_tile(r, _):
        rows = pl.ds(pl.multiple_of(r * PT, PT), PT)
        sgc[rows, :] = rounded(dot(mcn[rows, :], w_conv))
        return 0

    lax.fori_loop(0, T // PT, conv_tile, 0, unroll=2)
    rec_ring.far(0)
    rec_ring.far(1)
    rec_ring.mate_near()
    near = [x, lax.rem(x + 1, 4), lax.rem(x + 3, 4)]
    w_near = jnp.concatenate([chip_weight(10, xx) for xx in near], axis=0)

    def near_tile(r, _):
        rows = pl.ds(pl.multiple_of(r * PT, PT), PT)
        acc[rows, :] = dot(jnp.concatenate([chip_blocks(rows, xx) for xx in near], axis=1), w_near)
        return 0

    lax.fori_loop(0, T // PT, near_tile, 0, unroll=2)
    p2[4].rest()

    def finish_gc(start, rows, v):
        sgc[rows, :] = jax.nn.sigmoid(rounded(v)) * sgc[rows, :]

    project_all(4, finish_gc)
    rec_ring.mate_far()
    opposite = lax.rem(x + 2, 4)
    w_far = chip_weight(10, opposite)

    def last_tile(r, _):
        rows = pl.ds(pl.multiple_of(r * RT, RT), RT)
        y_rec = rounded(acc[rows, :] + dot(chip_blocks(rows, opposite), w_far))
        out[rows, :] = (sgr[rows, :] * y_rec + sgc[rows, :]).astype(BF16)
        return 0

    lax.fori_loop(0, T // RT, last_tile, 0, unroll=3)
    w.left(0, wb.at[pl.ds(0, 3), pl.ds(0, 3)], mate)
    w.left(8, wb.at[pl.ds(0, 9)], mate)
    w.left(1, xs.at[pl.ds(0, 7 * TD), :], mate)
    w.left(2, mc.at[pl.ds(0, 7)], mate)
    w.left(3, mr.at[pl.ds(0, 7)], mate)

    @pl.when(s < 15)
    def _():
        w.left(5, hsend, following)

    w.left(6, sty.at[pl.ds(0, 3), pl.ds(0, 130)], mate)
    for i in (1, 2, 3):

        @pl.when(z == 3 - i)
        def _(i=i):
            w.left(7, stz.at[pl.ds(0, i), pl.ds(0, 130)], mate)


def local(
    tokens, norm_gain, w_query, w_forget, w_input, w_outgate, w_conv_value, w_conv_gate, w_gate_rec, w_gate_conv,
    lower_bound, decay_shift, state_init, head_gain, conv_kernel, channel_gain, channel_bias, w_out_rec, w_out_conv,
):
    line = lambda v: v.reshape(1, -1)
    args = (
        tokens, line(norm_gain), w_forget, w_input, w_query, w_outgate, w_conv_value, w_conv_gate, w_gate_rec,
        w_gate_conv, line(lower_bound), decay_shift, state_init, line(head_gain), conv_kernel, line(channel_gain),
        line(channel_bias), w_out_rec, w_out_conv,
    )
    v = pltpu.VMEM
    scratch = [
        v((TD, 2048), BF16), v((1, 2048), F32), v((T, 2048), BF16), v((12, 4, 4, 128, 128), BF16),
        v((2, 128, 128), BF16), v((1, 128), F32), v((T, 128), F32), v((128, 128), F32), v((1, 128), F32),
        v((KW, 128), F32), v((1, 128), F32), v((1, 128), F32),
        v((T, 128), F32), v((T, 128), F32), v((T, 128), BF16), v((T, 128), F32), v((T, 128), F32),
        v((T + HALO, 128), F32), v((HALO, 128), BF16), v((HALO, 128), BF16), v((T, 256), F32), v((T, 256), F32),
        v((8, T + 16, 128), BF16), v((T, CONV), BF16), v((8, T, 128), BF16), v((T, 128), F32), v((T, 128), BF16),
        v((NC, 128, 128), BF16), v((16, 128), F32), v((4, 144, 128), BF16), v((4, 144, 128), BF16), v((NC, 128, 128), F32), v((T, 128), F32), v((T, 256), F32),
        pltpu.SemaphoreType.DMA((10,)), pltpu.SemaphoreType.DMA((9,)), pltpu.SemaphoreType.DMA((38,)),
    ]
    return pl.pallas_call(
        kernel,
        out_shape=jax.ShapeDtypeStruct((T, 256), BF16),
        in_specs=[pl.BlockSpec(memory_space=pltpu.HBM)] * len(args),
        out_specs=pl.BlockSpec(memory_space=pltpu.VMEM),
        scratch_shapes=scratch,
        compiler_params=pltpu.CompilerParams(
            collective_id=0, has_side_effects=True, vmem_limit_bytes=40 * 1024 * 1024
        ),
    )(*[pltpu.with_memory_space_constraint(a, pltpu.HBM) for a in args])


def solution(mesh):
    both = P("sp", "tp")
    in_specs = (
        P(("sp", "tp"), None), P(), both, both, both, both, both, both, both, both, P("tp"), both,
        P("tp", None, None), P("tp"), P(None, "tp"), P("tp"), P("tp"), P("tp", "sp"), P("tp", "sp"),
    )
    return jax.shard_map(local, mesh=mesh, in_specs=in_specs, out_specs=both, check_vma=False)
```

```python
import functools

import jax
import jax.numpy as jnp
from jax import lax
from jax.experimental import pallas as pl
from jax.experimental.pallas import tpu as pltpu
from jax.sharding import PartitionSpec as P

MESH = pl.DeviceIdType.MESH
F32 = jnp.float32
BF16 = jnp.bfloat16
HEAD = 128
CONV = 1024
KW = 31
EPS = 1e-06
L = 64
T = 768
NC = T // L
TD = 96
RT = 256
XT = 192
PT = 384
HALO = 32


class Wires:
    def __init__(self, send_sem, recv_sem):
        self.send_sem, self.recv_sem = send_sem, recv_sem
        self.count = 0

    def new(self):
        self.count += 1
        return self.count - 1

    def make(self, lane, k, src, dst, dev):
        return pltpu.make_async_remote_copy(
            src_ref=src,
            dst_ref=dst,
            send_sem=self.send_sem.at[lane],
            recv_sem=self.recv_sem.at[k],
            device_id=dev,
            device_id_type=MESH,
        )

    def start(self, lane, k, src, dst, dev):
        self.make(lane, k, src, dst, dev).start()

    def arrive(self, k, span, dev):
        self.make(0, k, span, span, dev).wait_recv()

    def left(self, lane, span, dev):
        self.make(lane, 0, span, span, dev).wait_send()


class Exchange:
    def __init__(self, wires, lane, rings, span, k=None):
        self.w, self.lane, self.rings, self.span = wires, lane, rings, span
        self.k = k or {"relay": wires.new(), "rest": wires.new()}

    def go(self, sem, view, dev):
        self.w.start(self.lane, self.k[sem], view, view, dev)

    def await_blocks(self, sem, n):
        self.w.arrive(self.k[sem], self.span(n * len(self.rings)), self.rings[0][1])

    def first(self):
        for pos, plus, minus, part in self.rings:
            self.go("relay", part(pos, 0), plus)
            self.go("relay", part(pos, 1), minus)

    def second(self):
        for pos, plus, minus, part in self.rings:
            self.go("rest", part(pos, 1), plus)
            self.go("rest", part(pos, 0), minus)

    def start(self):
        self.first()
        self.second()

    def relay(self):
        self.await_blocks("relay", 1)
        for pos, plus, minus, part in self.rings:
            self.go("rest", part(lax.rem(pos + 3, 4), 0), plus)
            self.go("rest", part(lax.rem(pos + 1, 4), 1), minus)

    def rest(self):
        self.await_blocks("rest", 2)


class ChipExchange:
    def __init__(self, wires, lane, pos, plus, minus, mate, sizes, view, span, k=None):
        self.w, self.lane, self.pos, self.plus, self.minus, self.mate = wires, lane, pos, plus, minus, mate
        self.sizes, self.view, self.span = sizes, view, span
        names = ("relay0", "relay1", "near", "far0", "far1")
        self.k = {n: k[n] if k else wires.new() for n in names}
        self.k.update({n: wires.new() for n in ("mate_near", "mate_far")})

    def piece(self, shift, half, i):
        row = sum(self.sizes[0]) * half + (self.sizes[half][0] if i else 0)
        return self.view(lax.rem(self.pos + shift, 4), row, self.sizes[half][i])

    def half(self, shift, half):
        return self.view(lax.rem(self.pos + shift, 4), sum(self.sizes[0]) * half, sum(self.sizes[half]))

    def go(self, sem, view, dev):
        self.w.start(self.lane, self.k[sem], view, view, dev)

    def take(self, sem, blocks, rows, dev):
        self.w.arrive(self.k[sem], self.span(blocks, rows), dev)

    def rows(self, i):
        return self.sizes[0][i] + self.sizes[1][i]

    def start(self):
        for i in range(2):
            self.go(f"relay{i}", self.piece(0, 0, i), self.plus)
            self.go(f"relay{i}", self.piece(0, 1, i), self.minus)
        self.go("near", self.half(0, 1), self.plus)
        self.go("near", self.half(0, 0), self.minus)
        for h in range(2):
            self.go("mate_near", self.half(0, h), self.mate)

    def relay(self, i):
        self.take(f"relay{i}", 0, self.rows(i), self.plus)
        left, right = self.piece(3, 0, i), self.piece(1, 1, i)
        self.go(f"far{i}", left, self.plus)
        self.go(f"far{i}", right, self.minus)
        self.go("mate_near", left, self.mate)
        self.go("mate_near", right, self.mate)

    def near(self):
        self.take("near", 1, 0, self.plus)
        self.go("mate_near", self.half(3, 1), self.mate)
        self.go("mate_near", self.half(1, 0), self.mate)

    def far(self, i):
        self.take(f"far{i}", 0, self.rows(i), self.plus)
        self.go("mate_far", self.piece(2, 0, i), self.mate)
        self.go("mate_far", self.piece(2, 1, i), self.mate)

    def mate_near(self):
        self.take("mate_near", 3, 0, self.mate)

    def mate_far(self):
        self.take("mate_far", 1, 0, self.mate)


def dot(a, b):
    return jnp.dot(a, b, preferred_element_type=F32)


def dot_last(a, b):
    return lax.dot_general(a, b, (((1,), (1,)), ((), ())), preferred_element_type=F32)


def dot_first(a, b):
    return lax.dot_general(a, b, (((0,), (0,)), ((), ())), preferred_element_type=F32)


def rounded(v):
    return v.astype(BF16).astype(F32)


def two(v):
    high = v.astype(BF16)
    return high, (v - high.astype(F32)).astype(BF16)


def kernel(
    tokens, gain, w_f, w_i, w_q, w_o, w_v, w_g, w_gr, w_gc, lb, shift, sinit, hgain, ck, cgain, cbias, w_or, w_oc,
    out,
    tok, gainv, xs, wb, stage, lbv, shv, siv, hgv, ckv, cgv, cbv,
    kgb, cb, vb, qb, ogb, ext, hsend, hrecv, sgr, sgc, mc, mcn, mr, head, qd, stb, rbuf, sty, stz, kv, scales, acc,
    load_sem, send_sem, recv_sem,
):
    s, t = lax.axis_index("sp"), lax.axis_index("tp")
    z, y, x, c = s // 4, lax.rem(s, 4), t // 2, lax.rem(t, 2)
    w = Wires(send_sem, recv_sem)

    def at(zz, yy):
        return (lax.rem(zz + 4, 4) * 4 + lax.rem(yy + 4, 4), t)

    def across(xx):
        return (s, lax.rem(xx + 4, 4) * 2 + c)

    mate = (s, 1 - c + 2 * x)
    swap = (2 * t + lax.rem(s, 2), s // 2)
    home = s // 2 == t
    following, preceding = (lax.rem(s + 1, 16), t), (lax.rem(s + 15, 16), t)

    def load(k, src, dst):
        copy = pltpu.make_async_copy(src, dst, load_sem.at[k])
        copy.start()
        return copy

    first = [load(0, tokens, tok), load(1, gain, gainv)]
    for b, src in enumerate(
        (
            w_v, w_g, w_f, w_i, w_q, w_o,
            w_gr.at[:, pl.ds(0, 128)], w_gr.at[:, pl.ds(128, 128)],
            w_gc.at[:, pl.ds(0, 128)], w_gc.at[:, pl.ds(128, 128)],
        )
    ):
        load(2, src, wb.at[b, z, y])
    load(2, w_or, stage.at[0])
    load(2, w_oc, stage.at[1])
    twelve = wb.at[0, pl.ds(0, 3)]
    own = pltpu.make_async_copy(twelve, twelve, load_sem.at[2])
    rest = [
        load(k + 3, a, b)
        for k, (a, b) in enumerate(
            (
                (shift, shv), (lb, lbv), (sinit.at[0], siv), (hgain, hgv), (ck, ckv), (cgain, cgv), (cbias, cbv),
            )
        )
    ]

    barrier = pltpu.get_barrier_semaphore()
    partners = [at(z, y + 1), at(z, y - 1), at(z + 1, y), at(z - 1, y), across(x + 1), across(x - 1), mate]
    for dev in partners:
        pl.semaphore_signal(barrier, inc=1, device_id=dev, device_id_type=MESH)

    for there, dev in ((s > 0, preceding),):

        @pl.when(there)
        def _(dev=dev):
            pl.semaphore_signal(barrier, inc=1, device_id=dev, device_id_type=MESH)

    @pl.when(jnp.logical_not(home))
    def _():
        pl.semaphore_signal(barrier, inc=1, device_id=swap, device_id_type=MESH)

    def exchange(lane, sizes, view, span, k=None):
        return ChipExchange(w, lane, x, across(x + 1), across(x - 1), mate, sizes, view, span, k)

    def token_view(xx, row, rows):
        return xs.at[pl.ds(pl.multiple_of((xx * 2 + c) * TD + row, 16), rows), :]

    def block_view(buf):
        return lambda xx, row, rows: buf.at[xx * 2 + c, pl.ds(row, rows)]

    def block_span(buf):
        return lambda blocks, rows: buf.at[0, pl.ds(0, rows)] if rows else buf.at[pl.ds(0, blocks)]

    token_ring = exchange(
        1, ((32, 16), (32, 16)), token_view, lambda blocks, rows: xs.at[pl.ds(0, blocks * TD + rows), :]
    )
    conv_ring = exchange(2, ((192, 192), (192, 208)), block_view(mc), block_span(mc))
    rec_ring = exchange(3, ((192, 192), (192, 192)), block_view(mr), block_span(mr), token_ring.k)

    def along_y(part):
        return (y, at(z, y + 1), at(z, y - 1), part)

    def along_z(part):
        return (z, at(z + 1, y), at(z - 1, y), part)

    p1, p2 = [], []
    for g in range(6):
        a, b = 2 * g, 2 * g + 1
        rings = [
            along_y(lambda p, h, b=a: wb.at[b, z, p, pl.ds(64 * h, 64)]),
            along_z(lambda p, h, b=b: wb.at[b, p, y, pl.ds(64 * h, 64)]),
        ]
        p1.append(Exchange(w, 0, rings, lambda n, b=a: wb.at[b, 0, pl.ds(0, n)]))
        rings = [
            along_z(lambda p, h, b=a: wb.at[b, p, pl.ds(2 * h, 2)]),
            along_y(lambda p, h, b=b: wb.at[b, pl.ds(2 * h, 2), p]),
        ]
        p2.append(Exchange(w, 8, rings, lambda n, b=a: wb.at[b, pl.ds(0, n)], p1[g - 3].k if g > 2 else None))

    stz[...] = jnp.zeros_like(stz)
    sty[...] = jnp.zeros_like(sty)
    own.wait()
    count = len(partners) + jnp.where(home, 0, 1) + jnp.where(s < 15, 1, 0)
    pl.semaphore_wait(barrier, count)
    for g in range(3):
        p1[g].start()
    swap_k, y_k, z_k, h_k = (w.new() for _ in range(4))

    def place(i):
        return wb.at[10 + i, swap[0] // 4, lax.rem(swap[0], 4)]

    @pl.when(jnp.logical_not(home))
    def _():
        for i in range(2):
            w.start(4, swap_k, stage.at[i], place(i), swap)

    @pl.when(home)
    def _():
        for i in range(2):
            pltpu.make_async_copy(stage.at[i], wb.at[10 + i, z, y], recv_sem.at[swap_k]).start()

    def swapped():
        @pl.when(jnp.logical_not(home))
        def _():
            w.arrive(swap_k, stage, swap)
            w.left(4, stage, swap)

        @pl.when(home)
        def _():
            pltpu.make_async_copy(stage, stage, recv_sem.at[swap_k]).wait()

    for copy in first:
        copy.wait()
    base = pl.multiple_of(t * TD, 16)

    def normalize(r, _):
        wide = tok[pl.ds(pl.multiple_of(r * 16, 16), 16), :].astype(F32)
        scale = lax.rsqrt(jnp.mean(wide * wide, axis=-1, keepdims=True) + EPS)
        xs[pl.ds(pl.multiple_of(base + r * 16, 16), 16), :] = (wide * scale * gainv[...]).astype(BF16)
        return 0

    lax.fori_loop(0, TD // 16, normalize, 0, unroll=TD // 16)
    token_ring.start()

    def whole(b):
        return wb[b].reshape(2048, 128)

    def project(group, finish, size, starts):
        weight = jnp.concatenate([whole(2 * group), whole(2 * group + 1)], axis=1)

        def tile(r, _):
            start = pl.multiple_of(starts(r), 32)
            rows = pl.ds(start, size)
            finish(start, rows, dot(xs[rows, :], weight))
            return 0

        def run(low, high):
            lax.fori_loop(low, high, tile, 0, unroll=high - low if high - low > 1 else None)

        return run

    def project_all(group, finish):
        project(group, finish, PT, lambda r: r * PT)(0, T // PT)

    def by_ring(r):
        return lax.rem(x + jnp.where(r == 1, 3, jnp.where(r == 2, 1, jnp.where(r == 3, 2, 0))), 4) * XT

    def finish_fi(start, rows, v):
        gate = (1.0 - lbv[...]) * jax.nn.sigmoid(-rounded(v[:, :128]))
        kgb[rows, :] = gate
        cb[rows, :] = jnp.log1p(-gate) + shv[rows, :]
        vb[rows, :] = v[:, 128:].astype(BF16)

    def finish_vg(start, rows, v):
        gated = (rounded(v[:, :128]) * jax.nn.sigmoid(rounded(v[:, 128:]))).astype(BF16)
        ext[pl.ds(pl.multiple_of(start + HALO, 8), XT), :] = gated.astype(F32)

    def finish_qo(start, rows, v):
        raw = rounded(v[:, :128])
        qb[rows, :] = raw * jax.nn.sigmoid(raw)
        raw = rounded(v[:, 128:])
        ogb[rows, :] = raw * jax.nn.sigmoid(raw)

    def finish_gate(buf):
        def finish(start, rows, v):
            buf[rows, :] = jax.nn.sigmoid(rounded(v))

        return finish

    at_or_after = lax.broadcasted_iota(jnp.int32, (L, L), 0) >= lax.broadcasted_iota(jnp.int32, (L, L), 1)
    ones_below = jnp.where(at_or_after, 1.0, 0.0).astype(BF16)

    def pack_block(buf, i, decay, state):
        buf[i, pl.ds(0, HEAD), :] = state.astype(BF16)
        extra = jnp.concatenate([a.astype(F32) for a in two(decay)] + [jnp.zeros((14, HEAD), F32)], axis=0)
        buf[i, pl.ds(HEAD, 16), :] = extra.astype(BF16)

    def block_of(buf, i):
        both = buf[i, pl.ds(HEAD, 16), :].astype(F32)
        return both[0:1, :] + both[1:2, :], buf[i, pl.ds(0, HEAD), :].astype(F32)

    def local_states():
        for i in range(NC):
            rows = pl.ds(i * L, L)
            sides = dot(ones_below, jnp.concatenate(two(cb[rows, :]), axis=1))
            total = sides[:, :128] + sides[:, 128:]
            cb[rows, :] = total
            ending = (kgb[rows, :] * jnp.exp(total[L - 1 : L, :] - total)).astype(BF16)
            kv[i] = dot_first(vb[rows, :], ending)
        state = jnp.zeros((HEAD, HEAD), F32)
        before = jnp.zeros((1, HEAD), F32)
        for i in range(NC):
            last = cb[pl.ds(i * L + L - 1, 1), :]
            stb[i] = state.astype(BF16)
            rbuf[pl.ds(i, 1), :] = before
            state = jnp.exp(last) * state + kv[i]
            before = before + last
        pack_block(sty, y, jnp.exp(before), state)

    def local_outputs():
        for i in range(NC):
            rows = pl.ds(i * L, L)
            total, q = cb[rows, :], qb[rows, :]
            middle = 0.5 * total[L - 1 : L, :]
            left = (q * jnp.exp(total - middle)).astype(BF16)
            right = (kgb[rows, :] * jnp.exp(middle - total)).astype(BF16)
            scores = jnp.where(at_or_after, dot_last(left, right), 0.0).astype(BF16)
            o = dot(scores, vb[rows, :])
            o = o + dot_last((q * jnp.exp(total)).astype(BF16), stb[i])
            head[rows, :] = o
            qd[rows, :] = (q * jnp.exp(total + rbuf[pl.ds(i, 1), :])).astype(BF16)

    def convolve(low, high):
        for i in range(low, high):
            acc = jnp.zeros((128, HEAD), F32)
            for j in range(KW):
                acc = acc + ckv[pl.ds(j, 1), :] * ext[pl.ds(i * 128 + HALO - KW + 1 + j, 128), :]
            mc[t, pl.ds(i * 128, 128), :] = acc.astype(BF16)

    def take_halo():
        @pl.when(s > 0)
        def _():
            w.arrive(h_k, hrecv, preceding)
            ext[pl.ds(0, HALO), :] = hrecv[...].astype(F32)

        @pl.when(s == 0)
        def _():
            ext[pl.ds(0, HALO), :] = jnp.zeros((HALO, HEAD), F32)

    def take_z():
        for i in (1, 2, 3):

            @pl.when(z == i)
            def _(i=i):
                w.arrive(z_k, stz.at[pl.ds(0, i), pl.ds(0, 130)], at(z + 1, y))

    def chip_weight(b, xx):
        top, low = ([wb[b, xx, 2 * k + j] for j in range(2)] for k in range(2))
        return jnp.concatenate([jnp.concatenate(top, axis=1), jnp.concatenate(low, axis=1)], axis=0)

    def chip_blocks(rows, xx):
        return jnp.concatenate([mr[2 * xx, rows, :], mr[2 * xx + 1, rows, :]], axis=1)

    p1[0].relay()
    p1[1].relay()
    p1[3].start()
    p1[4].start()
    p1[2].relay()
    p1[0].rest()
    p2[0].start()
    p1[1].rest()
    p2[1].first()
    token_ring.relay(0)
    token_ring.relay(1)
    p2[0].relay()
    p2[1].second()
    token_ring.near()
    p1[2].rest()
    p2[1].relay()
    p2[2].first()
    p1[3].relay()
    p1[4].relay()
    swapped()
    p1[5].start()
    for copy in rest:
        copy.wait()
    token_ring.far(0)
    token_ring.far(1)
    p2[0].rest()
    p2[2].second()
    token_ring.mate_near()
    project_vg = project(0, finish_vg, XT, by_ring)
    project_vg(0, 3)
    token_ring.mate_far()
    project_vg(3, 4)
    hsend[...] = ext[pl.ds(T, HALO), :].astype(BF16)

    @pl.when(s < 15)
    def _():
        w.start(5, h_k, hsend, hrecv, following)

    p2[1].rest()
    project_all(1, finish_fi)
    local_states()
    for i in (2, 1, 3):

        @pl.when((z < 3) | (y + i < 4))
        def _(i=i):
            w.start(6, y_k, sty.at[y, pl.ds(0, 130)], sty.at[y, pl.ds(0, 130)], at(z, y + i))


    p2[2].relay()
    p1[3].rest()
    p1[5].relay()
    p2[3].start()
    convolve(1, T // 128)
    extra = [a.astype(F32) for v in (cgv[...], cbv[...]) for a in two(v)]
    mc[t, pl.ds(T, 16), :] = jnp.concatenate(extra + [jnp.zeros((12, HEAD), F32)], axis=0).astype(BF16)
    take_halo()
    convolve(0, 1)
    conv_ring.start()
    for i in (1, 2, 3):

        @pl.when((z == 3) & (y == i) if i < 3 else (z < 3) | (y == 3))
        def _(i=i):
            w.arrive(y_k, sty.at[pl.ds(0, i), pl.ds(0, 130)], at(z, y + 1))

    row_decay, row_state = jnp.ones((1, HEAD), F32), jnp.zeros((HEAD, HEAD), F32)
    my_decay, my_state = row_decay, row_state
    for i in range(4):
        d, v = block_of(sty, i)
        row_decay, row_state = row_decay * d, d * row_state + v
        if i < 3:
            take = i < y
            my_decay = jnp.where(take, row_decay, my_decay)
            my_state = jnp.where(take, row_state, my_state)
    pack_block(stz, z, row_decay, row_state)
    for i in (2, 1, 3):

        @pl.when(z + i < 4)
        def _(i=i):
            w.start(7, z_k, stz.at[z, pl.ds(0, 130)], stz.at[z, pl.ds(0, 130)], at(z + i, y))


    p1[5].rest()
    p2[5].first()
    p2[2].rest()
    project_all(2, finish_qo)
    conv_ring.relay(0)
    conv_ring.relay(1)
    p2[3].relay()
    p2[5].second()
    local_outputs()
    p1[4].rest()
    p2[4].start()
    take_z()
    entering = siv[...].T
    for i in range(3):
        d, v = block_of(stz, i)
        entering = jnp.where(i < z, d * entering + v, entering)
    entering = (my_decay * entering + my_state).astype(BF16)

    def finish_head(low, high):
        for r in range(low, high):
            rows = pl.ds(r * 128, 128)
            h = head[rows, :] + dot_last(qd[rows, :], entering)
            h = h * lax.rsqrt(jnp.mean(h * h, axis=-1, keepdims=True) + EPS) * hgv[...]
            mr[t, rows, :] = (h * ogb[rows, :]).astype(BF16)

    finish_head(0, T // 128)
    rec_ring.start()
    conv_ring.near()
    p2[5].relay()
    conv_ring.far(0)
    conv_ring.far(1)
    rec_ring.relay(0)
    conv_ring.mate_near()
    conv_ring.mate_far()

    def conv_scale(r, _):
        rows = pl.ds(pl.multiple_of(r * 64, 64), 64)
        squares = sum(v * v for v in (mc[k, rows, :].astype(F32) for k in range(8)))
        scale = lax.rsqrt(jnp.sum(squares, axis=-1, keepdims=True) * (1.0 / CONV) + EPS)
        scales[rows, :] = jnp.broadcast_to(scale, (64, 128))
        return 0

    gains, biases = [], []
    for k in range(8):
        four = mc[k, pl.ds(T, 16), :].astype(F32)
        gains.append(0.5 * (four[0:1, :] + four[1:2, :]))
        biases.append(0.5 * (four[2:3, :] + four[3:4, :]))

    def normalize_conv(r, _):
        rows = pl.ds(pl.multiple_of(r * 64, 64), 64)
        scale = scales[rows, :]
        for k in range(8):
            half = mc[k, rows, :].astype(F32) * scale * gains[k] + biases[k]
            mcn[rows, pl.ds(k * 128, 128)] = (half + half * jnp.tanh(half)).astype(BF16)
        return 0

    lax.fori_loop(0, T // 64, conv_scale, 0, unroll=4)
    rec_ring.relay(1)
    p2[4].relay()
    p2[3].rest()
    project_all(3, finish_gate(sgr))
    rec_ring.near()
    lax.fori_loop(0, T // 64, normalize_conv, 0, unroll=2)
    p2[5].rest()
    w_conv = jnp.concatenate([chip_weight(11, xx) for xx in range(4)], axis=0)

    def conv_tile(r, _):
        rows = pl.ds(pl.multiple_of(r * PT, PT), PT)
        sgc[rows, :] = rounded(dot(mcn[rows, :], w_conv))
        return 0

    lax.fori_loop(0, T // PT, conv_tile, 0, unroll=2)
    rec_ring.far(0)
    rec_ring.far(1)
    rec_ring.mate_near()
    near = [x, lax.rem(x + 1, 4), lax.rem(x + 3, 4)]
    w_near = jnp.concatenate([chip_weight(10, xx) for xx in near], axis=0)

    def near_tile(r, _):
        rows = pl.ds(pl.multiple_of(r * PT, PT), PT)
        acc[rows, :] = dot(jnp.concatenate([chip_blocks(rows, xx) for xx in near], axis=1), w_near)
        return 0

    lax.fori_loop(0, T // PT, near_tile, 0, unroll=2)
    p2[4].rest()

    def finish_gc(start, rows, v):
        sgc[rows, :] = jax.nn.sigmoid(rounded(v)) * sgc[rows, :]

    project_all(4, finish_gc)
    rec_ring.mate_far()
    opposite = lax.rem(x + 2, 4)
    w_far = chip_weight(10, opposite)

    def last_tile(r, _):
        rows = pl.ds(pl.multiple_of(r * RT, RT), RT)
        y_rec = rounded(acc[rows, :] + dot(chip_blocks(rows, opposite), w_far))
        out[rows, :] = (sgr[rows, :] * y_rec + sgc[rows, :]).astype(BF16)
        return 0

    lax.fori_loop(0, T // RT, last_tile, 0, unroll=3)
    w.left(0, wb.at[pl.ds(0, 3), pl.ds(0, 3)], mate)
    w.left(8, wb.at[pl.ds(0, 9)], mate)
    w.left(1, xs.at[pl.ds(0, 7 * TD), :], mate)
    w.left(2, mc.at[pl.ds(0, 7)], mate)
    w.left(3, mr.at[pl.ds(0, 7)], mate)

    @pl.when(s < 15)
    def _():
        w.left(5, hsend, following)

    for i in (1, 2, 3):

        @pl.when((z == 3) & (y == 3 - i) if i < 3 else (z < 3) | (y == 0))
        def _(i=i):
            w.left(6, sty.at[pl.ds(0, i), pl.ds(0, 130)], mate)

    for i in (1, 2, 3):

        @pl.when(z == 3 - i)
        def _(i=i):
            w.left(7, stz.at[pl.ds(0, i), pl.ds(0, 130)], mate)


def local(
    tokens, norm_gain, w_query, w_forget, w_input, w_outgate, w_conv_value, w_conv_gate, w_gate_rec, w_gate_conv,
    lower_bound, decay_shift, state_init, head_gain, conv_kernel, channel_gain, channel_bias, w_out_rec, w_out_conv,
):
    line = lambda v: v.reshape(1, -1)
    args = (
        tokens, line(norm_gain), w_forget, w_input, w_query, w_outgate, w_conv_value, w_conv_gate, w_gate_rec,
        w_gate_conv, line(lower_bound), decay_shift, state_init, line(head_gain), conv_kernel, line(channel_gain),
        line(channel_bias), w_out_rec, w_out_conv,
    )
    v = pltpu.VMEM
    scratch = [
        v((TD, 2048), BF16), v((1, 2048), F32), v((T, 2048), BF16), v((12, 4, 4, 128, 128), BF16),
        v((2, 128, 128), BF16), v((1, 128), F32), v((T, 128), F32), v((128, 128), F32), v((1, 128), F32),
        v((KW, 128), F32), v((1, 128), F32), v((1, 128), F32),
        v((T, 128), F32), v((T, 128), F32), v((T, 128), BF16), v((T, 128), F32), v((T, 128), F32),
        v((T + HALO, 128), F32), v((HALO, 128), BF16), v((HALO, 128), BF16), v((T, 256), F32), v((T, 256), F32),
        v((8, T + 16, 128), BF16), v((T, CONV), BF16), v((8, T, 128), BF16), v((T, 128), F32), v((T, 128), BF16),
        v((NC, 128, 128), BF16), v((16, 128), F32), v((4, 144, 128), BF16), v((4, 144, 128), BF16), v((NC, 128, 128), F32), v((T, 128), F32), v((T, 256), F32),
        pltpu.SemaphoreType.DMA((10,)), pltpu.SemaphoreType.DMA((9,)), pltpu.SemaphoreType.DMA((38,)),
    ]
    return pl.pallas_call(
        kernel,
        out_shape=jax.ShapeDtypeStruct((T, 256), BF16),
        in_specs=[pl.BlockSpec(memory_space=pltpu.HBM)] * len(args),
        out_specs=pl.BlockSpec(memory_space=pltpu.VMEM),
        scratch_shapes=scratch,
        compiler_params=pltpu.CompilerParams(
            collective_id=0, has_side_effects=True, vmem_limit_bytes=40 * 1024 * 1024
        ),
    )(*[pltpu.with_memory_space_constraint(a, pltpu.HBM) for a in args])


def solution(mesh):
    both = P("sp", "tp")
    in_specs = (
        P(("sp", "tp"), None), P(), both, both, both, both, both, both, both, both, P("tp"), both,
        P("tp", None, None), P("tp"), P(None, "tp"), P("tp"), P("tp"), P("tp", "sp"), P("tp", "sp"),
    )
    return jax.shard_map(local, mesh=mesh, in_specs=in_specs, out_specs=both, check_vma=False)
```
